128 devices in a mesh: sp: 16 (over z, y), tp: 8 (over x, core).
Axes of the slice: x: 4, y: 4, z: 4, core: 2. Of those that a mesh axis runs over, the one named last changes fastest.
Arguments:
- residual: bfloat16 [10240, 2048], P(('sp', 'tp')), may hold values from -6 to 6
- small_value_inputs: bfloat16 [10240, 1024], P('sp', 'tp'), may hold values from -6 to 6
- large_value_inputs: bfloat16 [10240, 1024], P('sp', 'tp'), may hold values from -6 to 6
- small_gate_inputs: bfloat16 [10240, 1024], P('sp', 'tp'), may hold values from -6 to 6
- large_gate_inputs: bfloat16 [10240, 1024], P('sp', 'tp'), may hold values from -6 to 6
- state_projections: bfloat16 [10240, 4, 128], P('sp'), may hold values from -6 to 6
- small_step_inputs: bfloat16 [10240, 16], P('sp', 'tp'), may hold values from -2.5 to 2.5
- large_step_inputs: bfloat16 [10240, 8], P('sp', 'tp'), may hold values from -2.5 to 2.5
- small_decay_offsets: float32 [10240, 16], P('sp', 'tp'), may hold values from -1.4 to 0
- large_decay_offsets: float32 [10240, 8], P('sp', 'tp'), may hold values from -1.4 to 0
- small_decay_rates: float32 [16], P('tp'), may hold values from -11.1 to -3.1
- large_decay_rates: float32 [8], P('tp'), may hold values from -11.1 to -3.1
- small_filter_taps: bfloat16 [4, 1024], P(None, 'tp'), may hold values from -3 to 3
- large_filter_taps: bfloat16 [4, 1024], P(None, 'tp'), may hold values from -3 to 3
- state_filter_taps: bfloat16 [4, 4, 128], replicated, may hold values from -3 to 3
- small_head_gains: float32 [1024], P('tp'), may hold values from 0.1 to 1.9
- large_head_gains: float32 [1024], P('tp'), may hold values from 0.1 to 1.9
- small_output_projection: bfloat16 [1024, 2048], P('tp'), may hold values from -0.125 to 0.125
- large_output_projection: bfloat16 [1024, 2048], P('tp'), may hold values from -0.125 to 0.125
- channel_norm_gain: float32 [2048], replicated, may hold values from 0.1 to 1.9
- gate_matrix: bfloat16 [2048, 5632], P('sp', 'tp'), may hold values from -0.125 to 0.125
- up_matrix: bfloat16 [2048, 5632], P('sp', 'tp'), may hold values from -0.125 to 0.125
- down_matrix: bfloat16 [5632, 2048], P('tp', 'sp'), may hold values from -0.078125 to 0.078125
Outputs:
- layer_out: bfloat16 [10240, 2048], P(('sp', 'tp'))
The draws below stay inside these ranges and needn't reach their ends.
All inputs are finite; a program needn't handle non-finite values.
Results may differ from the reference program's by a relative error of at most 0.015.
Values may be sent and summed in bfloat16 or wider, within the bound.
A program may use at most 64 MiB of HBM per device.

```python
import jax
import jax.numpy as jnp
from jax import lax

D = 2048
FF = 5632
SMALL_HEADS = 16
LARGE_HEADS = 8
STATE = 128
BLOCK = 64
CONV = 4
TOK_DEV = 640
TOKENS = 10240
W1 = 1024
W2 = 1024
N_TP = 8


def step_draw(key, head_outputs):
    first, second = jax.random.split(key)
    blocks = TOKENS // TOK_DEV
    offset = jax.random.uniform(first, (blocks, 1, head_outputs), jnp.float32, -1.0, 1.0)
    base = 0.5 * jax.random.truncated_normal(second, -3.0, 3.0, (blocks, TOK_DEV, head_outputs), jnp.float32)
    return (base + offset).reshape(TOKENS, head_outputs).astype(jnp.bfloat16)


def rate_draw(key, head_outputs):
    first, second, third = jax.random.split(key, 3)
    quick = jax.random.uniform(first, (head_outputs,), jnp.float32) < 0.5
    slow_rate = jax.random.uniform(second, (head_outputs,), jnp.float32, 0.2, 0.8) / (0.75 * TOKENS)
    fast_rate = 1.0 / (0.75 * jax.random.uniform(third, (head_outputs,), jnp.float32, 30.0, 100.0))
    return jnp.log(jnp.where(quick, fast_rate, slow_rate)).astype(jnp.float32)


def decay_offset_sample(key, head_outputs):
    first, second = jax.random.split(key)
    places = jax.random.randint(first, (2, head_outputs), 0, TOKENS)
    sizes = jnp.log(jax.random.uniform(second, (2, head_outputs), jnp.float32, 0.5, 0.8))
    hit = jnp.arange(TOKENS, dtype=jnp.int32)[:, None, None] == places[None, :, :]
    return jnp.sum(jnp.where(hit, sizes[None, :, :], 0.0), axis=1).astype(jnp.float32)


def draw_small_step_inputs(key, part):
    return step_draw(jax.random.fold_in(key, 11), SMALL_HEADS)


def draw_large_step_inputs(key, part):
    return step_draw(jax.random.fold_in(key, 12), LARGE_HEADS)


def draw_small_decay_rates(key, part):
    return rate_draw(jax.random.fold_in(key, 21), SMALL_HEADS)


def draw_large_decay_rates(key, part):
    return rate_draw(jax.random.fold_in(key, 22), LARGE_HEADS)


def draw_small_decay_offsets(key, part):
    return decay_offset_sample(jax.random.fold_in(key, 31), SMALL_HEADS)


def draw_large_decay_offsets(key, part):
    return decay_offset_sample(jax.random.fold_in(key, 32), LARGE_HEADS)


def steps_of(own_key, dims, cuts, low, largest):
    level = 1.0
    for position, blocks in cuts:
        heights = jax.random.uniform(jax.random.fold_in(jax.random.fold_in(own_key, 6), position), (blocks,), jnp.float32, low / len(cuts), largest / len(cuts))
        level = level * jnp.repeat(jnp.exp(heights), dims[position] // blocks).reshape((-1,) + (1,) * (len(dims) - 1 - position))
    return level


def normal_values(stream_key, shape, scale, bound, cuts=(), kind=jnp.bfloat16):
    result = jax.random.normal(stream_key, shape, jnp.float32) * scale
    if len(cuts) > 0:
        result = steps_of(stream_key, shape, cuts, -0.22, 0.18) * result
    return jnp.clip(result, min=-bound, max=bound).astype(kind)


def setup_inputs(seed: int = 0) -> dict:
    arg_keys = jax.random.split(jax.random.key(seed), 24)
    return {
        "residual": normal_values(arg_keys[0], (TOKENS, D), 1.0, 6.0, ((0, 128),)),
        "small_value_inputs": normal_values(arg_keys[1], (TOKENS, W1), 1.0, 6.0, ((0, 16), (1, 8))),
        "large_value_inputs": normal_values(arg_keys[2], (TOKENS, W2), 1.0, 6.0, ((0, 16), (1, 8))),
        "small_gate_inputs": normal_values(arg_keys[3], (TOKENS, W1), 1.0, 6.0, ((0, 16), (1, 8))),
        "large_gate_inputs": normal_values(arg_keys[4], (TOKENS, W2), 1.0, 6.0, ((0, 16), (1, 8))),
        "state_projections": normal_values(arg_keys[5], (TOKENS, 4, STATE), 1.0, 6.0, ((0, 16),)),
        "small_step_inputs": draw_small_step_inputs(jax.random.fold_in(arg_keys[23], 71), 0),
        "large_step_inputs": draw_large_step_inputs(jax.random.fold_in(arg_keys[23], 71), 0),
        "small_decay_offsets": draw_small_decay_offsets(jax.random.fold_in(arg_keys[23], 71), 0),
        "large_decay_offsets": draw_large_decay_offsets(jax.random.fold_in(arg_keys[23], 71), 0),
        "small_decay_rates": draw_small_decay_rates(jax.random.fold_in(arg_keys[23], 71), 0),
        "large_decay_rates": draw_large_decay_rates(jax.random.fold_in(arg_keys[23], 71), 0),
        "small_filter_taps": normal_values(arg_keys[12], (CONV, W1), CONV ** -0.5, 3.0, ((1, 8),)),
        "large_filter_taps": normal_values(arg_keys[13], (CONV, W2), CONV ** -0.5, 3.0, ((1, 8),)),
        "state_filter_taps": normal_values(arg_keys[14], (CONV, 4, STATE), CONV ** -0.5, 3.0),
        "small_head_gains": jnp.clip(1.0 + 0.18 * jax.random.normal(arg_keys[15], (W1,), jnp.float32), 0.1, 1.9),
        "large_head_gains": jnp.clip(1.0 + 0.18 * jax.random.normal(arg_keys[16], (W2,), jnp.float32), 0.1, 1.9),
        "small_output_projection": normal_values(arg_keys[17], (W1, D), (W1 + W2) ** -0.5, 0.125, ((0, 8),)),
        "large_output_projection": normal_values(arg_keys[18], (W2, D), (W1 + W2) ** -0.5, 0.125, ((0, 8),)),
        "channel_norm_gain": jnp.clip(1.0 + 0.18 * jax.random.normal(arg_keys[19], (D,), jnp.float32), 0.1, 1.9),
        "gate_matrix": normal_values(arg_keys[20], (D, FF), D ** -0.5, 0.125, ((0, 16), (1, 8))),
        "up_matrix": normal_values(arg_keys[21], (D, FF), D ** -0.5, 0.125, ((0, 16), (1, 8))),
        "down_matrix": normal_values(arg_keys[22], (FF, D), FF ** -0.5, 0.078125, ((0, 8), (1, 16))),
    }


HIGH = lax.Precision.HIGHEST
head_eps = 1e-05
row_eps = 1e-06

def rounded(value):
    return lax.optimization_barrier(value.astype(jnp.bfloat16)).astype(jnp.float32)

def causal_conv(series, prior_tokens, filter_taps):
    width = filter_taps.shape[0]
    length = series.shape[0]
    padded = jnp.concatenate([prior_tokens.astype(jnp.float32), series.astype(jnp.float32)], axis=0)
    total = jnp.zeros(series.shape, jnp.float32)
    for offset in range(width):
        total = total + filter_taps[offset].astype(jnp.float32)[None, :] * padded[offset:offset + length]
    return jax.nn.silu(total)

def block_scan(driven, decay_logarithm, key_vectors, read_vectors, state):
    length, head_outputs, size = driven.shape
    blocks = length // BLOCK
    mask = jnp.tril(jnp.ones((BLOCK, BLOCK), dtype=bool))[:, :, None]

    def advance(carry, pieces):
        values, decays, key_rows, read_rows = pieces
        within = jnp.cumsum(decays, axis=0)
        spread = within[:, None, :] - within[None, :, :]
        weights = jnp.where(mask, jnp.exp(jnp.where(mask, spread, 0.0)), 0.0)
        scores = jnp.dot(read_rows, key_rows.T, precision=HIGH)
        inner = jnp.einsum('ls,lsh,shp->lhp', scores, weights, values, precision=HIGH)
        carried = jnp.einsum('ln,hpn,lh->lhp', read_rows, carry, jnp.exp(within), precision=HIGH)
        tail = jnp.exp(within[-1][None, :] - within)
        fresh = jnp.einsum('ln,lh,lhp->hpn', key_rows, tail, values, precision=HIGH)
        return (carry * jnp.exp(within[-1])[:, None, None] + fresh, inner + carried)
    pieces = (driven.reshape(blocks, BLOCK, head_outputs, size), decay_logarithm.reshape(blocks, BLOCK, head_outputs), key_vectors.reshape(blocks, BLOCK, key_vectors.shape[1]), read_vectors.reshape(blocks, BLOCK, read_vectors.shape[1]))
    final, outs = lax.scan(advance, state, pieces)
    return (final, outs.reshape(length, head_outputs, size))

def heads_per_group(input_rows, gate_inputs, step_inputs, decay_offsets, decay_rates, filter_taps, head_gains, key_vectors, read_vectors):
    length, width = input_rows.shape
    head_outputs = decay_rates.shape[0]
    size = width // head_outputs
    prior_tokens = jnp.zeros((filter_taps.shape[0] - 1, width), jnp.bfloat16)
    conv_values = causal_conv(input_rows, prior_tokens, filter_taps)
    step_amount = jax.nn.softplus(step_inputs.astype(jnp.float32))
    decay_logarithm = -jnp.exp(decay_rates)[None, :] * step_amount + decay_offsets
    driven = conv_values.reshape(length, head_outputs, size) * step_amount[:, :, None]
    start_state = jnp.zeros((head_outputs, size, key_vectors.shape[1]), jnp.float32)
    _, scan_out = block_scan(driven, decay_logarithm, key_vectors, read_vectors, start_state)
    gated = scan_out * jax.nn.silu(gate_inputs.reshape(length, head_outputs, size).astype(jnp.float32))
    scale = lax.rsqrt(lax.optimization_barrier(jnp.mean(gated * gated, axis=-1, keepdims=True)) + head_eps)
    normed = gated * scale * head_gains.reshape(head_outputs, size).astype(jnp.float32)
    return normed.reshape(length, width).astype(jnp.bfloat16)

def row_norm(rows, gain):
    wide = rows.astype(jnp.float32)
    scale = lax.rsqrt(lax.optimization_barrier(jnp.mean(wide * wide, axis=-1, keepdims=True)) + row_eps)
    return (wide * scale * gain[None, :]).astype(jnp.bfloat16)

def reference(residual, small_value_inputs, large_value_inputs, small_gate_inputs, large_gate_inputs, state_projections, small_step_inputs, large_step_inputs, small_decay_offsets, large_decay_offsets, small_decay_rates, large_decay_rates, small_filter_taps, large_filter_taps, state_filter_taps, small_head_gains, large_head_gains, small_output_projection, large_output_projection, channel_norm_gain, gate_matrix, up_matrix, down_matrix):
    length = residual.shape[0]
    planes = state_projections.shape[1] * state_projections.shape[2]
    flat = state_projections.reshape(length, planes)
    flat_taps = state_filter_taps.reshape(state_filter_taps.shape[0], planes)
    prior_tokens = jnp.zeros((state_filter_taps.shape[0] - 1, planes), jnp.bfloat16)
    convolved_state_maps = causal_conv(flat, prior_tokens, flat_taps).reshape(length, state_projections.shape[1], state_projections.shape[2])
    small_head_outputs = heads_per_group(small_value_inputs, small_gate_inputs, small_step_inputs, small_decay_offsets, small_decay_rates, small_filter_taps, small_head_gains, convolved_state_maps[:, 0], convolved_state_maps[:, 1])
    large_head_outputs = heads_per_group(large_value_inputs, large_gate_inputs, large_step_inputs, large_decay_offsets, large_decay_rates, large_filter_taps, large_head_gains, convolved_state_maps[:, 2], convolved_state_maps[:, 3])
    slice_small = W1 // N_TP
    slice_large = W2 // N_TP
    mixed = jnp.zeros((length, D), jnp.float32)
    for part in range(N_TP):
        term = jnp.dot(small_head_outputs[:, part * slice_small:(part + 1) * slice_small], small_output_projection[part * slice_small:(part + 1) * slice_small], preferred_element_type=jnp.float32)
        term = term + jnp.dot(large_head_outputs[:, part * slice_large:(part + 1) * slice_large], large_output_projection[part * slice_large:(part + 1) * slice_large], preferred_element_type=jnp.float32)
        mixed = mixed + rounded(term)
    middle = (residual.astype(jnp.float32) + mixed).astype(jnp.bfloat16)
    normed = row_norm(middle, channel_norm_gain)
    gate = jnp.dot(normed, gate_matrix, preferred_element_type=jnp.float32)
    up = jnp.dot(normed, up_matrix, preferred_element_type=jnp.float32)
    hidden = (jax.nn.silu(gate) * up).astype(jnp.bfloat16)
    slice_units = FF // N_TP
    down = jnp.zeros((length, D), jnp.float32)
    for part in range(N_TP):
        down = down + rounded(jnp.dot(hidden[:, part * slice_units:(part + 1) * slice_units], down_matrix[part * slice_units:(part + 1) * slice_units], preferred_element_type=jnp.float32))
    return (middle.astype(jnp.float32) + down).astype(jnp.bfloat16)
```

```python
import jax
import jax.numpy as jnp
from jax import lax
from jax.experimental import pallas as pl
from jax.experimental.pallas import tpu as pltpu
from jax.sharding import Mesh
from jax.sharding import PartitionSpec as P

F32 = jnp.float32
BF16 = jnp.bfloat16
SP = ("z", "y")
TP = ("x", "c")
SP_TP = ("z", "y", "x", "c")

T = 640
L = 128
NB = T // L
R = 80
FD = 704
DM = 2048
H = 1024
KROWS = 128
CUT = 352

head_eps = 1e-05
row_eps = 1e-06


def silu(x):
    return x / (1.0 + jnp.exp(-x))


def dot(a, b):
    return jnp.dot(a, b, preferred_element_type=F32)


def dot_nt(a, b):
    return lax.dot_general(a, b, (((1,), (1,)), ((), ())), preferred_element_type=F32)


def dot_tn(a, b):
    return lax.dot_general(a, b, (((0,), (0,)), ((), ())), preferred_element_type=F32)


def kernel(
    res_in, vs_in, vl_in, gs_in, gl_in, sp_in, ws_in, wl_in, g_in, u_in, d_in,
    meta, taps_s, taps_l, taps_m, gain_s, gain_l, gain_n,
    out,
    xin, gin, resv, halo, cbuf, conv_k, drive, fresh, inner, heads, hpart, lhs,
    wo, wg, wu, wd, st1, st2, psend, rp, rm, ag, hid, psend2, rp2, rm2, midv,
    loc_sem, halo_sem, w_send, w_recv, pair_sem, st_sem, hp_sem, rs_sem, ag_sem, rs2_sem,
):
    z, y, x, c = (lax.axis_index(n) for n in ("z", "y", "x", "c"))
    rem = lax.rem
    o = 1 - c

    def at(base, by):
        return rem(base + (by % 4), 4)

    last = y == 3
    first = y == 0
    nxt = {"z": rem(z + lax.div(y + 1, 4), 4), "y": rem(y + 1, 4)}
    prv = {"z": rem(z + 3 + lax.div(y + 3, 4), 4), "y": rem(y + 3, 4)}

    def there(**kw):
        base = {"z": z, "y": y, "x": x, "c": c}
        base.update(kw)
        return (base["z"], base["y"], base["x"], base["c"])

    def remote(src, dst, send, recv, **kw):
        return pltpu.make_async_remote_copy(
            src_ref=src, dst_ref=dst, send_sem=send, recv_sem=recv,
            device_id=there(**kw), device_id_type=pl.DeviceIdType.MESH,
        )

    pending = []

    def go(cp):
        cp.start()
        pending.append(cp)
        return cp

    def yl(i):
        return pl.ds(pl.multiple_of(i * 128, 128), 128)

    local = [
        (vs_in, xin.at[:, pl.ds(0, 128)]),
        (vl_in, xin.at[:, pl.ds(128, 128)]),
        (sp_in, xin.at[:, pl.ds(256, 512)]),
        (gs_in, gin.at[:, pl.ds(0, 128)]),
        (gl_in, gin.at[:, pl.ds(128, 128)]),
        (res_in, resv),
        (ws_in, wo.at[c, pl.ds(0, 128)]),
        (wl_in, wo.at[c, pl.ds(128, 128)]),
        (g_in, wg.at[c, z, y]),
        (u_in, wu.at[c, z, y]),
        (d_in, wd.at[c, z, :, yl(y)]),
    ]
    local = [pltpu.make_async_copy(a, b, loc_sem.at[i]) for i, (a, b) in enumerate(local)]
    for cp in local:
        cp.start()

    barrier = pltpu.get_barrier_semaphore()
    peers = [
        dict(c=o), dict(x=at(x, 1)), dict(x=at(x, 3)),
        dict(y=at(y, 1)), dict(y=at(y, 2)), dict(y=at(y, 3)),
        dict(z=at(z, 1)), dict(z=at(z, 2)), dict(z=at(z, 3)),
        nxt, prv,
    ]
    for p in peers:
        pl.semaphore_signal(barrier, inc=1, device_id=there(**p), device_id_type=pl.DeviceIdType.MESH)
    pl.semaphore_wait(barrier, len(peers))

    tail = pl.ds(T - 16, 16)
    halos = [
        go(remote(src.at[tail], halo.at[:, cols], halo_sem.at[0, i], halo_sem.at[1, i], **nxt))
        for i, (src, cols) in enumerate(
            ((vs_in, pl.ds(0, 128)), (vl_in, pl.ds(128, 128)), (sp_in, pl.ds(256, 512)))
        )
    ]

    names = ("G", "U", "A", "B")
    own_src = {
        "G": g_in, "U": u_in,
        "A": d_in.at[pl.ds(0, CUT)], "B": d_in.at[pl.ds(CUT, CUT)],
    }

    def unit(name, rz, ry):
        zz, yy = at(z, rz), at(y, ry)
        if name == "G":
            return wg.at[c, zz, yy]
        if name == "U":
            return wu.at[c, zz, yy]
        rows = pl.ds(0, CUT) if name == "A" else pl.ds(CUT, CUT)
        return wd.at[c, zz, rows, yl(yy)]

    n_sent = [0]

    def w_sem(name, rz, ry):
        return w_recv.at[names.index(name), rz % 4, ry % 4]

    def wsend(name, rz, ry, dz=0, dy=0):
        src = own_src[name] if (rz, ry) == (0, 0) else unit(name, rz, ry)
        k = n_sent[0]
        n_sent[0] += 1
        go(remote(
            src, unit(name, rz, ry), w_send.at[k], w_sem(name, rz - dz, ry - dy),
            z=at(z, dz), y=at(y, dy),
        ))

    def wwait(name, rz, ry):
        ref = unit(name, rz, ry)
        remote(ref, ref, w_send.at[0], w_sem(name, rz, ry)).wait_recv()

    def send(name, first_axis, second_axis, step):
        swap = name in ("U", "B")
        rz, ry = (first_axis, second_axis) if swap else (second_axis, first_axis)
        dz, dy = step if swap else (step[1], step[0])
        wsend(name, rz, ry, dz, dy)

    def wait(name, first_axis, second_axis):
        if name in ("U", "B"):
            wwait(name, first_axis, second_axis)
        else:
            wwait(name, second_axis, first_axis)

    UP, DOWN = 1, -1

    def w_own(pair):
        for n in pair:
            send(n, 0, 0, (UP, 0))
            send(n, 0, 0, (DOWN, 0))
        for n in pair:
            send(n, 0, 0, (0, UP))
            send(n, 0, 0, (0, DOWN))

    def w_first_relay(pair):
        for n in pair:
            if n in ("G", "U"):
                wait(n, -1, 0)
                send(n, -1, 0, (UP, 0))
                wait(n, 1, 0)
            else:
                wait(n, 1, 0)
                send(n, 1, 0, (DOWN, 0))
                wait(n, -1, 0)

    def w_second(pair, r):
        for n in pair:
            if r == 2:
                wait(n, 2, 0)
            send(n, r, 0, (0, UP))
            send(n, r, 0, (0, DOWN))

    def w_second_relay(pair, r):
        for n in pair:
            if r in (0, 1):
                wait(n, r, -1)
                send(n, r, -1, (0, UP))
                wait(n, r, 1)
            else:
                wait(n, r, 1)
                send(n, r, 1, (0, DOWN))
                wait(n, r, -1)

    def w_last(pair):
        for n in pair:
            for r in (0, 1, -1, 2):
                wait(n, r, 2)

    n_pair = [0]
    pair_waits = []

    def plane(name, core, k):
        if name == "G":
            return wg.at[core, k]
        if name == "A":
            return wd.at[core, k, pl.ds(0, CUT)]
        if name == "U":
            return wu.at[core, :, k]
        return wd.at[core, :, pl.ds(CUT, CUT), yl(k)]

    def share(name, r):
        k = n_pair[0]
        n_pair[0] += 1
        pos = at(y, r) if name in ("U", "B") else at(z, r)
        go(remote(plane(name, c, pos), plane(name, c, pos), pair_sem.at[0, k], pair_sem.at[1, k], c=o))
        got = plane(name, o, pos)
        pair_waits.append((name, remote(got, got, pair_sem.at[0, k], pair_sem.at[1, k], c=o)))

    w_own(("G", "U"))

    wo_copies = [
        go(remote(src, wo.at[c, rows], hp_sem.at[0, 4 + i], hp_sem.at[1, 4 + i], c=o))
        for i, (src, rows) in enumerate(((ws_in, pl.ds(0, 128)), (wl_in, pl.ds(128, 128))))
    ]

    lane = lax.broadcasted_iota(jnp.int32, (8, L), 1)
    rows = []
    both = []
    row8 = lax.broadcasted_iota(jnp.int32, (8, L), 0)
    for k in range(NB):
        raw = meta[:, k * L : (k + 1) * L]
        acc = raw
        for sft in (1, 2, 4, 8, 16, 32, 64):
            acc = acc + jnp.where(lane >= sft, pltpu.roll(acc, sft, 1), 0.0)
        rows.append(acc)
        both.append(jnp.where(row8 < 3, acc, raw))
    both.append(jnp.zeros((L - 8 * NB, L), F32))
    cols = jnp.concatenate(both, axis=0).T
    grown = jnp.exp(cols)
    shrunk = jnp.exp(cols[L - 1 : L, :] - cols)

    half = lax.broadcasted_iota(jnp.int32, (L, L), 1) < 64
    half1 = lax.broadcasted_iota(jnp.int32, (1, L), 1) < 64

    def spread(m, k, off):
        b = 8 * k + off
        small = jnp.where(half, m[:, b : b + 1], m[:, b + 1 : b + 2])
        large = jnp.broadcast_to(m[:, b + 2 : b + 3], (L, L))
        return small, large

    def block_decay(k):
        b = 8 * k
        e = grown[L - 1 : L]
        small = jnp.where(half1, e[:, b : b + 1], e[:, b + 1 : b + 2])
        large = jnp.broadcast_to(e[:, b + 2 : b + 3], (1, L))
        return jnp.concatenate([small, large], axis=1)

    tap_rows = []
    for j in range(4):
        m = taps_m[j].astype(F32)
        tap_rows.append(
            [taps_s[j : j + 1].astype(F32), taps_l[j : j + 1].astype(F32)]
            + [m[i : i + 1] for i in range(4)]
        )

    def conv(k, g):
        total = None
        for j in range(4):
            part = tap_rows[j][g] * cbuf[k * L + 5 + j : k * L + 5 + j + L, g * 128 : g * 128 + 128]
            total = part if total is None else total + part
        return silu(total)

    for i in range(3):
        local[i].wait()
    for k in range(NB):
        cbuf[8 + k * L : 8 + (k + 1) * L, :] = xin[k * L : (k + 1) * L, :].astype(F32)
    decays = [block_decay(k) for k in range(NB)]

    def first_pass(k):
        dt_s, dt_l = spread(cols, k, 3)
        sh_s, sh_l = spread(shrunk, k, 0)
        d_s = conv(k, 0) * dt_s
        d_l = conv(k, 1) * dt_l
        blk = pl.ds(k * L, L)
        drive[blk, 0:128] = d_s.astype(BF16)
        drive[blk, 128:256] = d_l.astype(BF16)
        k_s = conv(k, 2).astype(BF16)
        k_l = conv(k, 4).astype(BF16)
        conv_k[blk, 0:128] = k_s
        conv_k[blk, 128:256] = conv(k, 3).astype(BF16)
        conv_k[blk, 256:384] = k_l
        conv_k[blk, 384:512] = conv(k, 5).astype(BF16)
        fresh[k, :, 0:128] = dot_tn(k_s, (d_s * sh_s).astype(BF16))
        fresh[k, :, 128:256] = dot_tn(k_l, (d_l * sh_l).astype(BF16))

    for k in range(1, NB):
        first_pass(k)
    for cp in halos:
        cp.wait_recv()
    start = jnp.where(jnp.logical_and(z == 0, y == 0), 0.0, 1.0)
    cbuf[0:8, :] = halo[8:16, :].astype(F32) * start
    first_pass(0)

    state = fresh[0]
    total = decays[0]
    for k in range(1, NB):
        state = state * decays[k] + fresh[k]
        total = total * decays[k]

    st1[0, 0:128] = state.astype(BF16)
    st1[0, 128:144] = jnp.broadcast_to(total, (16, 256)).astype(BF16)
    for r in (1, 2, 3):
        go(remote(st1.at[0], st1.at[r], st_sem.at[0, r], st_sem.at[1, r], y=at(y, r)))

    mask = lax.broadcasted_iota(jnp.int32, (L, L), 0) >= lax.broadcasted_iota(jnp.int32, (L, L), 1)

    def weights_of(k, h):
        b = 8 * k + h
        diff = cols[:, b : b + 1] - rows[k][h : h + 1, :]
        return jnp.exp(jnp.where(mask, diff, -1e30))

    def second_pass(k):
        blk = pl.ds(k * L, L)
        s_s = dot_nt(conv_k[blk, 128:256], conv_k[blk, 0:128])
        s_l = dot_nt(conv_k[blk, 384:512], conv_k[blk, 256:384])
        d_s = drive[blk, 0:128]
        o_0 = dot((s_s * weights_of(k, 0)).astype(BF16), d_s)
        o_1 = dot((s_s * weights_of(k, 1)).astype(BF16), d_s)
        inner[blk, 0:128] = jnp.where(half, o_0, o_1)
        inner[blk, 128:256] = dot((s_l * weights_of(k, 2)).astype(BF16), drive[blk, 128:256])

    second_pass(0)
    second_pass(1)

    def slot_of(buf, me, other):
        return buf[rem(me - other + 4, 4)].astype(F32)

    for r in (1, 2, 3):
        remote(st1.at[0], st1.at[r], st_sem.at[0, r], st_sem.at[1, r]).wait_recv()
    inside = jnp.zeros((128, 256), F32)
    inside_d = jnp.ones((1, 256), F32)
    line = jnp.zeros((128, 256), F32)
    line_d = jnp.ones((1, 256), F32)
    for j in range(4):
        blob = slot_of(st1, y, j)
        s_j, d_j = blob[0:128], blob[128:129]
        line = line * d_j + s_j
        line_d = line_d * d_j
        inside = jnp.where(j < y, line, inside)
        inside_d = jnp.where(j < y, line_d, inside_d)
    st2[0, 0:128] = line.astype(BF16)
    st2[0, 128:144] = jnp.broadcast_to(line_d, (16, 256)).astype(BF16)
    for r in (1, 2, 3):
        go(remote(st2.at[0], st2.at[r], st_sem.at[2, r], st_sem.at[3, r], z=at(z, r)))

    w_first_relay(("G", "U"))
    w_second(("G", "U"), 1)
    w_second(("G", "U"), -1)
    w_own(("A", "B"))

    for k in range(2, NB):
        second_pass(k)

    for r in (1, 2, 3):
        remote(st2.at[0], st2.at[r], st_sem.at[2, r], st_sem.at[3, r]).wait_recv()
    before = jnp.zeros((128, 256), F32)
    run = jnp.zeros((128, 256), F32)
    for j in range(4):
        blob = slot_of(st2, z, j)
        run = run * blob[128:129] + blob[0:128]
        before = jnp.where(j < z, run, before)
    carry = before * inside_d + inside

    for i in (3, 4):
        local[i].wait()

    for k in range(NB):
        blk = pl.ds(k * L, L)
        gr_s, gr_l = spread(grown, k, 0)
        h_in = carry.astype(BF16)
        o_s = inner[blk, 0:128] + dot(conv_k[blk, 128:256], h_in[:, 0:128]) * gr_s
        o_l = inner[blk, 128:256] + dot(conv_k[blk, 384:512], h_in[:, 128:256]) * gr_l
        carry = carry * decays[k] + fresh[k]
        o_s = o_s * silu(gin[blk, 0:128].astype(F32))
        o_l = o_l * silu(gin[blk, 128:256].astype(F32))
        q = o_s * o_s
        q_0 = jnp.sum(jnp.where(half, q, 0.0), axis=1, keepdims=True)
        q_1 = jnp.sum(jnp.where(half, 0.0, q), axis=1, keepdims=True)
        q_l = jnp.sum(o_l * o_l, axis=1, keepdims=True)
        sc_0 = lax.rsqrt(q_0 * (1.0 / 64) + head_eps)
        sc_1 = lax.rsqrt(q_1 * (1.0 / 64) + head_eps)
        sc_l = lax.rsqrt(q_l * (1.0 / 128) + head_eps)
        heads[blk, 0:128] = (o_s * jnp.where(half, sc_0, sc_1) * gain_s[...]).astype(BF16)
        heads[blk, 128:256] = (o_l * sc_l * gain_l[...]).astype(BF16)

    def rows_of(b, core):
        return pl.ds(pl.multiple_of((2 * b + core) * R, 16), R)

    for b in range(4):
        go(remote(heads.at[rows_of(b, o)], hpart.at[b], hp_sem.at[0, b], hp_sem.at[1, b], c=o))
    for b in range(4):
        lhs[b] = heads[rows_of(b, c), :]
    for i in (6, 7):
        local[i].wait()
    own_rows = lhs[...].reshape(4 * R, 256)
    for cp in wo_copies:
        cp.wait_recv()
    for b in range(4):
        remote(hpart.at[b], hpart.at[b], hp_sem.at[0, b], hp_sem.at[1, b]).wait_recv()
    part_rows = hpart[...].reshape(4 * R, 256)

    x1, x2, x3 = at(x, 1), at(x, 2), at(x, 3)

    class Sum:
        def __init__(self, parts, from_left, from_right, sems):
            self.parts, self.left, self.right, self.sems = parts, from_left, from_right, sems

        def to_right(self, slot, block, h):
            go(remote(self.parts.at[block, h], self.left.at[slot], self.sems.at[0, slot], self.sems.at[1, slot], x=x1))

        def to_left(self, slot, block, h):
            go(remote(self.parts.at[block, h], self.right.at[slot], self.sems.at[2, slot], self.sems.at[3, slot], x=x3))

        def wait_left(self, slot):
            remote(self.left.at[slot], self.left.at[slot], self.sems.at[0, slot], self.sems.at[1, slot]).wait_recv()

        def wait_right(self, slot):
            remote(self.right.at[slot], self.right.at[slot], self.sems.at[2, slot], self.sems.at[3, slot]).wait_recv()

        def after_half(self, h):
            if h == 0:
                self.to_right(0, x2, 0)
                self.to_left(1, x3, 0)
            else:
                self.to_right(1, x1, 1)
                self.to_left(0, x2, 1)

        def merge(self):
            self.wait_left(0)
            self.parts[x1, 0] = (self.parts[x1, 0].astype(F32) + self.left[0].astype(F32)).astype(BF16)
            self.to_right(2, x1, 0)
            self.wait_right(0)
            self.parts[x3, 1] = (self.parts[x3, 1].astype(F32) + self.right[0].astype(F32)).astype(BF16)
            self.to_left(2, x3, 1)

        def result(self):
            self.wait_right(1)
            self.wait_left(1)
            self.wait_left(2)
            self.wait_right(2)
            lo = self.parts[x, 0].astype(F32) + self.left[2].astype(F32) + self.right[1].astype(F32)
            hi = self.parts[x, 1].astype(F32) + self.left[1].astype(F32) + self.right[2].astype(F32)
            return lo, hi

    mixed = Sum(psend, rp, rm, rs_sem)
    for h in range(2):
        for q in range(4):
            n = pl.ds(h * H + q * 256, 256)
            acc = dot(own_rows, wo[c, :, n]) + dot(part_rows, wo[o, :, n])
            psend[:, h, :, q * 256 : (q + 1) * 256] = acc.reshape(4, R, 256).astype(BF16)
        mixed.after_half(h)
    mixed.merge()

    w_first_relay(("A", "B"))
    w_second_relay(("G", "U"), 0)

    local[5].wait()
    lo, hi = mixed.result()
    mid_lo = (resv[:, 0:H].astype(F32) + lo).astype(BF16)
    mid_hi = (resv[:, H:DM].astype(F32) + hi).astype(BF16)
    midv[0] = mid_lo
    midv[1] = mid_hi
    f_lo, f_hi = mid_lo.astype(F32), mid_hi.astype(F32)
    square = jnp.sum(f_lo * f_lo, axis=1, keepdims=True) + jnp.sum(f_hi * f_hi, axis=1, keepdims=True)
    scale = lax.rsqrt(square * (1.0 / DM) + row_eps)
    ag[x, 0] = (f_lo * scale * gain_n[:, 0:H]).astype(BF16)
    ag[x, 1] = (f_hi * scale * gain_n[:, H:DM]).astype(BF16)

    def ag_right(slot, block, h):
        go(remote(ag.at[block, h], ag.at[block, h], ag_sem.at[0, slot], ag_sem.at[1, slot], x=x1))

    def ag_left(slot, block, h):
        go(remote(ag.at[block, h], ag.at[block, h], ag_sem.at[2, slot], ag_sem.at[3, slot], x=x3))

    def ag_wait(side, slot, block, h):
        remote(ag.at[block, h], ag.at[block, h], ag_sem.at[0, slot], ag_sem.at[side, slot]).wait_recv()

    ag_right(0, x, 0)
    ag_left(0, x, 1)
    ag_right(1, x, 1)
    ag_left(1, x, 0)

    w_second(("G", "U"), 2)
    w_second_relay(("G", "U"), 1)
    w_second_relay(("G", "U"), -1)

    ag_wait(1, 0, x3, 0)
    ag_right(2, x3, 0)
    ag_wait(3, 0, x1, 1)
    ag_left(2, x1, 1)

    for i in (8, 9, 10):
        local[i].wait()
    for n in ("G", "U"):
        share(n, 0)
    w_second_relay(("G", "U"), 2)
    for n in ("G", "U"):
        share(n, 1)
        share(n, -1)
    w_second(("A", "B"), 1)
    w_second(("A", "B"), -1)
    w_second(("A", "B"), 2)
    for r in (0, 1, -1, 2):
        w_second_relay(("A", "B"), r)
    w_last(("G", "U"))
    for n in ("G", "U"):
        share(n, 2)
    for n in ("A", "B"):
        share(n, 0)
        share(n, 1)
        share(n, -1)

    ag_wait(1, 1, x3, 1)
    ag_wait(3, 1, x1, 0)
    ag_wait(1, 2, x2, 0)
    ag_wait(3, 2, x2, 1)

    def expand(core):
        for n0, n in ((0, 256), (256, 256), (512, 192)):
            gate = up = None
            for h in range(2):
                a = ag[:, h].reshape(4 * R, H)
                zs = slice(2 * h, 2 * h + 2)
                w_gate = wg[core, zs, :, :, n0 : n0 + n].reshape(H, n)
                w_up = wu[core, zs, :, :, n0 : n0 + n].reshape(H, n)
                gate = dot(a, w_gate) if gate is None else gate + dot(a, w_gate)
                up = dot(a, w_up) if up is None else up + dot(a, w_up)
            hid[core, :, n0 : n0 + n] = (silu(gate) * up).astype(BF16)

    expand(c)
    for name, w in pair_waits:
        if name in ("G", "U"):
            w.wait_recv()
    expand(o)

    w_last(("A", "B"))
    for n in ("A", "B"):
        share(n, 2)
    for name, w in pair_waits:
        if name in ("A", "B"):
            w.wait_recv()

    down = Sum(psend2, rp2, rm2, rs2_sem)
    for h in range(2):
        for q in range(4):
            zz, n0 = 2 * h + q // 2, (q % 2) * 256
            acc = dot(hid[0], wd[0, zz, :, n0 : n0 + 256]) + dot(hid[1], wd[1, zz, :, n0 : n0 + 256])
            psend2[:, h, :, q * 256 : (q + 1) * 256] = acc.reshape(4, R, 256).astype(BF16)
        down.after_half(h)
    down.merge()
    lo, hi = down.result()
    out[:, 0:H] = (midv[0].astype(F32) + lo).astype(BF16)
    out[:, H:DM] = (midv[1].astype(F32) + hi).astype(BF16)

    for cp in pending:
        cp.wait_send()


def on_device(
    residual, small_value_inputs, large_value_inputs, small_gate_inputs, large_gate_inputs,
    state_projections, small_step_inputs, large_step_inputs, small_decay_offsets,
    large_decay_offsets, small_decay_rates, large_decay_rates, small_filter_taps,
    large_filter_taps, state_filter_taps, small_head_gains, large_head_gains,
    small_output_projection, large_output_projection, channel_norm_gain, gate_matrix,
    up_matrix, down_matrix,
):
    flat = state_projections.reshape(T, 512)
    steps = jnp.concatenate([small_step_inputs, large_step_inputs], axis=1).astype(F32)
    offsets = jnp.concatenate([small_decay_offsets, large_decay_offsets], axis=1)
    rates = jnp.concatenate([small_decay_rates, large_decay_rates])
    dt = jax.nn.softplus(steps)
    log_decay = -jnp.exp(rates)[None, :] * dt + offsets
    meta = jnp.concatenate([log_decay.T, dt.T, jnp.zeros((2, T), F32)], axis=0)

    anywhere = pl.BlockSpec(memory_space=pl.ANY)
    vmem = pl.BlockSpec(memory_space=pltpu.VMEM)
    dma = pltpu.SemaphoreType.DMA
    V = pltpu.VMEM
    return pl.pallas_call(
        kernel,
        out_shape=jax.ShapeDtypeStruct((R, DM), BF16),
        in_specs=[anywhere] * 11 + [vmem] * 7,
        out_specs=vmem,
        scratch_shapes=[
            V((T, 768), BF16),
            V((T, 256), BF16),
            V((R, DM), BF16),
            V((16, 768), BF16),
            V((T + 8, 768), F32),
            V((T, 512), BF16),
            V((T, 256), BF16),
            V((NB, 128, 256), F32),
            V((T, 256), F32),
            V((T, 256), BF16),
            V((4, R, 256), BF16),
            V((4, R, 256), BF16),
            V((2, 256, DM), BF16),
            V((2, 4, 4, KROWS, FD), BF16),
            V((2, 4, 4, KROWS, FD), BF16),
            V((2, 4, FD, 512), BF16),
            V((4, 144, 256), BF16),
            V((4, 144, 256), BF16),
            V((4, 2, R, H), BF16),
            V((3, R, H), BF16),
            V((3, R, H), BF16),
            V((4, 2, R, H), BF16),
            V((2, 4 * R, FD), BF16),
            V((4, 2, R, H), BF16),
            V((3, R, H), BF16),
            V((3, R, H), BF16),
            V((2, R, H), BF16),
            dma((11,)),
            dma((2, 3)),
            dma((60,)),
            dma((4, 4, 4)),
            dma((2, 16)),
            dma((4, 4)),
            dma((2, 6)),
            dma((4, 3)),
            dma((4, 3)),
            dma((4, 3)),
        ],
        compiler_params=pltpu.CompilerParams(
            collective_id=0, has_side_effects=True, vmem_limit_bytes=60 * 1024 * 1024
        ),
    )(
        residual, small_value_inputs, large_value_inputs, small_gate_inputs, large_gate_inputs,
        flat, small_output_projection, large_output_projection, gate_matrix, up_matrix, down_matrix,
        meta, small_filter_taps, large_filter_taps, state_filter_taps,
        small_head_gains.reshape(1, 128), large_head_gains.reshape(1, 128),
        channel_norm_gain.reshape(1, DM),
    )


def solution(mesh):
    split = Mesh(mesh.devices.reshape(4, 4, 4, 2), ("z", "y", "x", "c"))
    in_specs = (
        P(SP_TP, None),
        P(SP, TP),
        P(SP, TP),
        P(SP, TP),
        P(SP, TP),
        P(SP, None, None),
        P(SP, TP),
        P(SP, TP),
        P(SP, TP),
        P(SP, TP),
        P(TP),
        P(TP),
        P(None, TP),
        P(None, TP),
        P(),
        P(TP),
        P(TP),
        P(TP, None),
        P(TP, None),
        P(),
        P(SP, TP),
        P(SP, TP),
        P(TP, SP),
    )
    return jax.shard_map(
        on_device, mesh=split, in_specs=in_specs, out_specs=P(SP_TP, None), check_vma=False
    )
```

```python
import jax
import jax.numpy as jnp
from jax import lax
from jax.experimental import pallas as pl
from jax.experimental.pallas import tpu as pltpu
from jax.sharding import Mesh
from jax.sharding import PartitionSpec as P

F32 = jnp.float32
BF16 = jnp.bfloat16
SP = ("z", "y")
TP = ("x", "c")
SP_TP = ("z", "y", "x", "c")

T = 640
L = 128
NB = T // L
R = 80
FD = 704
DM = 2048
H = 1024
KROWS = 128
CUT = 352
Q = 512
ORDER = (0, 2, 1, 3)

head_eps = 1e-05
row_eps = 1e-06


def silu(x):
    return x / (1.0 + jnp.exp(-x))


def dot(a, b):
    return jnp.dot(a, b, preferred_element_type=F32)


def dot_nt(a, b):
    return lax.dot_general(a, b, (((1,), (1,)), ((), ())), preferred_element_type=F32)


def dot_tn(a, b):
    return lax.dot_general(a, b, (((0,), (0,)), ((), ())), preferred_element_type=F32)


def kernel(
    res_in, vs_in, vl_in, gs_in, gl_in, sp_in, ws_in, wl_in, g_in, u_in, d_in,
    steps_s, steps_l, offs_s, offs_l, rates_s, rates_l, taps_s, taps_l, taps_m, gain_s, gain_l, gain_n,
    out,
    xin, gin, resv, halo, cbuf, conv_k, drive, fresh, inner, heads, hpart, lhs,
    wo, wg, wu, wd, st1, st2, psend, rp, rm, ag, hid, psend2, rp2, rm2, midv,
    loc_sem, halo_sem, w_send, w_recv, pair_sem, st_sem, hp_sem, rs_sem, ag_sem, rs2_sem,
):
    z, y, x, c = (lax.axis_index(n) for n in ("z", "y", "x", "c"))
    rem = lax.rem
    o = 1 - c

    def at(base, by):
        return rem(base + (by % 4), 4)

    nxt = {"z": rem(z + lax.div(y + 1, 4), 4), "y": rem(y + 1, 4)}
    prv = {"z": rem(z + 3 + lax.div(y + 3, 4), 4), "y": rem(y + 3, 4)}

    def there(**kw):
        base = {"z": z, "y": y, "x": x, "c": c}
        base.update(kw)
        return (base["z"], base["y"], base["x"], base["c"])

    def remote(src, dst, send, recv, **kw):
        return pltpu.make_async_remote_copy(
            src_ref=src, dst_ref=dst, send_sem=send, recv_sem=recv,
            device_id=there(**kw), device_id_type=pl.DeviceIdType.MESH,
        )

    pending = []

    def go(cp):
        cp.start()
        pending.append(cp)
        return cp

    local = [
        (vs_in, xin.at[:, pl.ds(0, 128)]),
        (vl_in, xin.at[:, pl.ds(128, 128)]),
        (sp_in, xin.at[:, pl.ds(256, 512)]),
        (gs_in, gin.at[:, pl.ds(0, 128)]),
        (gl_in, gin.at[:, pl.ds(128, 128)]),
        (res_in, resv),
        (ws_in, wo.at[c, pl.ds(0, 128)]),
        (wl_in, wo.at[c, pl.ds(128, 128)]),
        (g_in, wg.at[c, z, y]),
        (u_in, wu.at[c, z, y]),
        (d_in, wd.at[c, z, y]),
    ]
    local = [pltpu.make_async_copy(a, b, loc_sem.at[i]) for i, (a, b) in enumerate(local)]
    for cp in local:
        cp.start()

    barrier = pltpu.get_barrier_semaphore()
    peers = [
        dict(c=o), dict(x=at(x, 1)), dict(x=at(x, 3)),
        dict(y=at(y, 1)), dict(y=at(y, 2)), dict(y=at(y, 3)),
        dict(z=at(z, 1)), dict(z=at(z, 2)), dict(z=at(z, 3)),
        nxt, prv,
    ]
    for p in peers:
        pl.semaphore_signal(barrier, inc=1, device_id=there(**p), device_id_type=pl.DeviceIdType.MESH)
    lane = lax.broadcasted_iota(jnp.int32, (8, L), 1)
    rows = []
    both = []
    row8 = lax.broadcasted_iota(jnp.int32, (8, L), 0)
    raw_steps = jnp.concatenate([steps_s[...].astype(F32), steps_l[...].astype(F32)], axis=0)
    softened = jnp.maximum(raw_steps, 0.0) + jnp.log1p(jnp.exp(-jnp.abs(raw_steps)))
    head = lax.broadcasted_iota(jnp.int32, (3, T), 0)
    rate = jnp.where(head == 0, rates_s[0], jnp.where(head == 1, rates_s[1], rates_l[0]))
    offsets = jnp.concatenate([offs_s[...], offs_l[...]], axis=0)
    meta = jnp.concatenate(
        [offsets - jnp.exp(rate) * softened, softened, jnp.zeros((2, T), F32)], axis=0
    )
    for k in range(NB):
        raw = meta[:, k * L : (k + 1) * L]
        acc = raw
        for sft in (1, 2, 4, 8, 16, 32, 64):
            acc = acc + jnp.where(lane >= sft, pltpu.roll(acc, sft, 1), 0.0)
        rows.append(acc)
        both.append(jnp.where(row8 < 3, acc, raw))
    both.append(jnp.zeros((L - 8 * NB, L), F32))
    cols = jnp.concatenate(both, axis=0).T
    grown = jnp.exp(cols)
    shrunk = jnp.exp(cols[L - 1 : L, :] - cols)

    half = lax.broadcasted_iota(jnp.int32, (L, L), 1) < 64
    half1 = lax.broadcasted_iota(jnp.int32, (1, L), 1) < 64

    def spread(m, k, off):
        b = 8 * k + off
        small = jnp.where(half, m[:, b : b + 1], m[:, b + 1 : b + 2])
        large = jnp.broadcast_to(m[:, b + 2 : b + 3], (L, L))
        return small, large

    def block_decay(k):
        b = 8 * k
        e = grown[L - 1 : L]
        small = jnp.where(half1, e[:, b : b + 1], e[:, b + 1 : b + 2])
        large = jnp.broadcast_to(e[:, b + 2 : b + 3], (1, L))
        return jnp.concatenate([small, large], axis=1)

    tap_rows = []
    for j in range(4):
        m = taps_m[j].astype(F32)
        tap_rows.append(
            [taps_s[j : j + 1].astype(F32), taps_l[j : j + 1].astype(F32)]
            + [m[i : i + 1] for i in range(4)]
        )

    def conv(k, g):
        total = None
        for j in range(4):
            part = tap_rows[j][g] * cbuf[k * L + 5 + j : k * L + 5 + j + L, g * 128 : g * 128 + 128]
            total = part if total is None else total + part
        return silu(total)

    for i in range(3):
        local[i].wait()
    for k in range(NB):
        cbuf[8 + k * L : 8 + (k + 1) * L, :] = xin[k * L : (k + 1) * L, :].astype(F32)
    decays = [block_decay(k) for k in range(NB)]

    def first_pass(k):
        dt_s, dt_l = spread(cols, k, 3)
        sh_s, sh_l = spread(shrunk, k, 0)
        d_s = conv(k, 0) * dt_s
        d_l = conv(k, 1) * dt_l
        blk = pl.ds(k * L, L)
        drive[blk, 0:128] = d_s.astype(BF16)
        drive[blk, 128:256] = d_l.astype(BF16)
        k_s = conv(k, 2).astype(BF16)
        k_l = conv(k, 4).astype(BF16)
        conv_k[blk, 0:128] = k_s
        conv_k[blk, 128:256] = conv(k, 3).astype(BF16)
        conv_k[blk, 256:384] = k_l
        conv_k[blk, 384:512] = conv(k, 5).astype(BF16)
        fresh[k, :, 0:128] = dot_tn(k_s, (d_s * sh_s).astype(BF16))
        fresh[k, :, 128:256] = dot_tn(k_l, (d_l * sh_l).astype(BF16))

    pl.semaphore_wait(barrier, len(peers))

    tail = pl.ds(T - 16, 16)
    halos = [
        go(remote(src.at[tail], halo.at[:, cols], halo_sem.at[0, i], halo_sem.at[1, i], **nxt))
        for i, (src, cols) in enumerate(
            ((vs_in, pl.ds(0, 128)), (vl_in, pl.ds(128, 128)), (sp_in, pl.ds(256, 512)))
        )
    ]

    names = ("G", "U", "A", "B")
    own_src = {
        "G": g_in, "U": u_in,
        "A": d_in.at[pl.ds(0, CUT)], "B": d_in.at[pl.ds(CUT, CUT)],
    }

    def unit(name, rz, ry):
        zz, yy = at(z, rz), at(y, ry)
        if name == "G":
            return wg.at[c, zz, yy]
        if name == "U":
            return wu.at[c, zz, yy]
        rows = pl.ds(0, CUT) if name == "A" else pl.ds(CUT, CUT)
        return wd.at[c, zz, yy, rows]

    n_sent = [0]

    def w_sem(name, rz, ry):
        return w_recv.at[names.index(name), rz % 4, ry % 4]

    def wsend(name, rz, ry, dz=0, dy=0):
        src = own_src[name] if (rz, ry) == (0, 0) else unit(name, rz, ry)
        k = n_sent[0]
        n_sent[0] += 1
        go(remote(
            src, unit(name, rz, ry), w_send.at[k], w_sem(name, rz - dz, ry - dy),
            z=at(z, dz), y=at(y, dy),
        ))

    def wwait(name, rz, ry):
        ref = unit(name, rz, ry)
        remote(ref, ref, w_send.at[0], w_sem(name, rz, ry)).wait_recv()

    def send(name, first_axis, second_axis, step):
        swap = name in ("U", "B")
        rz, ry = (first_axis, second_axis) if swap else (second_axis, first_axis)
        dz, dy = step if swap else (step[1], step[0])
        wsend(name, rz, ry, dz, dy)

    def wait(name, first_axis, second_axis):
        if name in ("U", "B"):
            wwait(name, first_axis, second_axis)
        else:
            wwait(name, second_axis, first_axis)

    UP, DOWN = 1, -1

    def w_own_first(pair):
        for n in pair:
            send(n, 0, 0, (UP, 0))
            send(n, 0, 0, (DOWN, 0))

    def w_own_second(pair):
        for n in pair:
            send(n, 0, 0, (0, UP))
            send(n, 0, 0, (0, DOWN))

    def w_near(pair):
        for n in pair:
            wait(n, 1, 0)
            wait(n, -1, 0)

    def w_first_relay(pair):
        for n in pair:
            if n in ("G", "U"):
                send(n, 1, 0, (DOWN, 0))
            else:
                send(n, -1, 0, (UP, 0))

    def w_second(pair, r):
        for n in pair:
            if r == 2:
                wait(n, 2, 0)
            send(n, r, 0, (0, UP))
            send(n, r, 0, (0, DOWN))

    def w_second_relay(pair, r):
        for n in pair:
            if r in (0, -1):
                wait(n, r, -1)
                send(n, r, -1, (0, UP))
            else:
                wait(n, r, 1)
                send(n, r, 1, (0, DOWN))

    def w_second_rest(pair, r):
        for n in pair:
            wait(n, r, 1 if r in (0, -1) else -1)

    def w_last(pair):
        for n in pair:
            for r in (0, 1, -1, 2):
                wait(n, r, 2)

    n_pair = [0]
    pair_waits = []

    def plane(name, core, k):
        if name == "G":
            return wg.at[core, k]
        if name == "A":
            return wd.at[core, k, :, pl.ds(0, CUT)]
        if name == "U":
            return wu.at[core, :, k]
        return wd.at[core, :, k, pl.ds(CUT, CUT)]

    def share(name, r):
        k = n_pair[0]
        n_pair[0] += 1
        pos = at(y, r) if name in ("U", "B") else at(z, r)
        go(remote(plane(name, c, pos), plane(name, c, pos), pair_sem.at[0, k], pair_sem.at[1, k], c=o))
        got = plane(name, o, pos)
        pair_waits.append((name, remote(got, got, pair_sem.at[0, k], pair_sem.at[1, k], c=o)))

    w_own_first(("G", "U"))
    send("G", 0, 0, (0, UP))
    send("G", 0, 0, (0, DOWN))
    w_own_first(("B",))

    wo_copies = [
        go(remote(src, wo.at[c, rows], hp_sem.at[0, 4 + i], hp_sem.at[1, 4 + i], c=o))
        for i, (src, rows) in enumerate(((ws_in, pl.ds(0, 128)), (wl_in, pl.ds(128, 128))))
    ]

    for k in range(1, NB):
        first_pass(k)
    for cp in halos:
        cp.wait_recv()
    start = jnp.where(jnp.logical_and(z == 0, y == 0), 0.0, 1.0)
    cbuf[0:8, :] = halo[8:16, :].astype(F32) * start
    first_pass(0)

    state = fresh[0]
    total = decays[0]
    for k in range(1, NB):
        state = state * decays[k] + fresh[k]
        total = total * decays[k]

    st1[0, 0:128] = state.astype(BF16)
    st1[0, 128:136] = jnp.broadcast_to(total, (8, 256)).astype(BF16)
    for r in (1, 2, 3):
        go(remote(st1.at[0], st1.at[r], st_sem.at[0, r], st_sem.at[1, r], y=at(y, r)))
    send("U", 0, 0, (0, UP))
    send("U", 0, 0, (0, DOWN))

    mask = lax.broadcasted_iota(jnp.int32, (L, L), 0) >= lax.broadcasted_iota(jnp.int32, (L, L), 1)

    def weights_of(k, h):
        b = 8 * k + h
        diff = cols[:, b : b + 1] - rows[k][h : h + 1, :]
        return jnp.exp(jnp.where(mask, diff, -1e30))

    def second_pass(k):
        blk = pl.ds(k * L, L)
        s_s = dot_nt(conv_k[blk, 128:256], conv_k[blk, 0:128])
        s_l = dot_nt(conv_k[blk, 384:512], conv_k[blk, 256:384])
        d_s = drive[blk, 0:128]
        o_0 = dot((s_s * weights_of(k, 0)).astype(BF16), d_s)
        o_1 = dot((s_s * weights_of(k, 1)).astype(BF16), d_s)
        inner[blk, 0:128] = jnp.where(half, o_0, o_1)
        inner[blk, 128:256] = dot((s_l * weights_of(k, 2)).astype(BF16), drive[blk, 128:256])

    second_pass(0)
    second_pass(1)

    def slot_of(buf, me, other):
        return buf[rem(me - other + 4, 4)].astype(F32)

    for r in (1, 2, 3):
        remote(st1.at[0], st1.at[r], st_sem.at[0, r], st_sem.at[1, r]).wait_recv()
    inside = jnp.zeros((128, 256), F32)
    inside_d = jnp.ones((1, 256), F32)
    line = jnp.zeros((128, 256), F32)
    line_d = jnp.ones((1, 256), F32)
    for j in range(4):
        blob = slot_of(st1, y, j)
        s_j, d_j = blob[0:128], blob[128:129]
        line = line * d_j + s_j
        line_d = line_d * d_j
        inside = jnp.where(j < y, line, inside)
        inside_d = jnp.where(j < y, line_d, inside_d)
    st2[0, 0:128] = line.astype(BF16)
    st2[0, 128:136] = jnp.broadcast_to(line_d, (8, 256)).astype(BF16)
    for r in (1, 2, 3):
        go(remote(st2.at[0], st2.at[r], st_sem.at[2, r], st_sem.at[3, r], z=at(z, r)))

    w_near(("G", "U"))
    w_first_relay(("G", "U"))
    w_second(("G", "U"), 1)
    w_second(("G", "U"), -1)
    w_own_first(("A",))
    w_own_second(("A", "B"))

    for k in range(2, NB):
        second_pass(k)

    for r in (1, 2, 3):
        remote(st2.at[0], st2.at[r], st_sem.at[2, r], st_sem.at[3, r]).wait_recv()
    before = jnp.zeros((128, 256), F32)
    run = jnp.zeros((128, 256), F32)
    for j in range(4):
        blob = slot_of(st2, z, j)
        run = run * blob[128:129] + blob[0:128]
        before = jnp.where(j < z, run, before)
    carry = before * inside_d + inside

    for i in (3, 4):
        local[i].wait()

    for k in range(NB):
        blk = pl.ds(k * L, L)
        gr_s, gr_l = spread(grown, k, 0)
        h_in = carry.astype(BF16)
        o_s = inner[blk, 0:128] + dot(conv_k[blk, 128:256], h_in[:, 0:128]) * gr_s
        o_l = inner[blk, 128:256] + dot(conv_k[blk, 384:512], h_in[:, 128:256]) * gr_l
        carry = carry * decays[k] + fresh[k]
        o_s = o_s * silu(gin[blk, 0:128].astype(F32))
        o_l = o_l * silu(gin[blk, 128:256].astype(F32))
        q = o_s * o_s
        q_0 = jnp.sum(jnp.where(half, q, 0.0), axis=1, keepdims=True)
        q_1 = jnp.sum(jnp.where(half, 0.0, q), axis=1, keepdims=True)
        q_l = jnp.sum(o_l * o_l, axis=1, keepdims=True)
        sc_0 = lax.rsqrt(q_0 * (1.0 / 64) + head_eps)
        sc_1 = lax.rsqrt(q_1 * (1.0 / 64) + head_eps)
        sc_l = lax.rsqrt(q_l * (1.0 / 128) + head_eps)
        heads[blk, 0:128] = (o_s * jnp.where(half, sc_0, sc_1) * gain_s[...]).astype(BF16)
        heads[blk, 128:256] = (o_l * sc_l * gain_l[...]).astype(BF16)

    def rows_of(b, core):
        return pl.ds(pl.multiple_of((2 * b + core) * R, 16), R)

    for b in range(4):
        go(remote(heads.at[rows_of(b, o)], hpart.at[b], hp_sem.at[0, b], hp_sem.at[1, b], c=o))
    for b in range(4):
        lhs[b] = heads[rows_of(b, c), :]
    for i in (6, 7):
        local[i].wait()
    own_rows = lhs[...].reshape(4 * R, 256)
    for cp in wo_copies:
        cp.wait_recv()
    for b in range(4):
        remote(hpart.at[b], hpart.at[b], hp_sem.at[0, b], hp_sem.at[1, b]).wait_recv()
    part_rows = hpart[...].reshape(4 * R, 256)

    x1, x2, x3 = at(x, 1), at(x, 2), at(x, 3)

    class Sum:
        def __init__(self, parts, from_left, from_right, sems):
            self.parts, self.left, self.right, self.sems = parts, from_left, from_right, sems

        def to_right(self, slot, block, h):
            go(remote(self.parts.at[block, h], self.left.at[slot], self.sems.at[0, slot], self.sems.at[1, slot], x=x1))

        def to_left(self, slot, block, h):
            go(remote(self.parts.at[block, h], self.right.at[slot], self.sems.at[2, slot], self.sems.at[3, slot], x=x3))

        def wait_left(self, slot):
            remote(self.left.at[slot], self.left.at[slot], self.sems.at[0, slot], self.sems.at[1, slot]).wait_recv()

        def wait_right(self, slot):
            remote(self.right.at[slot], self.right.at[slot], self.sems.at[2, slot], self.sems.at[3, slot]).wait_recv()

        def after_quarter(self, q):
            if q < 2:
                self.to_right(q, x2, q)
                self.to_left(q + 2, x3, q)
            else:
                self.to_left(q - 2, x2, q)
                self.to_right(q, x1, q)

        def merge(self, i):
            p = self.parts
            self.wait_left(i)
            p[x1, i] = (p[x1, i].astype(F32) + self.left[i].astype(F32)).astype(BF16)
            self.to_right(4 + i, x1, i)
            self.wait_right(i)
            p[x3, 2 + i] = (p[x3, 2 + i].astype(F32) + self.right[i].astype(F32)).astype(BF16)
            self.to_left(4 + i, x3, 2 + i)

        def result(self, q):
            a, b = (4 + q, 2 + q) if q < 2 else (q, 2 + q)
            self.wait_left(a)
            self.wait_right(b)
            return self.parts[x, q].astype(F32) + self.left[a].astype(F32) + self.right[b].astype(F32)

    mixed = Sum(psend, rp, rm, rs_sem)
    for q in ORDER:
        for e in range(2):
            n = pl.ds(q * Q + e * 256, 256)
            acc = dot(own_rows, wo[c, :, n]) + dot(part_rows, wo[o, :, n])
            psend[:, q, :, e * 256 : (e + 1) * 256] = acc.reshape(4, R, 256).astype(BF16)
        mixed.after_quarter(q)
    w_second(("G", "U"), 2)
    w_second_relay(("G", "U"), 0)
    w_near(("B",))
    w_first_relay(("B",))
    mixed.merge(0)
    w_second_relay(("G", "U"), 1)
    w_second_relay(("G", "U"), -1)
    w_near(("A",))
    w_first_relay(("A",))
    mixed.merge(1)
    local[5].wait()
    sums = [mixed.result(q) for q in (2, 3, 0, 1)]
    lo = jnp.concatenate(sums[2:], axis=1)
    hi = jnp.concatenate(sums[:2], axis=1)
    mid_lo = (resv[:, 0:H].astype(F32) + lo).astype(BF16)
    mid_hi = (resv[:, H:DM].astype(F32) + hi).astype(BF16)
    midv[0] = mid_lo
    midv[1] = mid_hi
    f_lo, f_hi = mid_lo.astype(F32), mid_hi.astype(F32)
    square = jnp.sum(f_lo * f_lo, axis=1, keepdims=True) + jnp.sum(f_hi * f_hi, axis=1, keepdims=True)
    scale = lax.rsqrt(square * (1.0 / DM) + row_eps)
    ag[x, 0] = (f_lo * scale * gain_n[:, 0:H]).astype(BF16)
    ag[x, 1] = (f_hi * scale * gain_n[:, H:DM]).astype(BF16)

    def ag_right(slot, block, h):
        go(remote(ag.at[block, h], ag.at[block, h], ag_sem.at[0, slot], ag_sem.at[1, slot], x=x1))

    def ag_left(slot, block, h):
        go(remote(ag.at[block, h], ag.at[block, h], ag_sem.at[2, slot], ag_sem.at[3, slot], x=x3))

    def ag_wait(side, slot, block, h):
        remote(ag.at[block, h], ag.at[block, h], ag_sem.at[0, slot], ag_sem.at[side, slot]).wait_recv()

    ag_right(0, x, 0)
    ag_left(0, x, 1)
    ag_right(1, x, 1)
    ag_left(1, x, 0)

    w_second_relay(("G", "U"), 2)
    w_second(("A", "B"), 1)
    w_second(("A", "B"), -1)
    w_second(("A", "B"), 2)
    ag_wait(1, 0, x3, 0)
    ag_right(2, x3, 0)
    ag_wait(3, 0, x1, 1)
    ag_left(2, x1, 1)

    for i in (8, 9, 10):
        local[i].wait()
    w_second_relay(("A", "B"), 0)
    w_second_relay(("A", "B"), 1)
    w_second_rest(("G", "U"), 0)
    for r in (1, -1, 2):
        w_second_rest(("G", "U"), r)
    for n in ("G", "U"):
        share(n, 0)
        share(n, 1)
        share(n, -1)
    w_second_relay(("A", "B"), -1)
    w_second_relay(("A", "B"), 2)
    w_last(("G", "U"))
    for n in ("G", "U"):
        share(n, 2)
    ag_wait(1, 1, x3, 1)
    ag_wait(3, 1, x1, 0)
    ag_wait(1, 2, x2, 0)
    ag_wait(3, 2, x2, 1)

    def lined_up(w, core, h, n0, n):
        parts = [w[core, 2 * h + j // 4, j % 4, n0 : n0 + n, :] for j in range(8)]
        return jnp.concatenate(parts, axis=1)

    def expand(core):
        for n0, n in ((0, 256), (256, 256), (512, 192)):
            gate = up = None
            for h in range(2):
                a = ag[:, h].reshape(4 * R, H)
                w_gate = lined_up(wg, core, h, n0, n)
                w_up = lined_up(wu, core, h, n0, n)
                gate = dot_nt(a, w_gate) if gate is None else gate + dot_nt(a, w_gate)
                up = dot_nt(a, w_up) if up is None else up + dot_nt(a, w_up)
            hid[core, :, n0 : n0 + n] = (silu(gate) * up).astype(BF16)

    expand(c)
    for name, w in pair_waits:
        if name in ("G", "U"):
            w.wait_recv()
    expand(o)

    for r in (0, 1, -1, 2):
        w_second_rest(("A", "B"), r)
    for n in ("A", "B"):
        share(n, 0)
        share(n, 1)
        share(n, -1)
    w_last(("A", "B"))
    for n in ("A", "B"):
        share(n, 2)
    for name, w in pair_waits:
        if name in ("A", "B"):
            w.wait_recv()

    down = Sum(psend2, rp2, rm2, rs2_sem)
    for q in ORDER:
        for e in range(2):
            acc = None
            for cc in range(2):
                w_down = jnp.concatenate([wd[cc, q, 2 * e], wd[cc, q, 2 * e + 1]], axis=1)
                acc = dot(hid[cc], w_down) if acc is None else acc + dot(hid[cc], w_down)
            psend2[:, q, :, e * 256 : (e + 1) * 256] = acc.reshape(4, R, 256).astype(BF16)
        down.after_quarter(q)
    down.merge(0)
    down.merge(1)
    sums = [down.result(q) for q in (2, 3, 0, 1)]
    lo = jnp.concatenate(sums[2:], axis=1)
    hi = jnp.concatenate(sums[:2], axis=1)
    out[:, 0:H] = (midv[0].astype(F32) + lo).astype(BF16)
    out[:, H:DM] = (midv[1].astype(F32) + hi).astype(BF16)

    for cp in pending:
        cp.wait_send()


def on_device(
    residual, small_value_inputs, large_value_inputs, small_gate_inputs, large_gate_inputs,
    state_projections, small_step_inputs, large_step_inputs, small_decay_offsets,
    large_decay_offsets, small_decay_rates, large_decay_rates, small_filter_taps,
    large_filter_taps, state_filter_taps, small_head_gains, large_head_gains,
    small_output_projection, large_output_projection, channel_norm_gain, gate_matrix,
    up_matrix, down_matrix,
):
    flat = state_projections.reshape(T, 512)

    anywhere = pl.BlockSpec(memory_space=pl.ANY)
    vmem = pl.BlockSpec(memory_space=pltpu.VMEM)
    smem = pl.BlockSpec(memory_space=pltpu.SMEM)
    dma = pltpu.SemaphoreType.DMA
    V = pltpu.VMEM
    return pl.pallas_call(
        kernel,
        out_shape=jax.ShapeDtypeStruct((R, DM), BF16),
        in_specs=[anywhere] * 11 + [vmem] * 4 + [smem] * 2 + [vmem] * 6,
        out_specs=vmem,
        scratch_shapes=[
            V((T, 768), BF16),
            V((T, 256), BF16),
            V((R, DM), BF16),
            V((16, 768), BF16),
            V((T + 8, 768), F32),
            V((T, 512), BF16),
            V((T, 256), BF16),
            V((NB, 128, 256), F32),
            V((T, 256), F32),
            V((T, 256), BF16),
            V((4, R, 256), BF16),
            V((4, R, 256), BF16),
            V((2, 256, DM), BF16),
            V((2, 4, 4, FD, KROWS), BF16),
            V((2, 4, 4, FD, KROWS), BF16),
            V((2, 4, 4, FD, KROWS), BF16),
            V((4, 136, 256), BF16),
            V((4, 136, 256), BF16),
            V((4, 4, R, Q), BF16),
            V((6, R, Q), BF16),
            V((6, R, Q), BF16),
            V((4, 2, R, H), BF16),
            V((2, 4 * R, FD), BF16),
            V((4, 4, R, Q), BF16),
            V((6, R, Q), BF16),
            V((6, R, Q), BF16),
            V((2, R, H), BF16),
            dma((11,)),
            dma((2, 3)),
            dma((60,)),
            dma((4, 4, 4)),
            dma((2, 16)),
            dma((4, 4)),
            dma((2, 6)),
            dma((4, 6)),
            dma((4, 3)),
            dma((4, 6)),
        ],
        compiler_params=pltpu.CompilerParams(
            collective_id=0, has_side_effects=True, vmem_limit_bytes=60 * 1024 * 1024
        ),
    )(
        residual, small_value_inputs, large_value_inputs, small_gate_inputs, large_gate_inputs,
        flat, small_output_projection, large_output_projection, gate_matrix.T, up_matrix.T, down_matrix,
        small_step_inputs.T, large_step_inputs.T, small_decay_offsets.T, large_decay_offsets.T,
        small_decay_rates, large_decay_rates, small_filter_taps, large_filter_taps, state_filter_taps,
        small_head_gains.reshape(1, 128), large_head_gains.reshape(1, 128),
        channel_norm_gain.reshape(1, DM),
    )


def solution(mesh):
    split = Mesh(mesh.devices.reshape(4, 4, 4, 2), ("z", "y", "x", "c"))
    in_specs = (
        P(SP_TP, None),
        P(SP, TP),
        P(SP, TP),
        P(SP, TP),
        P(SP, TP),
        P(SP, None, None),
        P(SP, TP),
        P(SP, TP),
        P(SP, TP),
        P(SP, TP),
        P(TP),
        P(TP),
        P(None, TP),
        P(None, TP),
        P(),
        P(TP),
        P(TP),
        P(TP, None),
        P(TP, None),
        P(),
        P(SP, TP),
        P(SP, TP),
        P(TP, SP),
    )
    return jax.shard_map(
        on_device, mesh=split, in_specs=in_specs, out_specs=P(SP_TP, None), check_vma=False
    )
```

```python
import jax
import jax.numpy as jnp
from jax import lax
from jax.experimental import pallas as pl
from jax.experimental.pallas import tpu as pltpu
from jax.sharding import Mesh
from jax.sharding import PartitionSpec as P

F32 = jnp.float32
BF16 = jnp.bfloat16
SP = ("z", "y")
TP = ("x", "c")
SP_TP = ("z", "y", "x", "c")

T = 640
L = 128
NB = T // L
R = 80
FD = 704
DM = 2048
H = 1024
KROWS = 128
CUT = 352
Q = 512
ORDER = (0, 2, 1, 3)
STEPS = (0, 1, -1, 2)
COLUMNS = (
    ((0, 0), (0, 1), (1, 0), (0, -1)),
    ((-1, 0), (1, 1), (0, 2), (1, -1)),
    ((2, 0), (-1, 1), (-1, -1), (2, 1)),
    ((1, 2), (2, -1), (-1, 2), (2, 2)),
)
SENDS = (
    ((0, 0, 0, 0, 1), (0, 0, 0, 0, -1), (1, 0, 0, 0, 1), (1, 0, 0, 0, -1), (0, 0, 0, 1, 1), (0, 0, 0, 1, -1)),
    ((1, 0, 0, 1, -1), (1, 0, 0, 1, 1)),
    ((0, 1, 0, 0, -1),),
    ((1, 1, 0, 0, -1), (1, 1, 0, 1, 1), (0, 1, 0, 1, 1)),
    ((1, 1, 0, 1, -1), (0, 1, 0, 1, -1), (1, -1, 0, 1, 1), (0, -1, 0, 1, 1)),
    ((1, -1, 0, 1, -1), (0, -1, 0, 1, -1)),
    ((1, 2, 0, 1, 1), (0, 2, 0, 1, 1), (1, 2, 0, 1, -1), (0, 2, 0, 1, -1), (1, 0, -1, 1, 1)),
    ((0, 0, -1, 1, 1), (1, 1, 1, 1, -1), (0, 1, 1, 1, -1)),
    ((1, -1, -1, 1, 1), (0, -1, -1, 1, 1)),
    ((1, 2, -1, 1, 1), (0, 2, -1, 1, 1), (2, 0, 0, 0, -1), (3, 0, 0, 0, -1), (3, 0, 0, 1, -1)),
    ((2, 0, 0, 0, 1), (3, 0, 0, 0, 1), (2, 0, 0, 1, -1), (3, 0, 0, 1, 1), (2, 0, 0, 1, 1)),
    ((2, 1, 0, 0, -1), (3, 1, 0, 0, -1), (3, 1, 0, 1, 1), (2, 1, 0, 1, -1), (3, 1, 0, 1, -1), (2, 1, 0, 1, 1), (3, 0, 1, 1, -1)),
    ((2, -1, 0, 1, -1), (2, -1, 0, 1, 1), (2, 0, 1, 1, -1)),
    ((3, 2, 0, 1, 1), (3, 2, 0, 1, -1), (2, 2, 0, 1, 1), (2, 2, 0, 1, -1), (3, -1, 0, 1, 1), (3, -1, 0, 1, -1)),
    ((2, 1, -1, 1, 1), (3, 1, -1, 1, 1)),
    ((3, 2, 1, 1, -1), (2, -1, -1, 1, 1)),
    ((2, 2, -1, 1, 1), (3, -1, -1, 1, 1)),
    (),
)
SHARES = (
    ((0, 0, 0), (1, 0, 0), (2, 0, 0), (3, 0, 0)),
    (),
    ((0, -1, 0), (0, 1, 0), (1, -1, 0), (1, 1, 0)),
    ((0, 0, -1), (0, 0, 1)),
    (),
    ((1, 0, 1), (1, 0, -1)),
    ((0, 2, 0), (1, 2, 0)),
    ((1, 1, -1), (0, 1, -1), (1, 1, 1), (0, 1, 1)),
    ((1, -1, -1), (0, -1, -1), (1, -1, 1)),
    ((0, -1, 1), (1, 2, -1), (0, 2, -1)),
    ((1, 2, 1), (0, 2, 1), (1, 0, 2), (0, 0, 2)),
    ((1, 1, 2), (0, 1, 2), (1, -1, 2), (2, 1, 0), (0, -1, 2), (3, 1, 0), (3, 0, 1)),
    ((2, 0, 1), (1, 2, 2), (0, 2, 2), (2, -1, 0)),
    ((3, -1, 0), (3, 0, -1), (2, 2, 0), (3, 2, 0), (2, 0, -1)),
    ((3, 1, -1), (2, 1, 1), (3, 1, 1), (2, 1, -1)),
    ((3, 0, 2), (2, -1, 1), (2, -1, -1), (2, 0, 2), (3, 2, -1), (3, 2, 1)),
    ((2, 2, -1), (2, 2, 1), (3, -1, -1), (3, -1, 1), (2, 1, 2)),
    ((3, 1, 2), (3, 2, 2), (2, -1, 2), (2, 2, 2), (3, -1, 2)),
)

head_eps = 1e-05
row_eps = 1e-06


def silu(x):
    return x / (1.0 + jnp.exp(-x))


def dot(a, b):
    return jnp.dot(a, b, preferred_element_type=F32)


def dot_nt(a, b):
    return lax.dot_general(a, b, (((1,), (1,)), ((), ())), preferred_element_type=F32)


def dot_tn(a, b):
    return lax.dot_general(a, b, (((0,), (0,)), ((), ())), preferred_element_type=F32)


def kernel(
    res_in, vs_in, vl_in, gs_in, gl_in, sp_in, ws_in, wl_in, g_in, u_in, d_in,
    steps_s, steps_l, offs_s, offs_l, rates_s, rates_l, taps_s, taps_l, taps_m, gain_s, gain_l, gain_n,
    out,
    xin, gin, resv, halo, cbuf, conv_k, drive, fresh, inner, heads, hpart, lhs,
    wo, wg, wu, wd, st1, st2, psend, rp, rm, ag, hid, psend2, rp2, rm2, midv,
    loc_sem, halo_sem, w_send, w_recv, pair_sem, st_sem, hp_sem, rs_sem, ag_sem, rs2_sem,
):
    z, y, x, c = (lax.axis_index(n) for n in ("z", "y", "x", "c"))
    rem = lax.rem
    o = 1 - c

    def at(base, by):
        return rem(base + (by % 4), 4)

    nxt = {"z": rem(z + lax.div(y + 1, 4), 4), "y": rem(y + 1, 4)}
    prv = {"z": rem(z + 3 + lax.div(y + 3, 4), 4), "y": rem(y + 3, 4)}

    def there(**kw):
        base = {"z": z, "y": y, "x": x, "c": c}
        base.update(kw)
        return (base["z"], base["y"], base["x"], base["c"])

    def remote(src, dst, send, recv, **kw):
        return pltpu.make_async_remote_copy(
            src_ref=src, dst_ref=dst, send_sem=send, recv_sem=recv,
            device_id=there(**kw), device_id_type=pl.DeviceIdType.MESH,
        )

    pending = []

    def go(cp):
        cp.start()
        pending.append(cp)
        return cp

    local = [
        (vs_in, xin.at[:, pl.ds(0, 128)]),
        (vl_in, xin.at[:, pl.ds(128, 128)]),
        (sp_in, xin.at[:, pl.ds(256, 512)]),
        (gs_in, gin.at[:, pl.ds(0, 128)]),
        (gl_in, gin.at[:, pl.ds(128, 128)]),
        (res_in, resv),
        (ws_in, wo.at[c, pl.ds(0, 128)]),
        (wl_in, wo.at[c, pl.ds(128, 128)]),
        (g_in, wg.at[c, z, y]),
        (u_in, wu.at[c, z, y]),
        (d_in, wd.at[c, z, y]),
    ]
    local = [pltpu.make_async_copy(a, b, loc_sem.at[i]) for i, (a, b) in enumerate(local)]
    for cp in local:
        cp.start()

    barrier = pltpu.get_barrier_semaphore()
    peers = [
        dict(c=o), dict(x=at(x, 1)), dict(x=at(x, 3)),
        dict(y=at(y, 1)), dict(y=at(y, 2)), dict(y=at(y, 3)),
        dict(z=at(z, 1)), dict(z=at(z, 2)), dict(z=at(z, 3)),
        nxt, prv,
    ]
    for p in peers:
        pl.semaphore_signal(barrier, inc=1, device_id=there(**p), device_id_type=pl.DeviceIdType.MESH)
    lane = lax.broadcasted_iota(jnp.int32, (8, L), 1)
    rows = []
    both = []
    row8 = lax.broadcasted_iota(jnp.int32, (8, L), 0)
    raw_steps = jnp.concatenate([steps_s[...].astype(F32), steps_l[...].astype(F32)], axis=0)
    softened = jnp.maximum(raw_steps, 0.0) + jnp.log1p(jnp.exp(-jnp.abs(raw_steps)))
    head = lax.broadcasted_iota(jnp.int32, (3, T), 0)
    rate = jnp.where(head == 0, rates_s[0], jnp.where(head == 1, rates_s[1], rates_l[0]))
    offsets = jnp.concatenate([offs_s[...], offs_l[...]], axis=0)
    meta = jnp.concatenate(
        [offsets - jnp.exp(rate) * softened, softened, jnp.zeros((2, T), F32)], axis=0
    )
    for k in range(NB):
        raw = meta[:, k * L : (k + 1) * L]
        acc = raw
        for sft in (1, 2, 4, 8, 16, 32, 64):
            acc = acc + jnp.where(lane >= sft, pltpu.roll(acc, sft, 1), 0.0)
        rows.append(acc)
        both.append(jnp.where(row8 < 3, acc, raw))
    both.append(jnp.zeros((L - 8 * NB, L), F32))
    cols = jnp.concatenate(both, axis=0).T
    grown = jnp.exp(cols)
    shrunk = jnp.exp(cols[L - 1 : L, :] - cols)

    half = lax.broadcasted_iota(jnp.int32, (L, L), 1) < 64
    half1 = lax.broadcasted_iota(jnp.int32, (1, L), 1) < 64

    def spread(m, k, off):
        b = 8 * k + off
        small = jnp.where(half, m[:, b : b + 1], m[:, b + 1 : b + 2])
        large = jnp.broadcast_to(m[:, b + 2 : b + 3], (L, L))
        return small, large

    def block_decay(k):
        b = 8 * k
        e = grown[L - 1 : L]
        small = jnp.where(half1, e[:, b : b + 1], e[:, b + 1 : b + 2])
        large = jnp.broadcast_to(e[:, b + 2 : b + 3], (1, L))
        return jnp.concatenate([small, large], axis=1)

    tap_rows = []
    for j in range(4):
        m = taps_m[j].astype(F32)
        tap_rows.append(
            [taps_s[j : j + 1].astype(F32), taps_l[j : j + 1].astype(F32)]
            + [m[i : i + 1] for i in range(4)]
        )

    def conv(k, g):
        total = None
        for j in range(4):
            part = tap_rows[j][g] * cbuf[k * L + 5 + j : k * L + 5 + j + L, g * 128 : g * 128 + 128]
            total = part if total is None else total + part
        return silu(total)

    for i in range(3):
        local[i].wait()
    for k in range(NB):
        cbuf[8 + k * L : 8 + (k + 1) * L, :] = xin[k * L : (k + 1) * L, :].astype(F32)
    decays = [block_decay(k) for k in range(NB)]

    def first_pass(k, kind):
        dt, sh = spread(cols, k, 3)[kind], spread(shrunk, k, 0)[kind]
        blk, at_kind = pl.ds(k * L, L), pl.ds(kind * 128, 128)
        d = conv(k, kind) * dt
        drive[blk, at_kind] = d.astype(BF16)
        key = conv(k, 2 + 2 * kind).astype(BF16)
        conv_k[blk, 256 * kind : 256 * kind + 128] = key
        conv_k[blk, 256 * kind + 128 : 256 * kind + 256] = conv(k, 3 + 2 * kind).astype(BF16)
        fresh[k, :, at_kind] = dot_tn(key, (d * sh).astype(BF16))

    pl.semaphore_wait(barrier, len(peers))

    tail = pl.ds(T - 16, 16)
    halos = [
        go(remote(src.at[tail], halo.at[:, cols], halo_sem.at[0, i], halo_sem.at[1, i], **nxt))
        for i, (src, cols) in enumerate(
            ((vs_in, pl.ds(0, 128)), (vl_in, pl.ds(128, 128)), (sp_in, pl.ds(256, 512)))
        )
    ]

    names = ("G", "U", "A", "B")
    own_src = {
        "G": g_in, "U": u_in,
        "A": d_in.at[pl.ds(0, CUT)], "B": d_in.at[pl.ds(CUT, CUT)],
    }

    def unit(name, rz, ry, core):
        zz, yy = at(z, rz), at(y, ry)
        if name == "G":
            return wg.at[core, zz, yy]
        if name == "U":
            return wu.at[core, zz, yy]
        rows = pl.ds(0, CUT) if name == "A" else pl.ds(CUT, CUT)
        return wd.at[core, zz, yy, rows]

    def place(name, f, s):
        return (f, s) if name in ("U", "B") else (s, f)

    def source(name, f, s):
        return own_src[name] if (f, s) == (0, 0) else unit(name, *place(name, f, s), c)

    def w_sem(name, rz, ry):
        return w_recv.at[names.index(name), rz % 4, ry % 4]

    n_sent = [0]
    here = {(n, 0, 0) for n in names}

    def w_wait(name, f, s):
        if (name, f, s) not in here:
            here.add((name, f, s))
            ref = unit(name, *place(name, f, s), c)
            remote(ref, ref, w_send.at[0], w_sem(name, *place(name, f, s))).wait_recv()

    def w_go(name, f, s, second, step):
        w_wait(name, f, s)
        dz, dy = place(name, 0, step) if second else place(name, step, 0)
        rz, ry = place(name, f, s)
        k = n_sent[0]
        n_sent[0] += 1
        go(remote(
            source(name, f, s), unit(name, rz, ry, c), w_send.at[k], w_sem(name, rz - dz, ry - dy),
            z=at(z, dz), y=at(y, dy),
        ))

    pair_index = {}

    def share(name, f, s):
        w_wait(name, f, s)
        k = pair_index.setdefault((name, f, s), len(pair_index))
        go(remote(
            source(name, f, s), unit(name, *place(name, f, s), c),
            pair_sem.at[0, k], pair_sem.at[1, k], c=o,
        ))

    def pair_wait(name, f, s):
        k = pair_index[(name, f, s)]
        ref = unit(name, *place(name, f, s), o)
        remote(ref, ref, pair_sem.at[0, k], pair_sem.at[1, k], c=o).wait_recv()

    def pump(i):
        for n, f, s, second, step in SENDS[i]:
            w_go(names[n], f, s, second, step)
        for n, f, s in SHARES[i]:
            share(names[n], f, s)

    pump(0)

    wo_copies = [
        go(remote(src, wo.at[c, rows], hp_sem.at[0, 4 + i], hp_sem.at[1, 4 + i], c=o))
        for i, (src, rows) in enumerate(((ws_in, pl.ds(0, 128)), (wl_in, pl.ds(128, 128))))
    ]

    for kind in range(2):
        for k in range(1, NB):
            first_pass(k, kind)
    for cp in halos:
        cp.wait_recv()
    start = jnp.where(jnp.logical_and(z == 0, y == 0), 0.0, 1.0)
    cbuf[0:8, :] = halo[8:16, :].astype(F32) * start

    def state_out(buf, kind, state, total, stage, **axis):
        buf[kind, 0, 0:128] = state.astype(BF16)
        buf[kind, 0, 128:136] = jnp.broadcast_to(total, (8, 128)).astype(BF16)
        for r in (1, 2, 3):
            ((name, me),) = axis.items()
            go(remote(
                buf.at[kind, 0], buf.at[kind, r],
                st_sem.at[2 * stage, kind, r], st_sem.at[2 * stage + 1, kind, r],
                **{name: at(me, r)},
            ))

    def states_in(buf, kind, stage):
        for r in (1, 2, 3):
            remote(
                buf.at[kind, 0], buf.at[kind, r],
                st_sem.at[2 * stage, kind, r], st_sem.at[2 * stage + 1, kind, r],
            ).wait_recv()

    def chained(buf, kind, me):
        line, line_d = jnp.zeros((128, 128), F32), jnp.ones((1, 128), F32)
        before, before_d = line, line_d
        for j in range(4):
            blob = buf[kind, rem(me - j + 4, 4)].astype(F32)
            line = line * blob[128:129] + blob[0:128]
            line_d = line_d * blob[128:129]
            before = jnp.where(j < me, line, before)
            before_d = jnp.where(j < me, line_d, before_d)
        return before, before_d, line, line_d

    for kind in range(2):
        first_pass(0, kind)
        own = slice(kind * 128, kind * 128 + 128)
        state, total = fresh[0, :, own], decays[0][:, own]
        for k in range(1, NB):
            state = state * decays[k][:, own] + fresh[k, :, own]
            total = total * decays[k][:, own]
        state_out(st1, kind, state, total, 0, y=y)
    pump(1)

    mask = lax.broadcasted_iota(jnp.int32, (L, L), 0) >= lax.broadcasted_iota(jnp.int32, (L, L), 1)

    def weights_of(k, h):
        b = 8 * k + h
        diff = cols[:, b : b + 1] - rows[k][h : h + 1, :]
        return jnp.exp(jnp.where(mask, diff, -1e30))

    def second_pass(k):
        blk = pl.ds(k * L, L)
        s_s = dot_nt(conv_k[blk, 128:256], conv_k[blk, 0:128])
        s_l = dot_nt(conv_k[blk, 384:512], conv_k[blk, 256:384])
        d_s = drive[blk, 0:128]
        o_0 = dot((s_s * weights_of(k, 0)).astype(BF16), d_s)
        o_1 = dot((s_s * weights_of(k, 1)).astype(BF16), d_s)
        inner[blk, 0:128] = jnp.where(half, o_0, o_1)
        inner[blk, 128:256] = dot((s_l * weights_of(k, 2)).astype(BF16), drive[blk, 128:256])

    for k in range(NB):
        second_pass(k)
    inside = []
    for kind in range(2):
        states_in(st1, kind, 0)
        before, before_d, line, line_d = chained(st1, kind, y)
        inside.append((before, before_d))
        state_out(st2, kind, line, line_d, 1, z=z)
        if kind == 0:
            pump(2)
    pump(3)

    for i in (3, 4):
        local[i].wait()

    def third_pass(k, kind, carry):
        blk, cols_k = pl.ds(k * L, L), pl.ds(kind * 128, 128)
        own = slice(kind * 128, kind * 128 + 128)
        reads = conv_k[blk, 256 * kind + 128 : 256 * kind + 256]
        out_k = inner[blk, cols_k] + dot(reads, carry.astype(BF16)) * spread(grown, k, 0)[kind]
        carry = carry * decays[k][:, own] + fresh[k, :, own]
        out_k = out_k * silu(gin[blk, cols_k].astype(F32))
        sq = out_k * out_k
        if kind == 0:
            sq_0 = jnp.sum(jnp.where(half, sq, 0.0), axis=1, keepdims=True)
            sq_1 = jnp.sum(jnp.where(half, 0.0, sq), axis=1, keepdims=True)
            mean = jnp.where(half, sq_0, sq_1) * (1.0 / 64)
            gain = gain_s[...]
        else:
            mean = jnp.sum(sq, axis=1, keepdims=True) * (1.0 / 128)
            gain = gain_l[...]
        heads[blk, cols_k] = (out_k * lax.rsqrt(mean + head_eps) * gain).astype(BF16)
        return carry

    for kind in range(2):
        states_in(st2, kind, 1)
        before = chained(st2, kind, z)[0]
        carry = before * inside[kind][1] + inside[kind][0]
        for k in range(NB):
            carry = third_pass(k, kind, carry)
        if kind == 0:
            pump(4)

    def rows_of(b, core):
        return pl.ds(pl.multiple_of((2 * b + core) * R, 16), R)

    for b in range(4):
        go(remote(heads.at[rows_of(b, o)], hpart.at[b], hp_sem.at[0, b], hp_sem.at[1, b], c=o))
    for b in range(4):
        lhs[b] = heads[rows_of(b, c), :]
    for i in (6, 7):
        local[i].wait()
    own_rows = lhs[...].reshape(4 * R, 256)
    for cp in wo_copies:
        cp.wait_recv()
    pump(5)
    for b in range(4):
        remote(hpart.at[b], hpart.at[b], hp_sem.at[0, b], hp_sem.at[1, b]).wait_recv()
    part_rows = hpart[...].reshape(4 * R, 256)

    x1, x2, x3 = at(x, 1), at(x, 2), at(x, 3)

    class Sum:
        def __init__(self, parts, from_left, from_right, sems):
            self.parts, self.left, self.right, self.sems = parts, from_left, from_right, sems

        def to_right(self, slot, block, h):
            go(remote(self.parts.at[block, h], self.left.at[slot], self.sems.at[0, slot], self.sems.at[1, slot], x=x1))

        def to_left(self, slot, block, h):
            go(remote(self.parts.at[block, h], self.right.at[slot], self.sems.at[2, slot], self.sems.at[3, slot], x=x3))

        def wait_left(self, slot):
            remote(self.left.at[slot], self.left.at[slot], self.sems.at[0, slot], self.sems.at[1, slot]).wait_recv()

        def wait_right(self, slot):
            remote(self.right.at[slot], self.right.at[slot], self.sems.at[2, slot], self.sems.at[3, slot]).wait_recv()

        def after_quarter(self, q):
            if q < 2:
                self.to_right(q, x2, q)
                self.to_left(q + 2, x3, q)
            else:
                self.to_left(q - 2, x2, q)
                self.to_right(q, x1, q)

        def merge(self, i):
            p = self.parts
            self.wait_left(i)
            p[x1, i] = (p[x1, i].astype(F32) + self.left[i].astype(F32)).astype(BF16)
            self.to_right(4 + i, x1, i)
            self.wait_right(i)
            p[x3, 2 + i] = (p[x3, 2 + i].astype(F32) + self.right[i].astype(F32)).astype(BF16)
            self.to_left(4 + i, x3, 2 + i)

        def result(self, q):
            a, b = (4 + q, 2 + q) if q < 2 else (q, 2 + q)
            self.wait_left(a)
            self.wait_right(b)
            return self.parts[x, q].astype(F32) + self.left[a].astype(F32) + self.right[b].astype(F32)

    mixed = Sum(psend, rp, rm, rs_sem)
    for q in ORDER:
        for e in range(2):
            n = pl.ds(q * Q + e * 256, 256)
            acc = dot(own_rows, wo[c, :, n]) + dot(part_rows, wo[o, :, n])
            psend[:, q, :, e * 256 : (e + 1) * 256] = acc.reshape(4, R, 256).astype(BF16)
        mixed.after_quarter(q)
    pump(6)
    mixed.merge(0)
    pump(7)
    mixed.merge(1)
    pump(8)
    local[5].wait()
    sums = {q: mixed.result(q) for q in (2, 3)}
    pump(9)
    sums.update({q: mixed.result(q) for q in (0, 1)})
    lo = jnp.concatenate([sums[0], sums[1]], axis=1)
    hi = jnp.concatenate([sums[2], sums[3]], axis=1)
    mid_lo = (resv[:, 0:H].astype(F32) + lo).astype(BF16)
    mid_hi = (resv[:, H:DM].astype(F32) + hi).astype(BF16)
    midv[:, 0:H] = mid_lo
    midv[:, H:DM] = mid_hi
    f_lo, f_hi = mid_lo.astype(F32), mid_hi.astype(F32)
    square = jnp.sum(f_lo * f_lo, axis=1, keepdims=True) + jnp.sum(f_hi * f_hi, axis=1, keepdims=True)
    scale = lax.rsqrt(square * (1.0 / DM) + row_eps)
    ag[x, 0] = (f_lo * scale * gain_n[:, 0:H]).astype(BF16)
    ag[x, 1] = (f_hi * scale * gain_n[:, H:DM]).astype(BF16)

    def ag_right(slot, block, h):
        go(remote(ag.at[block, h], ag.at[block, h], ag_sem.at[0, slot], ag_sem.at[1, slot], x=x1))

    def ag_left(slot, block, h):
        go(remote(ag.at[block, h], ag.at[block, h], ag_sem.at[2, slot], ag_sem.at[3, slot], x=x3))

    def ag_wait(side, slot, block, h):
        remote(ag.at[block, h], ag.at[block, h], ag_sem.at[0, slot], ag_sem.at[side, slot]).wait_recv()

    ag_right(0, x, 0)
    ag_left(0, x, 1)
    ag_right(1, x, 1)
    ag_left(1, x, 0)

    pump(10)
    ag_wait(1, 0, x3, 0)
    ag_right(2, x3, 0)
    ag_wait(3, 0, x1, 1)
    ag_left(2, x1, 1)
    pump(11)
    ag_wait(1, 1, x3, 1)
    ag_wait(3, 1, x1, 0)
    pump(12)
    ag_wait(1, 2, x2, 0)
    ag_wait(3, 2, x2, 1)
    pump(13)
    for i in (8, 9, 10):
        local[i].wait()
    def lined_up(w, core, h, n0, n):
        parts = [w[core, 2 * h + j // 4, j % 4, n0 : n0 + n, :] for j in range(8)]
        return jnp.concatenate(parts, axis=1)

    def expand(core):
        for n0, n in ((0, 256), (256, 256), (512, 192)):
            gate = up = None
            for h in range(2):
                a = ag[:, h].reshape(4 * R, H)
                w_gate = lined_up(wg, core, h, n0, n)
                w_up = lined_up(wu, core, h, n0, n)
                gate = dot_nt(a, w_gate) if gate is None else gate + dot_nt(a, w_gate)
                up = dot_nt(a, w_up) if up is None else up + dot_nt(a, w_up)
            hid[core, :, n0 : n0 + n] = (silu(gate) * up).astype(BF16)

    expand(c)
    pump(14)
    for name in ("G", "U"):
        for f in STEPS:
            for s in STEPS:
                pair_wait(name, f, s)
    expand(o)
    pump(15)

    down = Sum(psend2, rp2, rm2, rs2_sem)
    for i, q in enumerate(ORDER):
        if i >= 2:
            pump(14 + i)
        for rz, ry in COLUMNS[i]:
            for name in ("A", "B"):
                f, s = place(name, rz, ry)
                pair_wait(name, f, s)
        for e in range(2):
            acc = None
            for cc in range(2):
                w_down = jnp.concatenate(
                    [wd[cc, at(z, rz), at(y, ry)] for rz, ry in COLUMNS[i][2 * e : 2 * e + 2]], axis=1
                )
                acc = dot(hid[cc], w_down) if acc is None else acc + dot(hid[cc], w_down)
            psend2[:, q, :, e * 256 : (e + 1) * 256] = acc.reshape(4, R, 256).astype(BF16)
        down.after_quarter(q)
    down.merge(0)
    down.merge(1)
    for i, q in ((1, 2), (3, 3), (0, 0), (2, 1)):
        total = down.result(q)
        for j, (rz, ry) in enumerate(COLUMNS[i]):
            n = pl.ds(pl.multiple_of((at(z, rz) * 4 + at(y, ry)) * 128, 128), 128)
            out[:, n] = (midv[:, n].astype(F32) + total[:, 128 * j : 128 * j + 128]).astype(BF16)

    for cp in pending:
        cp.wait_send()


def on_device(
    residual, small_value_inputs, large_value_inputs, small_gate_inputs, large_gate_inputs,
    state_projections, small_step_inputs, large_step_inputs, small_decay_offsets,
    large_decay_offsets, small_decay_rates, large_decay_rates, small_filter_taps,
    large_filter_taps, state_filter_taps, small_head_gains, large_head_gains,
    small_output_projection, large_output_projection, channel_norm_gain, gate_matrix,
    up_matrix, down_matrix,
):
    flat = state_projections.reshape(T, 512)

    anywhere = pl.BlockSpec(memory_space=pl.ANY)
    vmem = pl.BlockSpec(memory_space=pltpu.VMEM)
    smem = pl.BlockSpec(memory_space=pltpu.SMEM)
    dma = pltpu.SemaphoreType.DMA
    V = pltpu.VMEM
    return pl.pallas_call(
        kernel,
        out_shape=jax.ShapeDtypeStruct((R, DM), BF16),
        in_specs=[anywhere] * 11 + [vmem] * 4 + [smem] * 2 + [vmem] * 6,
        out_specs=vmem,
        scratch_shapes=[
            V((T, 768), BF16),
            V((T, 256), BF16),
            V((R, DM), BF16),
            V((16, 768), BF16),
            V((T + 8, 768), F32),
            V((T, 512), BF16),
            V((T, 256), BF16),
            V((NB, 128, 256), F32),
            V((T, 256), F32),
            V((T, 256), BF16),
            V((4, R, 256), BF16),
            V((4, R, 256), BF16),
            V((2, 256, DM), BF16),
            V((2, 4, 4, FD, KROWS), BF16),
            V((2, 4, 4, FD, KROWS), BF16),
            V((2, 4, 4, FD, KROWS), BF16),
            V((2, 4, 136, 128), BF16),
            V((2, 4, 136, 128), BF16),
            V((4, 4, R, Q), BF16),
            V((6, R, Q), BF16),
            V((6, R, Q), BF16),
            V((4, 2, R, H), BF16),
            V((2, 4 * R, FD), BF16),
            V((4, 4, R, Q), BF16),
            V((6, R, Q), BF16),
            V((6, R, Q), BF16),
            V((R, DM), BF16),
            dma((11,)),
            dma((2, 3)),
            dma((60,)),
            dma((4, 4, 4)),
            dma((2, 64)),
            dma((4, 2, 4)),
            dma((2, 6)),
            dma((4, 6)),
            dma((4, 3)),
            dma((4, 6)),
        ],
        compiler_params=pltpu.CompilerParams(
            collective_id=0, has_side_effects=True, vmem_limit_bytes=60 * 1024 * 1024
        ),
    )(
        residual, small_value_inputs, large_value_inputs, small_gate_inputs, large_gate_inputs,
        flat, small_output_projection, large_output_projection, gate_matrix.T, up_matrix.T, down_matrix,
        small_step_inputs.T, large_step_inputs.T, small_decay_offsets.T, large_decay_offsets.T,
        small_decay_rates, large_decay_rates, small_filter_taps, large_filter_taps, state_filter_taps,
        small_head_gains.reshape(1, 128), large_head_gains.reshape(1, 128),
        channel_norm_gain.reshape(1, DM),
    )


def solution(mesh):
    split = Mesh(mesh.devices.reshape(4, 4, 4, 2), ("z", "y", "x", "c"))
    in_specs = (
        P(SP_TP, None),
        P(SP, TP),
        P(SP, TP),
        P(SP, TP),
        P(SP, TP),
        P(SP, None, None),
        P(SP, TP),
        P(SP, TP),
        P(SP, TP),
        P(SP, TP),
        P(TP),
        P(TP),
        P(None, TP),
        P(None, TP),
        P(),
        P(TP),
        P(TP),
        P(TP, None),
        P(TP, None),
        P(),
        P(SP, TP),
        P(SP, TP),
        P(TP, SP),
    )
    return jax.shard_map(
        on_device, mesh=split, in_specs=in_specs, out_specs=P(SP_TP, None), check_vma=False
    )
```

```python
import functools

import jax
import jax.numpy as jnp
from jax import lax
from jax.experimental import pallas as pl
from jax.experimental.pallas import tpu as pltpu
from jax.sharding import Mesh
from jax.sharding import PartitionSpec as P

F32 = jnp.float32
BF16 = jnp.bfloat16
SP = ("z", "y")
TP = ("x", "c")
SP_TP = ("z", "y", "x", "c")

T = 640
L = 128
NB = T // L
R = 80
FD = 704
DM = 2048
H = 1024
KROWS = 128
CUT = 352
Q = 512
ORDER = (0, 2, 1, 3)
STEPS = (0, 1, -1, 2)
COLUMNS = (
    ((0, 0), (0, 1), (0, -1), (1, 0)),
    ((-1, 0), (-1, 1), (1, 1), (1, -1)),
    ((-1, -1), (0, 2), (1, 2), (2, 0)),
    ((2, 1), (-1, 2), (2, -1), (2, 2)),
)
SENDS = (
    ((0, 0, 0, 0, 1), (0, 0, 0, 0, -1), (1, 0, 0, 0, 1), (1, 0, 0, 0, -1), (0, 0, 0, 1, 1), (0, 0, 0, 1, -1)),
    ((1, 0, 0, 1, -1), (1, 0, 0, 1, 1)),
    ((0, 1, 0, 0, -1),),
    ((1, 1, 0, 0, -1), (1, 1, 0, 1, 1), (0, 1, 0, 1, 1), (1, 1, 0, 1, -1)),
    ((0, 1, 0, 1, -1),),
    ((1, -1, 0, 1, 1), (0, -1, 0, 1, 1), (1, -1, 0, 1, -1), (0, -1, 0, 1, -1)),
    ((1, 2, 0, 1, 1), (0, 2, 0, 1, 1), (1, 2, 0, 1, -1), (0, 2, 0, 1, -1)),
    ((2, 0, 0, 0, 1), (3, 0, 0, 0, 1), (2, 0, 0, 0, -1), (3, 0, 0, 0, -1), (1, 0, -1, 1, 1), (0, 0, -1, 1, 1)),
    ((1, 1, 1, 1, -1), (0, 1, 1, 1, -1), (1, -1, -1, 1, 1), (0, -1, -1, 1, 1)),
    (),
    ((1, 2, 1, 1, -1), (2, -1, 0, 0, 1), (0, 2, 1, 1, -1), (3, -1, 0, 0, 1), (3, 0, 0, 1, -1), (3, 0, 0, 1, 1), (2, 0, 0, 1, -1), (2, 0, 0, 1, 1), (3, -1, 0, 1, -1)),
    ((3, 1, 0, 1, 1), (2, 1, 0, 1, -1), (2, 1, 0, 1, 1), (3, 1, 0, 1, -1), (3, -1, 0, 1, 1), (2, -1, 0, 1, -1), (2, -1, 0, 1, 1)),
    ((3, 2, 0, 1, -1), (3, 2, 0, 1, 1), (2, 2, 0, 1, -1), (2, 2, 0, 1, 1)),
    ((3, 0, 1, 1, -1), (3, 1, -1, 1, 1), (2, 0, 1, 1, -1), (2, 1, -1, 1, 1)),
    ((3, -1, 1, 1, -1),),
    (),
    ((2, -1, 1, 1, -1),),
    (),
    ((2, 2, -1, 1, 1), (3, 2, -1, 1, 1)),
    (),
    (),
    (),
)
SHARES = (
    ((0, 0, 0), (1, 0, 0), (2, 0, 0), (3, 0, 0)),
    (),
    ((0, -1, 0), (0, 1, 0), (1, -1, 0), (1, 1, 0)),
    (),
    ((0, 0, -1), (0, 0, 1), (1, 0, 1)),
    (),
    ((1, 0, -1), (0, 2, 0), (1, 2, 0)),
    ((1, 1, -1), (0, 1, -1), (1, 1, 1), (0, 1, 1)),
    ((1, -1, -1), (0, -1, -1), (1, -1, 1), (0, -1, 1)),
    ((1, 2, -1), (0, 2, -1), (1, 2, 1), (2, -1, 0), (0, 2, 1), (3, -1, 0)),
    (),
    ((2, 1, 0), (3, 1, 0), (1, 0, 2), (0, 0, 2), (1, 1, 2), (0, 1, 2)),
    ((1, -1, 2), (0, -1, 2), (1, 2, 2), (2, 2, 0), (0, 2, 2), (3, 2, 0)),
    ((3, 0, 1), (3, 0, -1), (2, 0, 1), (2, 0, -1), (3, -1, 1), (3, 1, -1), (2, 1, 1), (2, 1, -1)),
    ((3, 1, 1),),
    ((3, -1, -1),),
    ((2, -1, 1), (2, -1, -1)),
    ((3, 2, 1),),
    ((3, 2, -1), (2, 2, 1), (2, 2, -1)),
    (),
    ((3, 0, 2), (3, 1, 2), (2, 0, 2), (2, 1, 2)),
    ((3, -1, 2), (2, -1, 2), (2, 2, 2), (3, 2, 2)),
)

head_eps = 1e-05
row_eps = 1e-06


def silu(x):
    return x / (1.0 + jnp.exp(-x))


def dot(a, b):
    return jnp.dot(a, b, preferred_element_type=F32)


def dot_nt(a, b):
    return lax.dot_general(a, b, (((1,), (1,)), ((), ())), preferred_element_type=F32)


def dot_tn(a, b):
    return lax.dot_general(a, b, (((0,), (0,)), ((), ())), preferred_element_type=F32)


def kernel(
    res_in, vs_in, vl_in, gs_in, gl_in, sp_in, ws_in, wl_in, g_in, u_in, d_in,
    steps_s, steps_l, offs_s, offs_l, rates_s, rates_l, taps_s, taps_l, taps_m, gain_s, gain_l, gain_n,
    out,
    xin, sxin, gin, resv, halo, halo_m, cbuf, cmaps, conv_k, drive, fresh, inner, heads, hpart, lhs,
    wo, wg, wu, wd, st1, st2, psend, rp, rm, ag, hid, psend2, rp2, rm2, midv,
    loc_sem, halo_sem, w_send, w_recv, pair_sem, st_sem, hp_sem, rs_sem, ag_sem, rs2_sem,
):
    z, y, x, c = (lax.axis_index(n) for n in ("z", "y", "x", "c"))
    rem = lax.rem
    o = 1 - c

    def at(base, by):
        return rem(base + (by % 4), 4)

    nxt = {"z": rem(z + lax.div(y + 1, 4), 4), "y": rem(y + 1, 4)}
    prv = {"z": rem(z + 3 + lax.div(y + 3, 4), 4), "y": rem(y + 3, 4)}

    def there(**kw):
        base = {"z": z, "y": y, "x": x, "c": c}
        base.update(kw)
        return (base["z"], base["y"], base["x"], base["c"])

    def remote(src, dst, send, recv, **kw):
        return pltpu.make_async_remote_copy(
            src_ref=src, dst_ref=dst, send_sem=send, recv_sem=recv,
            device_id=there(**kw), device_id_type=pl.DeviceIdType.MESH,
        )

    pending = []

    def go(cp):
        cp.start()
        pending.append(cp)
        return cp

    local = [
        (vs_in, xin.at[:, pl.ds(0, 128)]),
        (vl_in, xin.at[:, pl.ds(128, 128)]),
        (sp_in, sxin),
        (gs_in, gin.at[:, pl.ds(0, 128)]),
        (gl_in, gin.at[:, pl.ds(128, 128)]),
        (res_in, resv),
        (ws_in, wo.at[c, pl.ds(0, 128)]),
        (wl_in, wo.at[c, pl.ds(128, 128)]),
        (g_in, wg.at[c, z, y]),
        (u_in, wu.at[c, z, y]),
        (d_in, wd.at[c, z, y]),
    ]
    local = [pltpu.make_async_copy(a, b, loc_sem.at[i]) for i, (a, b) in enumerate(local)]
    for cp in local:
        cp.start()

    barrier = pltpu.get_barrier_semaphore()
    peers = [
        dict(c=o), dict(x=at(x, 1)), dict(x=at(x, 3)),
        dict(y=at(y, 1)), dict(y=at(y, 2)), dict(y=at(y, 3)),
        dict(z=at(z, 1)), dict(z=at(z, 2)), dict(z=at(z, 3)),
        nxt, prv,
    ]
    for p in peers:
        pl.semaphore_signal(barrier, inc=1, device_id=there(**p), device_id_type=pl.DeviceIdType.MESH)
    pl.semaphore_wait(barrier, len(peers))

    tail = pl.ds(T - 16, 16)
    halos = [
        go(remote(src, dst, halo_sem.at[0, i], halo_sem.at[1, i], **nxt))
        for i, (src, dst) in enumerate((
            (vs_in.at[tail], halo.at[:, pl.ds(0, 128)]),
            (vl_in.at[tail], halo.at[:, pl.ds(128, 128)]),
            (sp_in.at[pl.ds(4 * T - 64, 64)], halo_m),
        ))
    ]

    names = ("G", "U", "A", "B")
    own_src = {
        "G": g_in, "U": u_in,
        "A": d_in.at[pl.ds(0, CUT)], "B": d_in.at[pl.ds(CUT, CUT)],
    }

    def unit(name, rz, ry, core):
        zz, yy = at(z, rz), at(y, ry)
        if name == "G":
            return wg.at[core, zz, yy]
        if name == "U":
            return wu.at[core, zz, yy]
        rows = pl.ds(0, CUT) if name == "A" else pl.ds(CUT, CUT)
        return wd.at[core, zz, yy, rows]

    def place(name, f, s):
        return (f, s) if name in ("U", "B") else (s, f)

    def source(name, f, s):
        return own_src[name] if (f, s) == (0, 0) else unit(name, *place(name, f, s), c)

    def w_sem(name, rz, ry):
        return w_recv.at[names.index(name), rz % 4, ry % 4]

    n_sent = [0]
    here = {(n, 0, 0) for n in names}

    def w_wait(name, f, s):
        if (name, f, s) not in here:
            here.add((name, f, s))
            ref = unit(name, *place(name, f, s), c)
            remote(ref, ref, w_send.at[0], w_sem(name, *place(name, f, s))).wait_recv()

    def w_go(name, f, s, second, step):
        w_wait(name, f, s)
        dz, dy = place(name, 0, step) if second else place(name, step, 0)
        rz, ry = place(name, f, s)
        k = n_sent[0]
        n_sent[0] += 1
        go(remote(
            source(name, f, s), unit(name, rz, ry, c), w_send.at[k], w_sem(name, rz - dz, ry - dy),
            z=at(z, dz), y=at(y, dy),
        ))

    pair_index = {}

    def share(name, f, s):
        w_wait(name, f, s)
        k = pair_index.setdefault((name, f, s), len(pair_index))
        go(remote(
            source(name, f, s), unit(name, *place(name, f, s), c),
            pair_sem.at[0, k], pair_sem.at[1, k], c=o,
        ))

    def pair_wait(name, f, s):
        k = pair_index[(name, f, s)]
        ref = unit(name, *place(name, f, s), o)
        remote(ref, ref, pair_sem.at[0, k], pair_sem.at[1, k], c=o).wait_recv()

    def pump(i):
        for n, f, s, second, step in SENDS[i]:
            w_go(names[n], f, s, second, step)
        for n, f, s in SHARES[i]:
            share(names[n], f, s)

    pump(0)

    wo_copies = [
        go(remote(src, wo.at[c, rows], hp_sem.at[0, 4 + i], hp_sem.at[1, 4 + i], c=o))
        for i, (src, rows) in enumerate(((ws_in, pl.ds(0, 128)), (wl_in, pl.ds(128, 128))))
    ]

    lane = lax.broadcasted_iota(jnp.int32, (8, L), 1)
    rows = []
    both = []
    row8 = lax.broadcasted_iota(jnp.int32, (8, L), 0)
    raw_steps = jnp.concatenate([steps_s[...].astype(F32), steps_l[...].astype(F32)], axis=0)
    softened = jnp.maximum(raw_steps, 0.0) + jnp.log1p(jnp.exp(-jnp.abs(raw_steps)))
    head = lax.broadcasted_iota(jnp.int32, (3, T), 0)
    rate = jnp.where(head == 0, rates_s[0], jnp.where(head == 1, rates_s[1], rates_l[0]))
    offsets = jnp.concatenate([offs_s[...], offs_l[...]], axis=0)
    meta = jnp.concatenate(
        [offsets - jnp.exp(rate) * softened, softened, jnp.zeros((2, T), F32)], axis=0
    )
    for k in range(NB):
        raw = meta[:, k * L : (k + 1) * L]
        acc = raw
        for sft in (1, 2, 4, 8, 16, 32, 64):
            acc = acc + jnp.where(lane >= sft, pltpu.roll(acc, sft, 1), 0.0)
        rows.append(acc)
        both.append(jnp.where(row8 < 3, acc, raw))
    both.append(jnp.zeros((L - 8 * NB, L), F32))
    cols = jnp.concatenate(both, axis=0).T
    grown = jnp.exp(cols)
    shrunk = jnp.exp(cols[L - 1 : L, :] - cols)

    half = lax.broadcasted_iota(jnp.int32, (L, L), 1) < 64
    half1 = lax.broadcasted_iota(jnp.int32, (1, L), 1) < 64

    def spread(m, k, off):
        b = 8 * k + off
        small = jnp.where(half, m[:, b : b + 1], m[:, b + 1 : b + 2])
        large = jnp.broadcast_to(m[:, b + 2 : b + 3], (L, L))
        return small, large

    def block_decay(k):
        b = 8 * k
        e = grown[L - 1 : L]
        small = jnp.where(half1, e[:, b : b + 1], e[:, b + 1 : b + 2])
        large = jnp.broadcast_to(e[:, b + 2 : b + 3], (1, L))
        return jnp.concatenate([small, large], axis=1)

    tap_rows = []
    for j in range(4):
        m = taps_m[j].astype(F32)
        tap_rows.append(
            [taps_s[j : j + 1].astype(F32), taps_l[j : j + 1].astype(F32)]
            + [m[i : i + 1] for i in range(4)]
        )

    def conv(k, g):
        total = None
        for j in range(4):
            row = k * L + 5 + j
            if g < 2:
                rows_j = cbuf[row : row + L, g * 128 : g * 128 + 128]
            else:
                rows_j = cmaps[pl.ds(4 * row + g - 2, L, 4), :]
            part = tap_rows[j][g] * rows_j
            total = part if total is None else total + part
        return silu(total)

    for i in range(3):
        local[i].wait()
    for k in range(NB):
        cbuf[8 + k * L : 8 + (k + 1) * L, :] = xin[k * L : (k + 1) * L, :].astype(F32)
        maps_k = pl.ds(32 + 4 * k * L, 4 * L)
        cmaps[maps_k, :] = sxin[4 * k * L : 4 * (k + 1) * L, :].astype(F32)
    decays = [block_decay(k) for k in range(NB)]

    def first_pass(k, kind):
        dt, sh = spread(cols, k, 3)[kind], spread(shrunk, k, 0)[kind]
        blk, at_kind = pl.ds(k * L, L), pl.ds(kind * 128, 128)
        d = conv(k, kind) * dt
        drive[blk, at_kind] = d.astype(BF16)
        key = conv(k, 2 + 2 * kind).astype(BF16)
        conv_k[blk, 256 * kind : 256 * kind + 128] = key
        conv_k[blk, 256 * kind + 128 : 256 * kind + 256] = conv(k, 3 + 2 * kind).astype(BF16)
        fresh[k, :, at_kind] = dot_tn(key, (d * sh).astype(BF16))

    for kind in range(2):
        for k in range(1, NB):
            first_pass(k, kind)
    for cp in halos:
        cp.wait_recv()
    start = jnp.where(jnp.logical_and(z == 0, y == 0), 0.0, 1.0)
    cbuf[0:8, :] = halo[8:16, :].astype(F32) * start
    cmaps[0:32, :] = halo_m[32:64, :].astype(F32) * start

    def state_out(buf, kind, state, total, stage, **axis):
        buf[kind, 0, 0:128] = state.astype(BF16)
        buf[kind, 0, 128:136] = jnp.broadcast_to(total, (8, 128)).astype(BF16)
        ((name, me),) = axis.items()
        copies = [
            remote(
                buf.at[kind, 0], buf.at[kind, r],
                st_sem.at[2 * stage, kind, r], st_sem.at[2 * stage + 1, kind, r],
                **{name: at(me, r)},
            )
            for r in (1, 2, 3)
        ]
        pending.extend(copies)
        return copies

    def start_all(copies):
        for cp in copies:
            cp.start()

    def states_in(buf, kind, stage):
        for r in (1, 2, 3):
            remote(
                buf.at[kind, 0], buf.at[kind, r],
                st_sem.at[2 * stage, kind, r], st_sem.at[2 * stage + 1, kind, r],
            ).wait_recv()

    def chained(buf, kind, me):
        line, line_d = jnp.zeros((128, 128), F32), jnp.ones((1, 128), F32)
        before, before_d = line, line_d
        for j in range(4):
            blob = buf[kind, rem(me - j + 4, 4)].astype(F32)
            line = line * blob[128:129] + blob[0:128]
            line_d = line_d * blob[128:129]
            before = jnp.where(j < me, line, before)
            before_d = jnp.where(j < me, line_d, before_d)
        return before, before_d, line, line_d

    later = []
    for kind in range(2):
        first_pass(0, kind)
        own = slice(kind * 128, kind * 128 + 128)
        state, total = fresh[0, :, own], decays[0][:, own]
        for k in range(1, NB):
            state = state * decays[k][:, own] + fresh[k, :, own]
            total = total * decays[k][:, own]
        copies = state_out(st1, kind, state, total, 0, y=y)
        pl.when(c == 0)(functools.partial(start_all, copies))
        later += copies

    mask = lax.broadcasted_iota(jnp.int32, (L, L), 0) >= lax.broadcasted_iota(jnp.int32, (L, L), 1)

    def weights_of(k, h):
        b = 8 * k + h
        diff = cols[:, b : b + 1] - rows[k][h : h + 1, :]
        return jnp.exp(jnp.where(mask, diff, -1e30))

    def second_pass(k):
        blk = pl.ds(k * L, L)
        s_s = dot_nt(conv_k[blk, 128:256], conv_k[blk, 0:128])
        s_l = dot_nt(conv_k[blk, 384:512], conv_k[blk, 256:384])
        d_s = drive[blk, 0:128]
        o_0 = dot((s_s * weights_of(k, 0)).astype(BF16), d_s)
        o_1 = dot((s_s * weights_of(k, 1)).astype(BF16), d_s)
        inner[blk, 0:128] = jnp.where(half, o_0, o_1)
        inner[blk, 128:256] = dot((s_l * weights_of(k, 2)).astype(BF16), drive[blk, 128:256])

    for k in range(NB):
        second_pass(k)
    pl.when(c == 1)(functools.partial(start_all, later))
    pump(1)
    inside = []
    for kind in range(2):
        states_in(st1, kind, 0)
        before, before_d, line, line_d = chained(st1, kind, y)
        inside.append((before, before_d))
        start_all(state_out(st2, kind, line, line_d, 1, z=z))
        if kind == 0:
            pump(2)
    pump(3)

    for i in (3, 4):
        local[i].wait()

    def third_pass(k, kind, carry):
        blk, cols_k = pl.ds(k * L, L), pl.ds(kind * 128, 128)
        own = slice(kind * 128, kind * 128 + 128)
        reads = conv_k[blk, 256 * kind + 128 : 256 * kind + 256]
        out_k = inner[blk, cols_k] + dot(reads, carry.astype(BF16)) * spread(grown, k, 0)[kind]
        carry = carry * decays[k][:, own] + fresh[k, :, own]
        out_k = out_k * silu(gin[blk, cols_k].astype(F32))
        sq = out_k * out_k
        if kind == 0:
            sq_0 = jnp.sum(jnp.where(half, sq, 0.0), axis=1, keepdims=True)
            sq_1 = jnp.sum(jnp.where(half, 0.0, sq), axis=1, keepdims=True)
            mean = jnp.where(half, sq_0, sq_1) * (1.0 / 64)
            gain = gain_s[...]
        else:
            mean = jnp.sum(sq, axis=1, keepdims=True) * (1.0 / 128)
            gain = gain_l[...]
        heads[blk, cols_k] = (out_k * lax.rsqrt(mean + head_eps) * gain).astype(BF16)
        return carry

    for kind in range(2):
        states_in(st2, kind, 1)
        before = chained(st2, kind, z)[0]
        carry = before * inside[kind][1] + inside[kind][0]
        for k in range(NB):
            carry = third_pass(k, kind, carry)
        if kind == 0:
            pump(4)

    def rows_of(b, core):
        return pl.ds(pl.multiple_of((2 * b + core) * R, 16), R)

    for b in range(4):
        go(remote(heads.at[rows_of(b, o)], hpart.at[b], hp_sem.at[0, b], hp_sem.at[1, b], c=o))
    for b in range(4):
        lhs[b] = heads[rows_of(b, c), :]
    for i in (6, 7):
        local[i].wait()
    own_rows = lhs[...].reshape(4 * R, 256)
    for cp in wo_copies:
        cp.wait_recv()
    pump(5)
    for b in range(4):
        remote(hpart.at[b], hpart.at[b], hp_sem.at[0, b], hp_sem.at[1, b]).wait_recv()
    part_rows = hpart[...].reshape(4 * R, 256)

    x1, x2, x3 = at(x, 1), at(x, 2), at(x, 3)

    class Sum:
        def __init__(self, parts, from_left, from_right, sems):
            self.parts, self.left, self.right, self.sems = parts, from_left, from_right, sems

        def to_right(self, slot, block, h):
            go(remote(self.parts.at[block, h], self.left.at[slot], self.sems.at[0, slot], self.sems.at[1, slot], x=x1))

        def to_left(self, slot, block, h):
            go(remote(self.parts.at[block, h], self.right.at[slot], self.sems.at[2, slot], self.sems.at[3, slot], x=x3))

        def wait_left(self, slot):
            remote(self.left.at[slot], self.left.at[slot], self.sems.at[0, slot], self.sems.at[1, slot]).wait_recv()

        def wait_right(self, slot):
            remote(self.right.at[slot], self.right.at[slot], self.sems.at[2, slot], self.sems.at[3, slot]).wait_recv()

        def after_quarter(self, q):
            if q < 2:
                self.to_right(q, x2, q)
                self.to_left(q + 2, x3, q)
            else:
                self.to_left(q - 2, x2, q)
                self.to_right(q, x1, q)

        def merge(self, i):
            p = self.parts
            self.wait_left(i)
            p[x1, i] = (p[x1, i].astype(F32) + self.left[i].astype(F32)).astype(BF16)
            self.to_right(4 + i, x1, i)
            self.wait_right(i)
            p[x3, 2 + i] = (p[x3, 2 + i].astype(F32) + self.right[i].astype(F32)).astype(BF16)
            self.to_left(4 + i, x3, 2 + i)

        def result(self, q):
            a, b = (4 + q, 2 + q) if q < 2 else (q, 2 + q)
            self.wait_left(a)
            self.wait_right(b)
            return self.parts[x, q].astype(F32) + self.left[a].astype(F32) + self.right[b].astype(F32)

    mixed = Sum(psend, rp, rm, rs_sem)
    for q in ORDER:
        for e in range(2):
            n = pl.ds(q * Q + e * 256, 256)
            acc = dot(own_rows, wo[c, :, n]) + dot(part_rows, wo[o, :, n])
            psend[:, q, :, e * 256 : (e + 1) * 256] = acc.reshape(4, R, 256).astype(BF16)
        mixed.after_quarter(q)
    pump(6)
    mixed.merge(0)
    pump(7)
    mixed.merge(1)
    pump(8)
    local[5].wait()
    sums = {q: mixed.result(q) for q in (2, 3)}
    pump(9)
    sums.update({q: mixed.result(q) for q in (0, 1)})
    lo = jnp.concatenate([sums[0], sums[1]], axis=1)
    hi = jnp.concatenate([sums[2], sums[3]], axis=1)
    mid_lo = (resv[:, 0:H].astype(F32) + lo).astype(BF16)
    mid_hi = (resv[:, H:DM].astype(F32) + hi).astype(BF16)
    midv[:, 0:H] = mid_lo
    midv[:, H:DM] = mid_hi
    f_lo, f_hi = mid_lo.astype(F32), mid_hi.astype(F32)
    square = jnp.sum(f_lo * f_lo, axis=1, keepdims=True) + jnp.sum(f_hi * f_hi, axis=1, keepdims=True)
    scale = lax.rsqrt(square * (1.0 / DM) + row_eps)
    ag[x, 0] = (f_lo * scale * gain_n[:, 0:H]).astype(BF16)
    ag[x, 1] = (f_hi * scale * gain_n[:, H:DM]).astype(BF16)

    def ag_right(slot, block, h):
        go(remote(ag.at[block, h], ag.at[block, h], ag_sem.at[0, slot], ag_sem.at[1, slot], x=x1))

    def ag_left(slot, block, h):
        go(remote(ag.at[block, h], ag.at[block, h], ag_sem.at[2, slot], ag_sem.at[3, slot], x=x3))

    def ag_wait(side, slot, block, h):
        remote(ag.at[block, h], ag.at[block, h], ag_sem.at[0, slot], ag_sem.at[side, slot]).wait_recv()

    ag_right(0, x, 0)
    ag_left(0, x, 1)
    ag_right(1, x, 1)
    ag_left(1, x, 0)

    pump(10)
    ag_wait(1, 0, x3, 0)
    ag_right(2, x3, 0)
    ag_wait(3, 0, x1, 1)
    ag_left(2, x1, 1)
    pump(11)
    ag_wait(1, 1, x3, 1)
    ag_wait(3, 1, x1, 0)
    pump(12)
    ag_wait(1, 2, x2, 0)
    ag_wait(3, 2, x2, 1)
    pump(13)
    for i in (8, 9, 10):
        local[i].wait()
    def lined_up(w, core, h, n0, n):
        parts = [w[core, 2 * h + j // 4, j % 4, n0 : n0 + n, :] for j in range(8)]
        return jnp.concatenate(parts, axis=1)

    def expand(core, points):
        for n0, n in ((0, 256), (256, 256), (512, 192)):
            if n0 > 0:
                pump(points[n0 // 256 - 1])
            gate = up = None
            for h in range(2):
                a = ag[:, h].reshape(4 * R, H)
                w_gate = lined_up(wg, core, h, n0, n)
                w_up = lined_up(wu, core, h, n0, n)
                gate = dot_nt(a, w_gate) if gate is None else gate + dot_nt(a, w_gate)
                up = dot_nt(a, w_up) if up is None else up + dot_nt(a, w_up)
            hid[core, :, n0 : n0 + n] = (silu(gate) * up).astype(BF16)

    expand(c, (14, 15))
    pump(16)
    for name in ("G", "U"):
        for f in STEPS:
            for s in STEPS:
                pair_wait(name, f, s)
    expand(o, (17, 18))
    pump(19)

    down = Sum(psend2, rp2, rm2, rs2_sem)
    for i, q in enumerate(ORDER):
        if i >= 2:
            pump(18 + i)
        for rz, ry in COLUMNS[i]:
            for name in ("A", "B"):
                f, s = place(name, rz, ry)
                pair_wait(name, f, s)
        for e in range(2):
            acc = None
            for cc in range(2):
                w_down = jnp.concatenate(
                    [wd[cc, at(z, rz), at(y, ry)] for rz, ry in COLUMNS[i][2 * e : 2 * e + 2]], axis=1
                )
                acc = dot(hid[cc], w_down) if acc is None else acc + dot(hid[cc], w_down)
            psend2[:, q, :, e * 256 : (e + 1) * 256] = acc.reshape(4, R, 256).astype(BF16)
        down.after_quarter(q)
    down.merge(0)
    down.merge(1)
    for i, q in ((1, 2), (3, 3), (0, 0), (2, 1)):
        total = down.result(q)
        for j, (rz, ry) in enumerate(COLUMNS[i]):
            n = pl.ds(pl.multiple_of((at(z, rz) * 4 + at(y, ry)) * 128, 128), 128)
            out[:, n] = (midv[:, n].astype(F32) + total[:, 128 * j : 128 * j + 128]).astype(BF16)

    for cp in pending:
        cp.wait_send()


def on_device(
    residual, small_value_inputs, large_value_inputs, small_gate_inputs, large_gate_inputs,
    state_projections, small_step_inputs, large_step_inputs, small_decay_offsets,
    large_decay_offsets, small_decay_rates, large_decay_rates, small_filter_taps,
    large_filter_taps, state_filter_taps, small_head_gains, large_head_gains,
    small_output_projection, large_output_projection, channel_norm_gain, gate_matrix,
    up_matrix, down_matrix,
):
    flat = state_projections.reshape(4 * T, 128)

    anywhere = pl.BlockSpec(memory_space=pl.ANY)
    vmem = pl.BlockSpec(memory_space=pltpu.VMEM)
    smem = pl.BlockSpec(memory_space=pltpu.SMEM)
    dma = pltpu.SemaphoreType.DMA
    V = pltpu.VMEM
    return pl.pallas_call(
        kernel,
        out_shape=jax.ShapeDtypeStruct((R, DM), BF16),
        in_specs=[anywhere] * 11 + [vmem] * 4 + [smem] * 2 + [vmem] * 6,
        out_specs=vmem,
        scratch_shapes=[
            V((T, 256), BF16),
            V((4 * T, 128), BF16),
            V((T, 256), BF16),
            V((R, DM), BF16),
            V((16, 256), BF16),
            V((64, 128), BF16),
            V((T + 8, 256), F32),
            V((4 * T + 32, 128), F32),
            V((T, 512), BF16),
            V((T, 256), BF16),
            V((NB, 128, 256), F32),
            V((T, 256), F32),
            V((T, 256), BF16),
            V((4, R, 256), BF16),
            V((4, R, 256), BF16),
            V((2, 256, DM), BF16),
            V((2, 4, 4, FD, KROWS), BF16),
            V((2, 4, 4, FD, KROWS), BF16),
            V((2, 4, 4, FD, KROWS), BF16),
            V((2, 4, 136, 128), BF16),
            V((2, 4, 136, 128), BF16),
            V((4, 4, R, Q), BF16),
            V((6, R, Q), BF16),
            V((6, R, Q), BF16),
            V((4, 2, R, H), BF16),
            V((2, 4 * R, FD), BF16),
            V((4, 4, R, Q), BF16),
            V((6, R, Q), BF16),
            V((6, R, Q), BF16),
            V((R, DM), BF16),
            dma((11,)),
            dma((2, 3)),
            dma((60,)),
            dma((4, 4, 4)),
            dma((2, 64)),
            dma((4, 2, 4)),
            dma((2, 6)),
            dma((4, 6)),
            dma((4, 3)),
            dma((4, 6)),
        ],
        compiler_params=pltpu.CompilerParams(
            collective_id=0, has_side_effects=True, vmem_limit_bytes=60 * 1024 * 1024
        ),
    )(
        residual, small_value_inputs, large_value_inputs, small_gate_inputs, large_gate_inputs,
        flat, small_output_projection, large_output_projection, gate_matrix.T, up_matrix.T, down_matrix,
        small_step_inputs.T, large_step_inputs.T, small_decay_offsets.T, large_decay_offsets.T,
        small_decay_rates, large_decay_rates, small_filter_taps, large_filter_taps, state_filter_taps,
        small_head_gains.reshape(1, 128), large_head_gains.reshape(1, 128),
        channel_norm_gain.reshape(1, DM),
    )


def solution(mesh):
    split = Mesh(mesh.devices.reshape(4, 4, 4, 2), ("z", "y", "x", "c"))
    in_specs = (
        P(SP_TP, None),
        P(SP, TP),
        P(SP, TP),
        P(SP, TP),
        P(SP, TP),
        P(SP, None, None),
        P(SP, TP),
        P(SP, TP),
        P(SP, TP),
        P(SP, TP),
        P(TP),
        P(TP),
        P(None, TP),
        P(None, TP),
        P(),
        P(TP),
        P(TP),
        P(TP, None),
        P(TP, None),
        P(),
        P(SP, TP),
        P(SP, TP),
        P(TP, SP),
    )
    return jax.shard_map(
        on_device, mesh=split, in_specs=in_specs, out_specs=P(SP_TP, None), check_vma=False
    )
```

```python
import functools

import jax
import jax.numpy as jnp
from jax import lax
from jax.experimental import pallas as pl
from jax.experimental.pallas import tpu as pltpu
from jax.sharding import Mesh
from jax.sharding import PartitionSpec as P

F32 = jnp.float32
BF16 = jnp.bfloat16
SP = ("z", "y")
TP = ("x", "c")
SP_TP = ("z", "y", "x", "c")

T = 640
L = 128
NB = T // L
R = 80
FD = 704
DM = 2048
H = 1024
KROWS = 128
CUT = 352
AFTER = (((0,), ()), ((1,), ()), ((2,), (0,)), ((), (1,)), ((3, 4), ()))
WIDTHS = (512, 256, 512, 512, 256)
LOTS = ((0, 48), (48, 32))
STEPS = (0, 1, -1, 2)
COLUMNS = (
    ((0, 0), (-1, 0), (0, -1), (0, 1)),
    ((1, 0), (-1, -1)),
    ((1, 1), (0, 2), (2, 0), (-1, 1)),
    ((1, -1), (2, 1), (1, 2), (-1, 2)),
    ((2, -1), (2, 2)),
)
SENDS = (
    ((0, 0, 0, 0, 1), (0, 0, 0, 0, -1), (1, 0, 0, 0, 1), (1, 0, 0, 0, -1), (0, 0, 0, 1, 1), (0, 0, 0, 1, -1)),
    ((1, 0, 0, 1, -1),),
    ((1, 0, 0, 1, 1),),
    ((0, 1, 0, 0, -1), (1, 1, 0, 0, -1), (0, 1, 0, 1, 1), (1, 1, 0, 1, 1)),
    ((1, 1, 0, 1, -1), (0, 1, 0, 1, -1)),
    ((0, -1, 0, 1, 1), (1, -1, 0, 1, 1), (1, -1, 0, 1, -1)),
    ((0, 2, 0, 1, -1), (0, 2, 0, 1, 1), (1, 2, 0, 1, 1), (1, 2, 0, 1, -1)),
    ((0, -1, 0, 1, -1), (3, 0, 0, 0, 1), (2, 0, 0, 0, 1)),
    ((2, 0, 0, 0, -1), (3, 0, 0, 0, -1), (0, 0, -1, 1, 1), (0, 2, 1, 1, -1), (1, 0, -1, 1, 1), (1, 1, 1, 1, -1)),
    ((1, 2, -1, 1, 1), (0, 1, -1, 1, 1)),
    ((2, 1, 0, 0, -1), (3, 1, 0, 0, -1)),
    ((1, -1, 1, 1, -1), (0, -1, 1, 1, -1), (2, 0, 0, 1, 1), (3, 0, 0, 1, 1), (2, 1, 0, 1, 1)),
    ((3, 0, 0, 1, -1), (2, 0, 0, 1, -1), (3, 1, 0, 1, 1), (2, -1, 0, 1, 1), (3, -1, 0, 1, 1)),
    ((3, 2, 0, 1, -1), (2, 2, 0, 1, -1), (2, 2, 0, 1, 1), (3, 2, 0, 1, 1), (3, 1, 0, 1, -1), (2, 1, 0, 1, -1), (3, -1, 0, 1, -1)),
    ((2, -1, 0, 1, -1), (2, 0, -1, 1, 1), (3, 0, -1, 1, 1), (2, 1, -1, 1, 1), (3, 1, -1, 1, 1)),
    ((2, 2, 1, 1, -1), (3, 2, 1, 1, -1), (2, -1, -1, 1, 1), (3, -1, -1, 1, 1)),
    (),
    (),
    (),
    (),
)
SHARES = (
    ((0, 0, 0), (1, 0, 0), (2, 0, 0), (3, 0, 0)),
    (),
    ((0, -1, 0), (0, 1, 0), (1, -1, 0), (1, 1, 0)),
    (),
    ((0, 0, -1), (0, 0, 1)),
    ((1, 0, 1),),
    ((1, 0, -1), (0, 2, 0), (1, 2, 0)),
    ((0, 1, -1), (1, 1, -1), (1, 1, 1), (0, 1, 1)),
    ((0, -1, -1), (1, -1, -1), (1, -1, 1), (0, 2, 1)),
    ((0, 2, -1), (1, 2, -1)),
    ((1, 2, 1), (0, -1, 1), (3, -1, 0), (2, -1, 0), (2, 1, 0), (3, 1, 0)),
    (),
    ((0, 0, 2), (1, 0, 2), (1, 1, 2), (0, 2, 2)),
    ((2, 2, 0), (3, 2, 0), (0, 1, 2), (1, 2, 2), (1, -1, 2), (0, -1, 2)),
    ((2, 0, -1), (3, 0, -1), (2, 1, -1), (3, 1, -1), (3, 0, 1), (2, 0, 1), (2, -1, -1), (3, -1, -1)),
    ((3, 2, 1), (2, 2, 1), (2, 2, -1), (3, 2, -1), (3, 1, 1), (2, 1, 1), (2, 0, 2), (3, 0, 2), (3, -1, 1)),
    ((2, -1, 1), (2, 1, 2), (3, 1, 2), (3, -1, 2)),
    ((2, 2, 2), (3, 2, 2), (2, -1, 2)),
    (),
    (),
)

head_eps = 1e-05
row_eps = 1e-06


def silu(x):
    return x / (1.0 + jnp.exp(-x))


def dot(a, b):
    return jnp.dot(a, b, preferred_element_type=F32)


def dot_nt(a, b):
    return lax.dot_general(a, b, (((1,), (1,)), ((), ())), preferred_element_type=F32)


def dot_tn(a, b):
    return lax.dot_general(a, b, (((0,), (0,)), ((), ())), preferred_element_type=F32)


def kernel(
    res_in, vs_in, vl_in, gs_in, gl_in, sp_in, ws_in, wl_in, g_in, u_in, d_in,
    small_in_0, small_in_1, small_in_2, small_in_3, small_in_4, small_in_5, small_in_6, small_in_7,
    small_in_8, small_in_9, small_in_10, small_in_11,
    out_hbm,
    small, out, out_sem,
    xin, sxin, gin, resv, halo, halo_m, cbuf, cmaps, conv_k, drive, fresh, inner, heads, hpart_0, hpart_1, lhs_0, lhs_1,
    wo, wg, wu, wd, st1, st2, parts_0, parts_1, left_0, left_1, right_0, right_1, ag, hid,
    dparts, dleft, dright, mid_0, mid_1,
    loc_sem, halo_sem, w_send, w_recv, pair_sem, st_sem, hp_sem, rs_sem, ag_sem, rs2_sem,
):
    z, y, x, c = (lax.axis_index(n) for n in ("z", "y", "x", "c"))
    rem = lax.rem
    o = 1 - c

    def at(base, by):
        return rem(base + (by % 4), 4)

    nxt = {"z": rem(z + lax.div(y + 1, 4), 4), "y": rem(y + 1, 4)}
    prv = {"z": rem(z + 3 + lax.div(y + 3, 4), 4), "y": rem(y + 3, 4)}

    def there(**kw):
        base = {"z": z, "y": y, "x": x, "c": c}
        base.update(kw)
        return (base["z"], base["y"], base["x"], base["c"])

    def remote(src, dst, send, recv, **kw):
        return pltpu.make_async_remote_copy(
            src_ref=src, dst_ref=dst, send_sem=send, recv_sem=recv,
            device_id=there(**kw), device_id_type=pl.DeviceIdType.MESH,
        )

    pending = []

    def go(cp):
        cp.start()
        pending.append(cp)
        return cp

    barrier = pltpu.get_barrier_semaphore()
    peers = [
        dict(c=o), dict(x=at(x, 1)), dict(x=at(x, 3)),
        dict(y=at(y, 1)), dict(y=at(y, 2)), dict(y=at(y, 3)),
        dict(z=at(z, 1)), dict(z=at(z, 2)), dict(z=at(z, 3)),
        nxt, prv,
    ]
    for p in peers:
        pl.semaphore_signal(barrier, inc=1, device_id=there(**p), device_id_type=pl.DeviceIdType.MESH)
    local = [
        *zip(
            (small_in_0, small_in_1, small_in_2, small_in_3, small_in_4, small_in_5, small_in_6,
             small_in_7, small_in_8, small_in_9, small_in_10, small_in_11), small,
        ),
        (vs_in, xin.at[:, pl.ds(0, 128)]),
        (vl_in, xin.at[:, pl.ds(128, 128)]),
        (sp_in, sxin),
        (gs_in, gin.at[:, pl.ds(0, 128)]),
        (gl_in, gin.at[:, pl.ds(128, 128)]),
        (res_in, resv),
        (ws_in, wo.at[c, pl.ds(0, 128)]),
        (wl_in, wo.at[c, pl.ds(128, 128)]),
        (g_in, wg.at[c, z, y]),
        (u_in, wu.at[c, z, y]),
        (d_in, wd.at[c, z, y]),
    ]
    local = [pltpu.make_async_copy(a, b, loc_sem.at[i]) for i, (a, b) in enumerate(local)]
    for cp in local:
        cp.start()
    fetched, local = local[:12], local[12:]
    steps_s, steps_l, offs_s, offs_l, rates_s, rates_l, taps_s, taps_l, taps_m, gain_s, gain_l, gain_n = small

    pl.semaphore_wait(barrier, len(peers))

    tail = pl.ds(T - 16, 16)
    halos = [
        go(remote(src, dst, halo_sem.at[0, i], halo_sem.at[1, i], **nxt))
        for i, (src, dst) in enumerate((
            (vs_in.at[tail], halo.at[:, pl.ds(0, 128)]),
            (vl_in.at[tail], halo.at[:, pl.ds(128, 128)]),
            (sp_in.at[pl.ds(4 * T - 64, 64)], halo_m),
        ))
    ]

    names = ("G", "U", "A", "B")
    own_src = {
        "G": g_in, "U": u_in,
        "A": d_in.at[pl.ds(0, CUT)], "B": d_in.at[pl.ds(CUT, CUT)],
    }

    def unit(name, rz, ry, core):
        zz, yy = at(z, rz), at(y, ry)
        if name == "G":
            return wg.at[core, zz, yy]
        if name == "U":
            return wu.at[core, zz, yy]
        rows = pl.ds(0, CUT) if name == "A" else pl.ds(CUT, CUT)
        return wd.at[core, zz, yy, rows]

    def place(name, f, s):
        return (f, s) if name in ("U", "B") else (s, f)

    def source(name, f, s):
        return own_src[name] if (f, s) == (0, 0) else unit(name, *place(name, f, s), c)

    def w_sem(name, rz, ry):
        return w_recv.at[names.index(name), rz % 4, ry % 4]

    n_sent = [0]
    here = {(n, 0, 0) for n in names}

    def w_wait(name, f, s):
        if (name, f, s) not in here:
            here.add((name, f, s))
            ref = unit(name, *place(name, f, s), c)
            remote(ref, ref, w_send.at[0], w_sem(name, *place(name, f, s))).wait_recv()

    def w_go(name, f, s, second, step):
        w_wait(name, f, s)
        dz, dy = place(name, 0, step) if second else place(name, step, 0)
        rz, ry = place(name, f, s)
        k = n_sent[0]
        n_sent[0] += 1
        go(remote(
            source(name, f, s), unit(name, rz, ry, c), w_send.at[k], w_sem(name, rz - dz, ry - dy),
            z=at(z, dz), y=at(y, dy),
        ))

    pair_index = {}

    def share(name, f, s):
        w_wait(name, f, s)
        k = pair_index.setdefault((name, f, s), len(pair_index))
        go(remote(
            source(name, f, s), unit(name, *place(name, f, s), c),
            pair_sem.at[0, k], pair_sem.at[1, k], c=o,
        ))

    def pair_wait(name, f, s):
        k = pair_index[(name, f, s)]
        ref = unit(name, *place(name, f, s), o)
        remote(ref, ref, pair_sem.at[0, k], pair_sem.at[1, k], c=o).wait_recv()

    def pump(i):
        for n, f, s, second, step in SENDS[i]:
            w_go(names[n], f, s, second, step)
        for n, f, s in SHARES[i]:
            share(names[n], f, s)

    pump(0)

    wo_copies = [
        go(remote(src, wo.at[c, rows], hp_sem.at[0, 8 + i], hp_sem.at[1, 8 + i], c=o))
        for i, (src, rows) in enumerate(((ws_in, pl.ds(0, 128)), (wl_in, pl.ds(128, 128))))
    ]

    for cp in fetched:
        cp.wait()
    lane = lax.broadcasted_iota(jnp.int32, (8, L), 1)
    rows = []
    both = []
    row8 = lax.broadcasted_iota(jnp.int32, (8, L), 0)
    raw_steps = jnp.concatenate([steps_s[...].astype(F32), steps_l[...].astype(F32)], axis=0)
    softened = jnp.maximum(raw_steps, 0.0) + jnp.log1p(jnp.exp(-jnp.abs(raw_steps)))
    head = lax.broadcasted_iota(jnp.int32, (3, T), 0)
    rate = jnp.where(head == 0, rates_s[0:1, 0:1], jnp.where(head == 1, rates_s[0:1, 1:2], rates_l[0:1, 0:1]))
    offsets = jnp.concatenate([offs_s[...], offs_l[...]], axis=0)
    meta = jnp.concatenate(
        [offsets - jnp.exp(rate) * softened, softened, jnp.zeros((2, T), F32)], axis=0
    )
    for k in range(NB):
        raw = meta[:, k * L : (k + 1) * L]
        acc = raw
        for sft in (1, 2, 4, 8, 16, 32, 64):
            acc = acc + jnp.where(lane >= sft, pltpu.roll(acc, sft, 1), 0.0)
        rows.append(acc)
        both.append(jnp.where(row8 < 3, acc, raw))
    both.append(jnp.zeros((L - 8 * NB, L), F32))
    cols = jnp.concatenate(both, axis=0).T
    grown = jnp.exp(cols)
    shrunk = jnp.exp(cols[L - 1 : L, :] - cols)

    half = lax.broadcasted_iota(jnp.int32, (L, L), 1) < 64
    half1 = lax.broadcasted_iota(jnp.int32, (1, L), 1) < 64

    def spread(m, k, off):
        b = 8 * k + off
        small = jnp.where(half, m[:, b : b + 1], m[:, b + 1 : b + 2])
        large = jnp.broadcast_to(m[:, b + 2 : b + 3], (L, L))
        return small, large

    def block_decay(k):
        b = 8 * k
        e = grown[L - 1 : L]
        small = jnp.where(half1, e[:, b : b + 1], e[:, b + 1 : b + 2])
        large = jnp.broadcast_to(e[:, b + 2 : b + 3], (1, L))
        return jnp.concatenate([small, large], axis=1)

    tap_rows = []
    for j in range(4):
        m = taps_m[j].astype(F32)
        tap_rows.append(
            [taps_s[j : j + 1].astype(F32), taps_l[j : j + 1].astype(F32)]
            + [m[i : i + 1] for i in range(4)]
        )

    def conv(k, g):
        total = None
        for j in range(4):
            row = k * L + 5 + j
            if g < 2:
                rows_j = cbuf[row : row + L, g * 128 : g * 128 + 128]
            else:
                rows_j = cmaps[pl.ds(4 * row + g - 2, L, 4), :]
            part = tap_rows[j][g] * rows_j
            total = part if total is None else total + part
        return silu(total)

    for i in range(3):
        local[i].wait()
    for k in range(NB):
        cbuf[8 + k * L : 8 + (k + 1) * L, :] = xin[k * L : (k + 1) * L, :].astype(F32)
        maps_k = pl.ds(32 + 4 * k * L, 4 * L)
        cmaps[maps_k, :] = sxin[4 * k * L : 4 * (k + 1) * L, :].astype(F32)
    decays = [block_decay(k) for k in range(NB)]

    def first_pass(k, kind):
        dt, sh = spread(cols, k, 3)[kind], spread(shrunk, k, 0)[kind]
        blk, at_kind = pl.ds(k * L, L), pl.ds(kind * 128, 128)
        d = conv(k, kind) * dt
        drive[blk, at_kind] = d.astype(BF16)
        key = conv(k, 2 + 2 * kind).astype(BF16)
        conv_k[blk, 256 * kind : 256 * kind + 128] = key
        conv_k[blk, 256 * kind + 128 : 256 * kind + 256] = conv(k, 3 + 2 * kind).astype(BF16)
        fresh[k, :, at_kind] = dot_tn(key, (d * sh).astype(BF16))

    for kind in range(2):
        for k in range(1, NB):
            first_pass(k, kind)
    for cp in halos:
        cp.wait_recv()
    start = jnp.where(jnp.logical_and(z == 0, y == 0), 0.0, 1.0)
    cbuf[0:8, :] = halo[8:16, :].astype(F32) * start
    cmaps[0:32, :] = halo_m[32:64, :].astype(F32) * start

    def state_out(buf, kind, state, total, stage, **axis):
        buf[kind, 0, 0:128] = state.astype(BF16)
        buf[kind, 0, 128:136] = jnp.broadcast_to(total, (8, 128)).astype(BF16)
        ((name, me),) = axis.items()
        copies = [
            remote(
                buf.at[kind, 0], buf.at[kind, r],
                st_sem.at[2 * stage, kind, r], st_sem.at[2 * stage + 1, kind, r],
                **{name: at(me, r)},
            )
            for r in (1, 2, 3)
        ]
        pending.extend(copies)
        return copies

    def start_all(copies):
        for cp in copies:
            cp.start()

    def states_in(buf, kind, stage):
        for r in (1, 2, 3):
            remote(
                buf.at[kind, 0], buf.at[kind, r],
                st_sem.at[2 * stage, kind, r], st_sem.at[2 * stage + 1, kind, r],
            ).wait_recv()

    def chained(buf, kind, me):
        line, line_d = jnp.zeros((128, 128), F32), jnp.ones((1, 128), F32)
        before, before_d = line, line_d
        for j in range(4):
            blob = buf[kind, rem(me - j + 4, 4)].astype(F32)
            line = line * blob[128:129] + blob[0:128]
            line_d = line_d * blob[128:129]
            before = jnp.where(j < me, line, before)
            before_d = jnp.where(j < me, line_d, before_d)
        return before, before_d, line, line_d

    later = []
    for kind in range(2):
        first_pass(0, kind)
        own = slice(kind * 128, kind * 128 + 128)
        state, total = fresh[0, :, own], decays[0][:, own]
        for k in range(1, NB):
            state = state * decays[k][:, own] + fresh[k, :, own]
            total = total * decays[k][:, own]
        copies = state_out(st1, kind, state, total, 0, y=y)
        pl.when(c == 0)(functools.partial(start_all, copies))
        later += copies

    mask = lax.broadcasted_iota(jnp.int32, (L, L), 0) >= lax.broadcasted_iota(jnp.int32, (L, L), 1)

    def weights_of(k, h):
        b = 8 * k + h
        diff = cols[:, b : b + 1] - rows[k][h : h + 1, :]
        return jnp.exp(jnp.where(mask, diff, -1e30))

    def second_pass(k):
        blk = pl.ds(k * L, L)
        s_s = dot_nt(conv_k[blk, 128:256], conv_k[blk, 0:128])
        s_l = dot_nt(conv_k[blk, 384:512], conv_k[blk, 256:384])
        d_s = drive[blk, 0:128]
        o_0 = dot((s_s * weights_of(k, 0)).astype(BF16), d_s)
        o_1 = dot((s_s * weights_of(k, 1)).astype(BF16), d_s)
        inner[blk, 0:128] = jnp.where(half, o_0, o_1)
        inner[blk, 128:256] = dot((s_l * weights_of(k, 2)).astype(BF16), drive[blk, 128:256])

    for k in range(NB):
        second_pass(k)
    pl.when(c == 1)(functools.partial(start_all, later))
    pump(1)
    inside = []
    for kind in range(2):
        states_in(st1, kind, 0)
        before, before_d, line, line_d = chained(st1, kind, y)
        inside.append((before, before_d))
        start_all(state_out(st2, kind, line, line_d, 1, z=z))
        if kind == 0:
            pump(2)
    pump(3)

    for i in (3, 4):
        local[i].wait()

    def third_pass(k, kind, carry):
        blk, cols_k = pl.ds(k * L, L), pl.ds(kind * 128, 128)
        own = slice(kind * 128, kind * 128 + 128)
        reads = conv_k[blk, 256 * kind + 128 : 256 * kind + 256]
        out_k = inner[blk, cols_k] + dot(reads, carry.astype(BF16)) * spread(grown, k, 0)[kind]
        carry = carry * decays[k][:, own] + fresh[k, :, own]
        out_k = out_k * silu(gin[blk, cols_k].astype(F32))
        sq = out_k * out_k
        if kind == 0:
            sq_0 = jnp.sum(jnp.where(half, sq, 0.0), axis=1, keepdims=True)
            sq_1 = jnp.sum(jnp.where(half, 0.0, sq), axis=1, keepdims=True)
            mean = jnp.where(half, sq_0, sq_1) * (1.0 / 64)
            gain = gain_s[...]
        else:
            mean = jnp.sum(sq, axis=1, keepdims=True) * (1.0 / 128)
            gain = gain_l[...]
        heads[blk, cols_k] = (out_k * lax.rsqrt(mean + head_eps) * gain).astype(BF16)
        return carry

    for kind in range(2):
        states_in(st2, kind, 1)
        before = chained(st2, kind, z)[0]
        carry = before * inside[kind][1] + inside[kind][0]
        for k in range(NB):
            carry = third_pass(k, kind, carry)
        if kind == 0:
            pump(4)

    hpart, lhs = (hpart_0, hpart_1), (lhs_0, lhs_1)
    parts, left, right = (parts_0, parts_1), (left_0, left_1), (right_0, right_1)
    mid = (mid_0, mid_1)

    def rows_of(b, core, t):
        first, n = LOTS[t]
        return pl.ds(pl.multiple_of((2 * b + core) * R + first, 16), n)

    def block_of(b, t):
        n = LOTS[t][1]
        return pl.ds(b * n if isinstance(b, int) else pl.multiple_of(b * n, 16), n)

    def row_of(b, t):
        first, n = LOTS[t]
        return pl.ds(pl.multiple_of(4 * first + b * n, 16), n)

    hp_copies = [
        [
            go(remote(
                heads.at[rows_of(b, o, t)], hpart[t].at[block_of(b, t)],
                hp_sem.at[0, 4 * t + b], hp_sem.at[1, 4 * t + b], c=o,
            ))
            for b in range(4)
        ]
        for t in range(2)
    ]
    for t in range(2):
        for b in range(4):
            lhs[t][block_of(b, t), :] = heads[rows_of(b, c, t), :]
    pump(5)
    for i in (6, 7):
        local[i].wait()
    for cp in wo_copies:
        cp.wait_recv()

    x1, x2, x3 = at(x, 1), at(x, 2), at(x, 3)

    class Sum:
        def __init__(self, part, from_left, from_right, sem):
            self.part, self.left, self.right, self.sem = part, from_left, from_right, sem

        def to_right(self, slot, block, role):
            go(remote(self.part(block, role), self.left(slot), self.sem(0, slot), self.sem(1, slot), x=x1))

        def to_left(self, slot, block, role):
            go(remote(self.part(block, role), self.right(slot), self.sem(2, slot), self.sem(3, slot), x=x3))

        def wait_left(self, slot):
            ref = self.left(slot)
            remote(ref, ref, self.sem(0, slot), self.sem(1, slot)).wait_recv()
            return ref[...].astype(F32)

        def wait_right(self, slot):
            ref = self.right(slot)
            remote(ref, ref, self.sem(2, slot), self.sem(3, slot)).wait_recv()
            return ref[...].astype(F32)

        def relayed(self):
            self.to_right(0, x2, 0)
            self.to_left(0, x2, 1)

        def direct(self):
            self.to_right(1, x1, 1)
            self.to_left(1, x3, 0)

        def merge(self):
            mine = self.part(x1, 0)
            mine[...] = (self.wait_left(0) + mine[...].astype(F32)).astype(BF16)
            self.to_right(2, x1, 0)
            mine = self.part(x3, 1)
            mine[...] = (self.wait_right(0) + mine[...].astype(F32)).astype(BF16)
            self.to_left(2, x3, 1)

        def result(self, role):
            a, b = (2, 1) if role == 0 else (1, 2)
            return self.part(x, role)[...].astype(F32) + self.wait_left(a) + self.wait_right(b)

    def mixed_sum(t):
        return Sum(
            lambda block, role: parts[t].at[block, role],
            lambda slot: left[t].at[slot], lambda slot: right[t].at[slot],
            lambda k, slot: rs_sem.at[t, k, slot],
        )

    mixed = [mixed_sum(0), mixed_sum(1)]

    def project(t):
        n = LOTS[t][1]
        for cp in hp_copies[t]:
            cp.wait_recv()
        mine, other = lhs[t][...], hpart[t][...]
        for role in range(2):
            for e in range(4):
                cols_e = pl.ds(role * H + e * 256, 256)
                acc = dot(mine, wo[c, :, cols_e]) + dot(other, wo[o, :, cols_e])
                parts[t][:, role, :, e * 256 : (e + 1) * 256] = acc.reshape(4, n, 256).astype(BF16)

    project(0)
    mixed[0].relayed()
    mixed[0].direct()
    project(1)
    mixed[1].relayed()
    pump(6)
    mixed[0].merge()
    mixed[1].direct()
    pump(7)
    mixed[1].merge()
    pump(8)
    local[5].wait()

    def norm(t):
        first, n = LOTS[t]
        wide = []
        for role in range(2):
            at_role = slice(role * H, role * H + H)
            m = (resv[first : first + n, at_role].astype(F32) + mixed[t].result(role)).astype(BF16)
            mid[t][:, at_role] = m
            wide.append(m.astype(F32))
        square = sum(jnp.sum(w * w, axis=1, keepdims=True) for w in wide)
        scale = lax.rsqrt(square * (1.0 / DM) + row_eps)
        for role in range(2):
            at_role = slice(role * H, role * H + H)
            ag[role, row_of(x, t), :] = (wide[role] * scale * gain_n[:, at_role]).astype(BF16)

    def ag_right(t, slot, block, role):
        ref = ag.at[role, row_of(block, t)]
        go(remote(ref, ref, ag_sem.at[t, 0, slot], ag_sem.at[t, 1, slot], x=x1))

    def ag_left(t, slot, block, role):
        ref = ag.at[role, row_of(block, t)]
        go(remote(ref, ref, ag_sem.at[t, 2, slot], ag_sem.at[t, 3, slot], x=x3))

    def ag_wait(t, side, slot, block, role):
        ref = ag.at[role, row_of(block, t)]
        remote(ref, ref, ag_sem.at[t, 0, slot], ag_sem.at[t, side, slot]).wait_recv()

    def ag_relay(t):
        ag_wait(t, 1, 0, x3, 0)
        ag_right(t, 2, x3, 0)
        ag_wait(t, 3, 0, x1, 1)
        ag_left(t, 2, x1, 1)

    def ag_rest(t):
        ag_wait(t, 1, 1, x3, 1)
        ag_wait(t, 3, 1, x1, 0)
        ag_wait(t, 1, 2, x2, 0)
        ag_wait(t, 3, 2, x2, 1)

    norm(0)
    ag_right(0, 0, x, 0)
    ag_left(0, 0, x, 1)
    ag_right(0, 1, x, 1)
    ag_left(0, 1, x, 0)
    pump(9)
    norm(1)
    ag_right(1, 0, x, 0)
    ag_left(1, 0, x, 1)
    pump(10)
    ag_relay(0)
    ag_right(1, 1, x, 1)
    ag_left(1, 1, x, 0)
    pump(11)
    ag_relay(1)
    pump(12)
    ag_rest(0)
    pump(13)
    ag_rest(1)
    for i in (8, 9, 10):
        local[i].wait()

    def lined_up(w, core, h, n0, n):
        pieces = [w[core, 2 * h + j // 4, j % 4, n0 : n0 + n, :] for j in range(8)]
        return jnp.concatenate(pieces, axis=1)

    def expand(core):
        for n0, n in ((0, 256), (256, 256), (512, 192)):
            gate = up = None
            for h in range(2):
                a = ag[h]
                w_gate = lined_up(wg, core, h, n0, n)
                w_up = lined_up(wu, core, h, n0, n)
                gate = dot_nt(a, w_gate) if gate is None else gate + dot_nt(a, w_gate)
                up = dot_nt(a, w_up) if up is None else up + dot_nt(a, w_up)
            hid[core, :, n0 : n0 + n] = (silu(gate) * up).astype(BF16)

    expand(c)
    pump(14)
    for name in ("G", "U"):
        for f in STEPS:
            for st in STEPS:
                pair_wait(name, f, st)
    expand(o)

    def rows_in(i, role):
        return role if i % 2 == 0 else 1 - role

    def down_sum(i):
        return Sum(
            lambda block, role: dparts[i][rows_in(i, role)].at[block],
            lambda slot: dleft[i][rows_in(i, slot % 2)].at[slot],
            lambda slot: dright[i][rows_in(i, 1 - slot % 2)].at[slot],
            lambda k, slot: rs2_sem.at[i, k, slot],
        )

    down = [down_sum(i) for i in range(5)]

    outgoing = []

    def finish(i):
        for role in range(2):
            t = rows_in(i, role)
            first, n = LOTS[t]
            total = down[i].result(role)
            for j, (rz, ry) in enumerate(COLUMNS[i]):
                at_j = pl.ds(pl.multiple_of((at(z, rz) * 4 + at(y, ry)) * 128, 128), 128)
                out[first : first + n, at_j] = (
                    mid[t][:, at_j].astype(F32) + total[:, 128 * j : 128 * j + 128]
                ).astype(BF16)
                place_j = (pl.ds(first, n), at_j)
                cp = pltpu.make_async_copy(out.at[place_j], out_hbm.at[place_j], out_sem.at[len(outgoing)])
                cp.start()
                outgoing.append(cp)

    for i in range(5):
        for rz, ry in COLUMNS[i]:
            for name in ("A", "B"):
                pair_wait(name, *place(name, rz, ry))
        for e in range(WIDTHS[i] // 256):
            acc = None
            for cc in range(2):
                w_down = jnp.concatenate(
                    [wd[cc, at(z, rz), at(y, ry)] for rz, ry in COLUMNS[i][2 * e : 2 * e + 2]], axis=1
                )
                acc = dot(hid[cc], w_down) if acc is None else acc + dot(hid[cc], w_down)
            for t, (first, n) in enumerate(LOTS):
                lot_acc = acc[4 * first : 4 * first + 4 * n].reshape(4, n, 256)
                dparts[i][t][:, :, e * 256 : (e + 1) * 256] = lot_acc.astype(BF16)
        down[i].relayed()
        for j in AFTER[i][0]:
            down[j].direct()
        for j in AFTER[i][1]:
            down[j].merge()
        pump(15 + i)
    down[2].merge()
    down[3].merge()
    down[4].merge()
    for i in range(5):
        finish(i)

    for cp in outgoing:
        cp.wait()
    for cp in pending:
        cp.wait_send()


def on_device(
    residual, small_value_inputs, large_value_inputs, small_gate_inputs, large_gate_inputs,
    state_projections, small_step_inputs, large_step_inputs, small_decay_offsets,
    large_decay_offsets, small_decay_rates, large_decay_rates, small_filter_taps,
    large_filter_taps, state_filter_taps, small_head_gains, large_head_gains,
    small_output_projection, large_output_projection, channel_norm_gain, gate_matrix,
    up_matrix, down_matrix,
):
    flat = state_projections.reshape(4 * T, 128)

    anywhere = pl.BlockSpec(memory_space=pl.ANY)
    dma = pltpu.SemaphoreType.DMA
    V = pltpu.VMEM
    return pl.pallas_call(
        kernel,
        out_shape=jax.ShapeDtypeStruct((R, DM), BF16),
        in_specs=[anywhere] * 23,
        out_specs=anywhere,
        scratch_shapes=[
            [
                V((2, T), BF16), V((1, T), BF16), V((2, T), F32), V((1, T), F32), V((1, 2), F32), V((1, 1), F32),
                V((4, 128), BF16), V((4, 128), BF16), V((4, 4, 128), BF16), V((1, 128), F32), V((1, 128), F32),
                V((1, DM), F32),
            ],
            V((R, DM), BF16),
            dma((32,)),
            V((T, 256), BF16),
            V((4 * T, 128), BF16),
            V((T, 256), BF16),
            V((R, DM), BF16),
            V((16, 256), BF16),
            V((64, 128), BF16),
            V((T + 8, 256), F32),
            V((4 * T + 32, 128), F32),
            V((T, 512), BF16),
            V((T, 256), BF16),
            V((NB, 128, 256), F32),
            V((T, 256), F32),
            V((T, 256), BF16),
            *[V((4 * n, 256), BF16) for _, n in LOTS],
            *[V((4 * n, 256), BF16) for _, n in LOTS],
            V((2, 256, DM), BF16),
            V((2, 4, 4, FD, KROWS), BF16),
            V((2, 4, 4, FD, KROWS), BF16),
            V((2, 4, 4, FD, KROWS), BF16),
            V((2, 4, 136, 128), BF16),
            V((2, 4, 136, 128), BF16),
            *[V((4, 2, n, H), BF16) for _, n in LOTS],
            *[V((3, n, H), BF16) for _, n in LOTS],
            *[V((3, n, H), BF16) for _, n in LOTS],
            V((2, 4 * R, H), BF16),
            V((2, 4 * R, FD), BF16),
            [[V((4, n, w), BF16) for _, n in LOTS] for w in WIDTHS],
            [[V((3, n, w), BF16) for _, n in LOTS] for w in WIDTHS],
            [[V((3, n, w), BF16) for _, n in LOTS] for w in WIDTHS],
            *[V((n, DM), BF16) for _, n in LOTS],
            dma((23,)),
            dma((2, 3)),
            dma((60,)),
            dma((4, 4, 4)),
            dma((2, 64)),
            dma((4, 2, 4)),
            dma((2, 10)),
            dma((2, 4, 3)),
            dma((2, 4, 3)),
            dma((5, 4, 3)),
        ],
        compiler_params=pltpu.CompilerParams(
            collective_id=0, has_side_effects=True, vmem_limit_bytes=60 * 1024 * 1024
        ),
    )(
        residual, small_value_inputs, large_value_inputs, small_gate_inputs, large_gate_inputs,
        flat, small_output_projection, large_output_projection, gate_matrix.T, up_matrix.T, down_matrix,
        small_step_inputs.T, large_step_inputs.T, small_decay_offsets.T, large_decay_offsets.T,
        small_decay_rates.reshape(1, 2), large_decay_rates.reshape(1, 1), small_filter_taps, large_filter_taps, state_filter_taps,
        small_head_gains.reshape(1, 128), large_head_gains.reshape(1, 128),
        channel_norm_gain.reshape(1, DM),
    )


def solution(mesh):
    split = Mesh(mesh.devices.reshape(4, 4, 4, 2), ("z", "y", "x", "c"))
    in_specs = (
        P(SP_TP, None),
        P(SP, TP),
        P(SP, TP),
        P(SP, TP),
        P(SP, TP),
        P(SP, None, None),
        P(SP, TP),
        P(SP, TP),
        P(SP, TP),
        P(SP, TP),
        P(TP),
        P(TP),
        P(None, TP),
        P(None, TP),
        P(),
        P(TP),
        P(TP),
        P(TP, None),
        P(TP, None),
        P(),
        P(SP, TP),
        P(SP, TP),
        P(TP, SP),
    )
    return jax.shard_map(
        on_device, mesh=split, in_specs=in_specs, out_specs=P(SP_TP, None), check_vma=False
    )
```

```python
import functools

import jax
import jax.numpy as jnp
from jax import lax
from jax.experimental import pallas as pl
from jax.experimental.pallas import tpu as pltpu
from jax.sharding import Mesh
from jax.sharding import PartitionSpec as P

F32 = jnp.float32
BF16 = jnp.bfloat16
SP = ("z", "y")
TP = ("x", "c")
SP_TP = ("z", "y", "x", "c")

T = 640
L = 128
NB = T // L
R = 80
FD = 704
DM = 2048
H = 1024
KROWS = 128
CUT = 352
AFTER = (((0,), (), ()), ((1,), (), (15,)), ((2,), (0,), (16, 17)), ((), (1,), ()), ((3, 4), (), (18, 19)))
WIDTHS = (512, 256, 512, 512, 256)
LOTS = ((0, 48), (48, 32))
STEPS = (0, 1, -1, 2)
COLUMNS = (
    ((0, 0), (-1, 0), (0, -1), (0, 1)),
    ((1, 0), (-1, -1)),
    ((1, 1), (0, 2), (2, 0), (-1, 1)),
    ((1, -1), (2, 1), (1, 2), (-1, 2)),
    ((2, -1), (2, 2)),
)
SENDS = (
    ((0, 0, 0, 0, 1), (0, 0, 0, 0, -1), (1, 0, 0, 0, 1), (1, 0, 0, 0, -1), (0, 0, 0, 1, 1), (0, 0, 0, 1, -1)),
    ((1, 0, 0, 1, -1),),
    ((1, 0, 0, 1, 1),),
    ((0, 1, 0, 0, -1), (1, 1, 0, 0, -1), (0, 1, 0, 1, 1), (1, 1, 0, 1, 1)),
    ((1, 1, 0, 1, -1), (0, 1, 0, 1, -1)),
    ((0, -1, 0, 1, 1), (1, -1, 0, 1, 1), (1, -1, 0, 1, -1)),
    ((0, 2, 0, 1, -1), (0, 2, 0, 1, 1), (1, 2, 0, 1, 1), (1, 2, 0, 1, -1)),
    ((0, -1, 0, 1, -1), (3, 0, 0, 0, 1), (2, 0, 0, 0, 1)),
    ((2, 0, 0, 0, -1), (3, 0, 0, 0, -1), (0, 0, -1, 1, 1), (0, 2, 1, 1, -1), (1, 0, -1, 1, 1), (1, 1, 1, 1, -1)),
    ((1, 2, -1, 1, 1), (0, 1, -1, 1, 1)),
    ((2, 1, 0, 0, -1), (3, 1, 0, 0, -1)),
    ((1, -1, 1, 1, -1), (0, -1, 1, 1, -1), (2, 0, 0, 1, 1), (3, 0, 0, 1, 1), (2, 1, 0, 1, 1)),
    ((3, 0, 0, 1, -1), (2, 0, 0, 1, -1), (3, 1, 0, 1, 1), (2, -1, 0, 1, 1), (3, -1, 0, 1, 1)),
    ((3, 2, 0, 1, -1), (2, 2, 0, 1, -1), (2, 2, 0, 1, 1), (3, 2, 0, 1, 1), (3, 1, 0, 1, -1), (2, 1, 0, 1, -1), (3, -1, 0, 1, -1)),
    ((2, -1, 0, 1, -1), (2, 0, -1, 1, 1), (3, 0, -1, 1, 1), (2, 1, -1, 1, 1), (3, 1, -1, 1, 1)),
    ((2, 2, 1, 1, -1), (3, 2, 1, 1, -1), (2, -1, -1, 1, 1), (3, -1, -1, 1, 1)),
    (),
    (),
    (),
    (),
)
SHARES = (
    ((0, 0, 0), (1, 0, 0), (2, 0, 0), (3, 0, 0)),
    (),
    ((0, -1, 0), (0, 1, 0), (1, -1, 0), (1, 1, 0)),
    (),
    ((0, 0, -1), (0, 0, 1)),
    ((1, 0, 1),),
    ((1, 0, -1), (0, 2, 0), (1, 2, 0)),
    ((0, 1, -1), (1, 1, -1), (1, 1, 1), (0, 1, 1)),
    ((0, -1, -1), (1, -1, -1), (1, -1, 1), (0, 2, 1)),
    ((0, 2, -1), (1, 2, -1)),
    ((1, 2, 1), (0, -1, 1), (3, -1, 0), (2, -1, 0), (2, 1, 0), (3, 1, 0)),
    (),
    ((0, 0, 2), (1, 0, 2), (1, 1, 2), (0, 2, 2)),
    ((2, 2, 0), (3, 2, 0), (0, 1, 2), (1, 2, 2), (1, -1, 2), (0, -1, 2)),
    ((2, 0, -1), (3, 0, -1), (2, 1, -1), (3, 1, -1), (3, 0, 1), (2, 0, 1), (2, -1, -1), (3, -1, -1)),
    ((3, 2, 1), (2, 2, 1), (2, 2, -1), (3, 2, -1), (3, 1, 1), (2, 1, 1), (2, 0, 2), (3, 0, 2), (3, -1, 1)),
    ((2, -1, 1), (2, 1, 2), (3, 1, 2), (3, -1, 2)),
    ((2, 2, 2), (3, 2, 2), (2, -1, 2)),
    (),
    (),
)

head_eps = 1e-05
row_eps = 1e-06


def silu(x):
    return x / (1.0 + jnp.exp(-x))


def dot(a, b):
    return jnp.dot(a, b, preferred_element_type=F32)


def dot_nt(a, b):
    return lax.dot_general(a, b, (((1,), (1,)), ((), ())), preferred_element_type=F32)


def dot_tn(a, b):
    return lax.dot_general(a, b, (((0,), (0,)), ((), ())), preferred_element_type=F32)


def kernel(
    res_in, vs_in, vl_in, gs_in, gl_in, sp_in, ws_in, wl_in, g_in, u_in, d_in,
    small_in_0, small_in_1, small_in_2, small_in_3, small_in_4, small_in_5, small_in_6, small_in_7,
    small_in_8, small_in_9, small_in_10, small_in_11,
    out,
    small,
    xin, sxin, gin, resv, halo, halo_m, cbuf, cmaps, conv_k, drive, fresh, inner, heads, hpart_0, hpart_1, lhs_0, lhs_1,
    wo, wg, wu, wd, st1, st2, parts_0, parts_1, left_0, left_1, right_0, right_1, ag, hid,
    dparts, dleft, dright, mid_0, mid_1,
    loc_sem, halo_sem, w_send, w_recv, pair_sem, st_sem, hp_sem, rs_sem, ag_sem, rs2_sem,
):
    z, y, x, c = (lax.axis_index(n) for n in ("z", "y", "x", "c"))
    rem = lax.rem
    o = 1 - c

    def at(base, by):
        return rem(base + (by % 4), 4)

    nxt = {"z": rem(z + lax.div(y + 1, 4), 4), "y": rem(y + 1, 4)}
    prv = {"z": rem(z + 3 + lax.div(y + 3, 4), 4), "y": rem(y + 3, 4)}

    def there(**kw):
        base = {"z": z, "y": y, "x": x, "c": c}
        base.update(kw)
        return (base["z"], base["y"], base["x"], base["c"])

    def remote(src, dst, send, recv, **kw):
        return pltpu.make_async_remote_copy(
            src_ref=src, dst_ref=dst, send_sem=send, recv_sem=recv,
            device_id=there(**kw), device_id_type=pl.DeviceIdType.MESH,
        )

    pending = []

    def go(cp):
        cp.start()
        pending.append(cp)
        return cp

    barrier = pltpu.get_barrier_semaphore()
    peers = [
        dict(c=o), dict(x=at(x, 1)), dict(x=at(x, 3)),
        dict(y=at(y, 1)), dict(y=at(y, 2)), dict(y=at(y, 3)),
        dict(z=at(z, 1)), dict(z=at(z, 2)), dict(z=at(z, 3)),
        nxt, prv,
    ]
    for p in peers:
        pl.semaphore_signal(barrier, inc=1, device_id=there(**p), device_id_type=pl.DeviceIdType.MESH)
    local = [
        *zip(
            (small_in_0, small_in_1, small_in_2, small_in_3, small_in_4, small_in_5, small_in_6,
             small_in_7, small_in_8, small_in_9, small_in_10, small_in_11), small,
        ),
        (vs_in, xin.at[:, pl.ds(0, 128)]),
        (vl_in, xin.at[:, pl.ds(128, 128)]),
        (sp_in, sxin),
        (gs_in, gin.at[:, pl.ds(0, 128)]),
        (gl_in, gin.at[:, pl.ds(128, 128)]),
        (res_in, resv),
        (ws_in, wo.at[c, pl.ds(0, 128)]),
        (wl_in, wo.at[c, pl.ds(128, 128)]),
        (g_in, wg.at[c, z, y]),
        (u_in, wu.at[c, z, y]),
        (d_in, wd.at[c, z, y]),
    ]
    local = [pltpu.make_async_copy(a, b, loc_sem.at[i]) for i, (a, b) in enumerate(local)]
    for cp in local:
        cp.start()
    fetched, local = local[:12], local[12:]
    steps_s, steps_l, offs_s, offs_l, rates_s, rates_l, taps_s, taps_l, taps_m, gain_s, gain_l, gain_n = small

    pl.semaphore_wait(barrier, len(peers))

    tail = pl.ds(T - 16, 16)
    halos = [
        go(remote(src, dst, halo_sem.at[0, i], halo_sem.at[1, i], **nxt))
        for i, (src, dst) in enumerate((
            (vs_in.at[tail], halo.at[:, pl.ds(0, 128)]),
            (vl_in.at[tail], halo.at[:, pl.ds(128, 128)]),
            (sp_in.at[pl.ds(4 * T - 64, 64)], halo_m),
        ))
    ]

    names = ("G", "U", "A", "B")
    own_src = {
        "G": g_in, "U": u_in,
        "A": d_in.at[pl.ds(0, CUT)], "B": d_in.at[pl.ds(CUT, CUT)],
    }

    def unit(name, rz, ry, core):
        zz, yy = at(z, rz), at(y, ry)
        if name == "G":
            return wg.at[core, zz, yy]
        if name == "U":
            return wu.at[core, zz, yy]
        rows = pl.ds(0, CUT) if name == "A" else pl.ds(CUT, CUT)
        return wd.at[core, zz, yy, rows]

    def place(name, f, s):
        return (f, s) if name in ("U", "B") else (s, f)

    def source(name, f, s):
        return own_src[name] if (f, s) == (0, 0) else unit(name, *place(name, f, s), c)

    def w_sem(name, rz, ry):
        return w_recv.at[names.index(name), rz % 4, ry % 4]

    n_sent = [0]
    here = {(n, 0, 0) for n in names}

    def w_wait(name, f, s):
        if (name, f, s) not in here:
            here.add((name, f, s))
            ref = unit(name, *place(name, f, s), c)
            remote(ref, ref, w_send.at[0], w_sem(name, *place(name, f, s))).wait_recv()

    def w_go(name, f, s, second, step):
        w_wait(name, f, s)
        dz, dy = place(name, 0, step) if second else place(name, step, 0)
        rz, ry = place(name, f, s)
        k = n_sent[0]
        n_sent[0] += 1
        go(remote(
            source(name, f, s), unit(name, rz, ry, c), w_send.at[k], w_sem(name, rz - dz, ry - dy),
            z=at(z, dz), y=at(y, dy),
        ))

    pair_index = {}

    def share(name, f, s):
        w_wait(name, f, s)
        k = pair_index.setdefault((name, f, s), len(pair_index))
        go(remote(
            source(name, f, s), unit(name, *place(name, f, s), c),
            pair_sem.at[0, k], pair_sem.at[1, k], c=o,
        ))

    def pair_wait(name, f, s):
        k = pair_index[(name, f, s)]
        ref = unit(name, *place(name, f, s), o)
        remote(ref, ref, pair_sem.at[0, k], pair_sem.at[1, k], c=o).wait_recv()

    def pump(i):
        for n, f, s, second, step in SENDS[i]:
            w_go(names[n], f, s, second, step)
        for n, f, s in SHARES[i]:
            share(names[n], f, s)

    pump(0)

    wo_copies = [
        go(remote(src, wo.at[c, rows], hp_sem.at[0, 8 + i], hp_sem.at[1, 8 + i], c=o))
        for i, (src, rows) in enumerate(((ws_in, pl.ds(0, 128)), (wl_in, pl.ds(128, 128))))
    ]

    for cp in fetched:
        cp.wait()
    lane = lax.broadcasted_iota(jnp.int32, (8, L), 1)
    rows = []
    both = []
    row8 = lax.broadcasted_iota(jnp.int32, (8, L), 0)
    raw_steps = jnp.concatenate([steps_s[...].astype(F32), steps_l[...].astype(F32)], axis=0)
    softened = jnp.maximum(raw_steps, 0.0) + jnp.log1p(jnp.exp(-jnp.abs(raw_steps)))
    head = lax.broadcasted_iota(jnp.int32, (3, T), 0)
    rate = jnp.where(head == 0, rates_s[0:1, 0:1], jnp.where(head == 1, rates_s[0:1, 1:2], rates_l[0:1, 0:1]))
    offsets = jnp.concatenate([offs_s[...], offs_l[...]], axis=0)
    meta = jnp.concatenate(
        [offsets - jnp.exp(rate) * softened, softened, jnp.zeros((2, T), F32)], axis=0
    )
    for k in range(NB):
        raw = meta[:, k * L : (k + 1) * L]
        acc = raw
        for sft in (1, 2, 4, 8, 16, 32, 64):
            acc = acc + jnp.where(lane >= sft, pltpu.roll(acc, sft, 1), 0.0)
        rows.append(acc)
        both.append(jnp.where(row8 < 3, acc, raw))
    both.append(jnp.zeros((L - 8 * NB, L), F32))
    cols = jnp.concatenate(both, axis=0).T
    grown = jnp.exp(cols)
    shrunk = jnp.exp(cols[L - 1 : L, :] - cols)

    half = lax.broadcasted_iota(jnp.int32, (L, L), 1) < 64
    half1 = lax.broadcasted_iota(jnp.int32, (1, L), 1) < 64

    def spread(m, k, off):
        b = 8 * k + off
        small = jnp.where(half, m[:, b : b + 1], m[:, b + 1 : b + 2])
        large = jnp.broadcast_to(m[:, b + 2 : b + 3], (L, L))
        return small, large

    def block_decay(k):
        b = 8 * k
        e = grown[L - 1 : L]
        small = jnp.where(half1, e[:, b : b + 1], e[:, b + 1 : b + 2])
        large = jnp.broadcast_to(e[:, b + 2 : b + 3], (1, L))
        return jnp.concatenate([small, large], axis=1)

    tap_rows = []
    for j in range(4):
        m = taps_m[j].astype(F32)
        tap_rows.append(
            [taps_s[j : j + 1].astype(F32), taps_l[j : j + 1].astype(F32)]
            + [m[i : i + 1] for i in range(4)]
        )

    def conv(k, g):
        total = None
        for j in range(4):
            row = k * L + 5 + j
            if g < 2:
                rows_j = cbuf[row : row + L, g * 128 : g * 128 + 128]
            else:
                rows_j = cmaps[pl.ds(4 * row + g - 2, L, 4), :]
            part = tap_rows[j][g] * rows_j
            total = part if total is None else total + part
        return silu(total)

    for i in range(3):
        local[i].wait()
    for k in range(NB):
        cbuf[8 + k * L : 8 + (k + 1) * L, :] = xin[k * L : (k + 1) * L, :].astype(F32)
        maps_k = pl.ds(32 + 4 * k * L, 4 * L)
        cmaps[maps_k, :] = sxin[4 * k * L : 4 * (k + 1) * L, :].astype(F32)
    decays = [block_decay(k) for k in range(NB)]

    def first_pass(k, kind):
        dt, sh = spread(cols, k, 3)[kind], spread(shrunk, k, 0)[kind]
        blk, at_kind = pl.ds(k * L, L), pl.ds(kind * 128, 128)
        d = conv(k, kind) * dt
        drive[blk, at_kind] = d.astype(BF16)
        key = conv(k, 2 + 2 * kind).astype(BF16)
        conv_k[blk, 256 * kind : 256 * kind + 128] = key
        conv_k[blk, 256 * kind + 128 : 256 * kind + 256] = conv(k, 3 + 2 * kind).astype(BF16)
        fresh[k, :, at_kind] = dot_tn(key, (d * sh).astype(BF16))

    for kind in range(2):
        for k in range(1, NB):
            first_pass(k, kind)
    for cp in halos:
        cp.wait_recv()
    start = jnp.where(jnp.logical_and(z == 0, y == 0), 0.0, 1.0)
    cbuf[0:8, :] = halo[8:16, :].astype(F32) * start
    cmaps[0:32, :] = halo_m[32:64, :].astype(F32) * start

    def state_out(buf, kind, state, total, stage, **axis):
        buf[kind, 0, 0:128] = state.astype(BF16)
        buf[kind, 0, 128:136] = jnp.broadcast_to(total, (8, 128)).astype(BF16)
        ((name, me),) = axis.items()
        copies = [
            remote(
                buf.at[kind, 0], buf.at[kind, r],
                st_sem.at[2 * stage, kind, r], st_sem.at[2 * stage + 1, kind, r],
                **{name: at(me, r)},
            )
            for r in (1, 2, 3)
        ]
        pending.extend(copies)
        return copies

    def start_all(copies):
        for cp in copies:
            cp.start()

    def states_in(buf, kind, stage):
        for r in (1, 2, 3):
            remote(
                buf.at[kind, 0], buf.at[kind, r],
                st_sem.at[2 * stage, kind, r], st_sem.at[2 * stage + 1, kind, r],
            ).wait_recv()

    def chained(buf, kind, me):
        line, line_d = jnp.zeros((128, 128), F32), jnp.ones((1, 128), F32)
        before, before_d = line, line_d
        for j in range(4):
            blob = buf[kind, rem(me - j + 4, 4)].astype(F32)
            line = line * blob[128:129] + blob[0:128]
            line_d = line_d * blob[128:129]
            before = jnp.where(j < me, line, before)
            before_d = jnp.where(j < me, line_d, before_d)
        return before, before_d, line, line_d

    later = []
    for kind in range(2):
        first_pass(0, kind)
        own = slice(kind * 128, kind * 128 + 128)
        state, total = fresh[0, :, own], decays[0][:, own]
        for k in range(1, NB):
            state = state * decays[k][:, own] + fresh[k, :, own]
            total = total * decays[k][:, own]
        copies = state_out(st1, kind, state, total, 0, y=y)
        pl.when(c == 0)(functools.partial(start_all, copies))
        later += copies

    mask = lax.broadcasted_iota(jnp.int32, (L, L), 0) >= lax.broadcasted_iota(jnp.int32, (L, L), 1)

    def weights_of(k, h):
        b = 8 * k + h
        diff = cols[:, b : b + 1] - rows[k][h : h + 1, :]
        return jnp.exp(jnp.where(mask, diff, -1e30))

    def second_pass(k):
        blk = pl.ds(k * L, L)
        s_s = dot_nt(conv_k[blk, 128:256], conv_k[blk, 0:128])
        s_l = dot_nt(conv_k[blk, 384:512], conv_k[blk, 256:384])
        d_s = drive[blk, 0:128]
        o_0 = dot((s_s * weights_of(k, 0)).astype(BF16), d_s)
        o_1 = dot((s_s * weights_of(k, 1)).astype(BF16), d_s)
        inner[blk, 0:128] = jnp.where(half, o_0, o_1)
        inner[blk, 128:256] = dot((s_l * weights_of(k, 2)).astype(BF16), drive[blk, 128:256])

    for k in range(NB):
        second_pass(k)
    pl.when(c == 1)(functools.partial(start_all, later))
    pump(1)
    inside = []
    for kind in range(2):
        states_in(st1, kind, 0)
        before, before_d, line, line_d = chained(st1, kind, y)
        inside.append((before, before_d))
        start_all(state_out(st2, kind, line, line_d, 1, z=z))
        if kind == 0:
            pump(2)
    pump(3)

    for i in (3, 4):
        local[i].wait()

    def third_pass(k, kind, carry):
        blk, cols_k = pl.ds(k * L, L), pl.ds(kind * 128, 128)
        own = slice(kind * 128, kind * 128 + 128)
        reads = conv_k[blk, 256 * kind + 128 : 256 * kind + 256]
        out_k = inner[blk, cols_k] + dot(reads, carry.astype(BF16)) * spread(grown, k, 0)[kind]
        carry = carry * decays[k][:, own] + fresh[k, :, own]
        out_k = out_k * silu(gin[blk, cols_k].astype(F32))
        sq = out_k * out_k
        if kind == 0:
            sq_0 = jnp.sum(jnp.where(half, sq, 0.0), axis=1, keepdims=True)
            sq_1 = jnp.sum(jnp.where(half, 0.0, sq), axis=1, keepdims=True)
            mean = jnp.where(half, sq_0, sq_1) * (1.0 / 64)
            gain = gain_s[...]
        else:
            mean = jnp.sum(sq, axis=1, keepdims=True) * (1.0 / 128)
            gain = gain_l[...]
        heads[blk, cols_k] = (out_k * lax.rsqrt(mean + head_eps) * gain).astype(BF16)
        return carry

    for kind in range(2):
        states_in(st2, kind, 1)
        before = chained(st2, kind, z)[0]
        carry = before * inside[kind][1] + inside[kind][0]
        for k in range(NB):
            carry = third_pass(k, kind, carry)
        if kind == 0:
            pump(4)

    hpart, lhs = (hpart_0, hpart_1), (lhs_0, lhs_1)
    parts, left, right = (parts_0, parts_1), (left_0, left_1), (right_0, right_1)
    mid = (mid_0, mid_1)

    def rows_of(b, core, t):
        first, n = LOTS[t]
        return pl.ds(pl.multiple_of((2 * b + core) * R + first, 16), n)

    def block_of(b, t):
        n = LOTS[t][1]
        return pl.ds(b * n if isinstance(b, int) else pl.multiple_of(b * n, 16), n)

    def row_of(b, t):
        first, n = LOTS[t]
        return pl.ds(pl.multiple_of(4 * first + b * n, 16), n)

    hp_copies = [
        [
            go(remote(
                heads.at[rows_of(b, o, t)], hpart[t].at[block_of(b, t)],
                hp_sem.at[0, 4 * t + b], hp_sem.at[1, 4 * t + b], c=o,
            ))
            for b in range(4)
        ]
        for t in range(2)
    ]
    for t in range(2):
        for b in range(4):
            lhs[t][block_of(b, t), :] = heads[rows_of(b, c, t), :]
    pump(5)
    for i in (6, 7):
        local[i].wait()
    for cp in wo_copies:
        cp.wait_recv()

    x1, x2, x3 = at(x, 1), at(x, 2), at(x, 3)

    class Sum:
        def __init__(self, part, from_left, from_right, sem):
            self.part, self.left, self.right, self.sem = part, from_left, from_right, sem

        def to_right(self, slot, block, role):
            go(remote(self.part(block, role), self.left(slot), self.sem(0, slot), self.sem(1, slot), x=x1))

        def to_left(self, slot, block, role):
            go(remote(self.part(block, role), self.right(slot), self.sem(2, slot), self.sem(3, slot), x=x3))

        def wait_left(self, slot):
            ref = self.left(slot)
            remote(ref, ref, self.sem(0, slot), self.sem(1, slot)).wait_recv()
            return ref[...].astype(F32)

        def wait_right(self, slot):
            ref = self.right(slot)
            remote(ref, ref, self.sem(2, slot), self.sem(3, slot)).wait_recv()
            return ref[...].astype(F32)

        def relayed(self):
            self.to_right(0, x2, 0)
            self.to_left(0, x2, 1)

        def direct(self):
            self.to_right(1, x1, 1)
            self.to_left(1, x3, 0)

        def merge(self):
            mine = self.part(x1, 0)
            mine[...] = (self.wait_left(0) + mine[...].astype(F32)).astype(BF16)
            self.to_right(2, x1, 0)
            mine = self.part(x3, 1)
            mine[...] = (self.wait_right(0) + mine[...].astype(F32)).astype(BF16)
            self.to_left(2, x3, 1)

        def result(self, role):
            a, b = (2, 1) if role == 0 else (1, 2)
            return self.part(x, role)[...].astype(F32) + self.wait_left(a) + self.wait_right(b)

    def mixed_sum(t):
        return Sum(
            lambda block, role: parts[t].at[block, role],
            lambda slot: left[t].at[slot], lambda slot: right[t].at[slot],
            lambda k, slot: rs_sem.at[t, k, slot],
        )

    mixed = [mixed_sum(0), mixed_sum(1)]

    def project(t):
        n = LOTS[t][1]
        for cp in hp_copies[t]:
            cp.wait_recv()
        mine, other = lhs[t][...], hpart[t][...]
        for role in range(2):
            for e in range(4):
                cols_e = pl.ds(role * H + e * 256, 256)
                acc = dot(mine, wo[c, :, cols_e]) + dot(other, wo[o, :, cols_e])
                parts[t][:, role, :, e * 256 : (e + 1) * 256] = acc.reshape(4, n, 256).astype(BF16)

    project(0)
    mixed[0].relayed()
    mixed[0].direct()
    project(1)
    mixed[1].relayed()
    pump(6)
    mixed[0].merge()
    mixed[1].direct()
    pump(7)
    mixed[1].merge()
    pump(8)
    local[5].wait()

    def norm(t):
        first, n = LOTS[t]
        wide = []
        for role in range(2):
            at_role = slice(role * H, role * H + H)
            m = (resv[first : first + n, at_role].astype(F32) + mixed[t].result(role)).astype(BF16)
            mid[t][:, at_role] = m
            wide.append(m.astype(F32))
        square = sum(jnp.sum(w * w, axis=1, keepdims=True) for w in wide)
        scale = lax.rsqrt(square * (1.0 / DM) + row_eps)
        for role in range(2):
            at_role = slice(role * H, role * H + H)
            ag[role, row_of(x, t), :] = (wide[role] * scale * gain_n[:, at_role]).astype(BF16)

    def ag_right(t, slot, block, role):
        ref = ag.at[role, row_of(block, t)]
        go(remote(ref, ref, ag_sem.at[t, 0, slot], ag_sem.at[t, 1, slot], x=x1))

    def ag_left(t, slot, block, role):
        ref = ag.at[role, row_of(block, t)]
        go(remote(ref, ref, ag_sem.at[t, 2, slot], ag_sem.at[t, 3, slot], x=x3))

    def ag_wait(t, side, slot, block, role):
        ref = ag.at[role, row_of(block, t)]
        remote(ref, ref, ag_sem.at[t, 0, slot], ag_sem.at[t, side, slot]).wait_recv()

    def ag_relay(t):
        ag_wait(t, 1, 0, x3, 0)
        ag_right(t, 2, x3, 0)
        ag_wait(t, 3, 0, x1, 1)
        ag_left(t, 2, x1, 1)

    def ag_rest(t):
        ag_wait(t, 1, 1, x3, 1)
        ag_wait(t, 3, 1, x1, 0)
        ag_wait(t, 1, 2, x2, 0)
        ag_wait(t, 3, 2, x2, 1)

    norm(0)
    ag_right(0, 0, x, 0)
    ag_left(0, 0, x, 1)
    ag_right(0, 1, x, 1)
    ag_left(0, 1, x, 0)
    pump(9)
    norm(1)
    ag_right(1, 0, x, 0)
    ag_left(1, 0, x, 1)
    pump(10)
    ag_relay(0)
    ag_right(1, 1, x, 1)
    ag_left(1, 1, x, 0)
    pump(11)
    ag_relay(1)
    pump(12)
    ag_rest(0)
    pump(13)
    ag_rest(1)
    for i in (8, 9, 10):
        local[i].wait()

    def lined_up(w, core, h, n0, n):
        pieces = [w[core, 2 * h + j // 4, j % 4, n0 : n0 + n, :] for j in range(8)]
        return jnp.concatenate(pieces, axis=1)

    def expand(core):
        for n0, n in ((0, 256), (256, 256), (512, 192)):
            gate = up = None
            for h in range(2):
                a = ag[h]
                w_gate = lined_up(wg, core, h, n0, n)
                w_up = lined_up(wu, core, h, n0, n)
                gate = dot_nt(a, w_gate) if gate is None else gate + dot_nt(a, w_gate)
                up = dot_nt(a, w_up) if up is None else up + dot_nt(a, w_up)
            hid[core, :, n0 : n0 + n] = (silu(gate) * up).astype(BF16)

    expand(c)
    pump(14)
    for name in ("G", "U"):
        for f in STEPS:
            for st in STEPS:
                pair_wait(name, f, st)
    expand(o)

    def rows_in(i, role):
        return role if i % 2 == 0 else 1 - role

    def down_sum(i):
        return Sum(
            lambda block, role: dparts[i][rows_in(i, role)].at[block],
            lambda slot: dleft[i][rows_in(i, slot % 2)].at[slot],
            lambda slot: dright[i][rows_in(i, 1 - slot % 2)].at[slot],
            lambda k, slot: rs2_sem.at[i, k, slot],
        )

    down = [down_sum(i) for i in range(5)]

    def finish(i):
        for role in range(2):
            t = rows_in(i, role)
            first, n = LOTS[t]
            total = down[i].result(role)
            for j, (rz, ry) in enumerate(COLUMNS[i]):
                at_j = pl.ds(pl.multiple_of((at(z, rz) * 4 + at(y, ry)) * 128, 128), 128)
                out[first : first + n, at_j] = (
                    mid[t][:, at_j].astype(F32) + total[:, 128 * j : 128 * j + 128]
                ).astype(BF16)

    for i in range(5):
        if i == 2:
            settled = len(pending)
        for rz, ry in COLUMNS[i]:
            for name in ("A", "B"):
                pair_wait(name, *place(name, rz, ry))
        for e in range(WIDTHS[i] // 256):
            acc = None
            for cc in range(2):
                w_down = jnp.concatenate(
                    [wd[cc, at(z, rz), at(y, ry)] for rz, ry in COLUMNS[i][2 * e : 2 * e + 2]], axis=1
                )
                acc = dot(hid[cc], w_down) if acc is None else acc + dot(hid[cc], w_down)
            for t, (first, n) in enumerate(LOTS):
                lot_acc = acc[4 * first : 4 * first + 4 * n].reshape(4, n, 256)
                dparts[i][t][:, :, e * 256 : (e + 1) * 256] = lot_acc.astype(BF16)
        down[i].relayed()
        for j in AFTER[i][0]:
            down[j].direct()
        for j in AFTER[i][1]:
            down[j].merge()
        for j in AFTER[i][2]:
            pump(j)
    down[2].merge()
    for cp in pending[:settled]:
        cp.wait_send()
    del pending[:settled]
    down[3].merge()
    down[4].merge()
    for i in range(5):
        finish(i)

    for cp in pending:
        cp.wait_send()


def on_device(
    residual, small_value_inputs, large_value_inputs, small_gate_inputs, large_gate_inputs,
    state_projections, small_step_inputs, large_step_inputs, small_decay_offsets,
    large_decay_offsets, small_decay_rates, large_decay_rates, small_filter_taps,
    large_filter_taps, state_filter_taps, small_head_gains, large_head_gains,
    small_output_projection, large_output_projection, channel_norm_gain, gate_matrix,
    up_matrix, down_matrix,
):
    flat = state_projections.reshape(4 * T, 128)

    anywhere = pl.BlockSpec(memory_space=pl.ANY)
    dma = pltpu.SemaphoreType.DMA
    V = pltpu.VMEM
    return pl.pallas_call(
        kernel,
        out_shape=pltpu.VMEM((R, DM), BF16),
        in_specs=[anywhere] * 23,
        out_specs=pl.BlockSpec(memory_space=pltpu.VMEM),
        scratch_shapes=[
            [
                V((2, T), BF16), V((1, T), BF16), V((2, T), F32), V((1, T), F32), V((1, 2), F32), V((1, 1), F32),
                V((4, 128), BF16), V((4, 128), BF16), V((4, 4, 128), BF16), V((1, 128), F32), V((1, 128), F32),
                V((1, DM), F32),
            ],
            V((T, 256), BF16),
            V((4 * T, 128), BF16),
            V((T, 256), BF16),
            V((R, DM), BF16),
            V((16, 256), BF16),
            V((64, 128), BF16),
            V((T + 8, 256), F32),
            V((4 * T + 32, 128), F32),
            V((T, 512), BF16),
            V((T, 256), BF16),
            V((NB, 128, 256), F32),
            V((T, 256), F32),
            V((T, 256), BF16),
            *[V((4 * n, 256), BF16) for _, n in LOTS],
            *[V((4 * n, 256), BF16) for _, n in LOTS],
            V((2, 256, DM), BF16),
            V((2, 4, 4, FD, KROWS), BF16),
            V((2, 4, 4, FD, KROWS), BF16),
            V((2, 4, 4, FD, KROWS), BF16),
            V((2, 4, 136, 128), BF16),
            V((2, 4, 136, 128), BF16),
            *[V((4, 2, n, H), BF16) for _, n in LOTS],
            *[V((3, n, H), BF16) for _, n in LOTS],
            *[V((3, n, H), BF16) for _, n in LOTS],
            V((2, 4 * R, H), BF16),
            V((2, 4 * R, FD), BF16),
            [[V((4, n, w), BF16) for _, n in LOTS] for w in WIDTHS],
            [[V((3, n, w), BF16) for _, n in LOTS] for w in WIDTHS],
            [[V((3, n, w), BF16) for _, n in LOTS] for w in WIDTHS],
            *[V((n, DM), BF16) for _, n in LOTS],
            dma((23,)),
            dma((2, 3)),
            dma((60,)),
            dma((4, 4, 4)),
            dma((2, 64)),
            dma((4, 2, 4)),
            dma((2, 10)),
            dma((2, 4, 3)),
            dma((2, 4, 3)),
            dma((5, 4, 3)),
        ],
        compiler_params=pltpu.CompilerParams(
            collective_id=0, has_side_effects=True, vmem_limit_bytes=60 * 1024 * 1024
        ),
    )(
        residual, small_value_inputs, large_value_inputs, small_gate_inputs, large_gate_inputs,
        flat, small_output_projection, large_output_projection, gate_matrix.T, up_matrix.T, down_matrix,
        small_step_inputs.T, large_step_inputs.T, small_decay_offsets.T, large_decay_offsets.T,
        small_decay_rates.reshape(1, 2), large_decay_rates.reshape(1, 1), small_filter_taps, large_filter_taps, state_filter_taps,
        small_head_gains.reshape(1, 128), large_head_gains.reshape(1, 128),
        channel_norm_gain.reshape(1, DM),
    )


def solution(mesh):
    split = Mesh(mesh.devices.reshape(4, 4, 4, 2), ("z", "y", "x", "c"))
    in_specs = (
        P(SP_TP, None),
        P(SP, TP),
        P(SP, TP),
        P(SP, TP),
        P(SP, TP),
        P(SP, None, None),
        P(SP, TP),
        P(SP, TP),
        P(SP, TP),
        P(SP, TP),
        P(TP),
        P(TP),
        P(None, TP),
        P(None, TP),
        P(),
        P(TP),
        P(TP),
        P(TP, None),
        P(TP, None),
        P(),
        P(SP, TP),
        P(SP, TP),
        P(TP, SP),
    )
    return jax.shard_map(
        on_device, mesh=split, in_specs=in_specs, out_specs=P(SP_TP, None), check_vma=False
    )
```

```python
import functools

import jax
import jax.numpy as jnp
from jax import lax
from jax.experimental import pallas as pl
from jax.experimental.pallas import tpu as pltpu
from jax.sharding import Mesh
from jax.sharding import PartitionSpec as P

F32 = jnp.float32
BF16 = jnp.bfloat16
SP = ("z", "y")
TP = ("x", "c")
SP_TP = ("z", "y", "x", "c")

T = 640
L = 128
NB = T // L
R = 80
FD = 704
DM = 2048
H = 1024
KROWS = 128
CUT = 352
AFTER = (((0,), (), ()), ((1,), (), (15,)), ((2,), (0,), (16, 17)), ((), (1,), ()), ((3, 4), (), (18, 19)))
WIDTHS = (512, 256, 512, 512, 256)
LOTS = ((0, 48), (48, 32))
STEPS = (0, 1, -1, 2)
COLUMNS = (
    ((0, 0), (1, 0), (0, 1), (-1, 0)),
    ((0, -1), (1, 1)),
    ((1, -1), (-1, 1), (-1, -1), (2, 0)),
    ((0, 2), (1, 2), (2, 1), (-1, 2)),
    ((2, -1), (2, 2)),
)
SENDS = (
    ((0, 0, 0, 0, 1), (0, 0, 0, 0, -1), (1, 0, 0, 0, 1), (1, 0, 0, 0, -1), (0, 0, 0, 1, 1), (0, 0, 0, 1, -1)),
    ((1, 0, 0, 1, 1), (1, 0, 0, 1, -1)),
    (),
    ((1, -1, 0, 0, 1), (0, -1, 0, 0, 1), (0, 1, 0, 1, -1), (1, 1, 0, 1, -1)),
    ((0, 1, 0, 1, 1), (0, -1, 0, 1, -1), (1, 1, 0, 1, 1), (1, -1, 0, 1, -1)),
    (),
    ((0, -1, 0, 1, 1), (1, -1, 0, 1, 1), (3, 0, 0, 0, -1), (2, 0, 0, 0, -1), (0, 0, 1, 1, -1), (1, 0, 1, 1, -1)),
    ((0, 2, 0, 1, 1), (1, 2, 0, 1, 1), (0, 2, 0, 1, -1), (1, 2, 0, 1, -1)),
    ((3, 0, 0, 0, 1), (2, 0, 0, 0, 1)),
    ((0, 1, -1, 1, 1), (0, -1, 1, 1, -1), (1, 1, -1, 1, 1), (1, -1, 1, 1, -1)),
    ((0, 2, -1, 1, 1), (1, 2, -1, 1, 1), (3, 1, 0, 0, -1), (2, 1, 0, 0, -1)),
    ((2, 0, 0, 1, -1), (3, 0, 0, 1, -1), (2, 0, 0, 1, 1), (2, 1, 0, 1, -1), (3, 0, 0, 1, 1), (3, 1, 0, 1, -1)),
    ((2, 1, 0, 1, 1), (2, -1, 0, 1, -1), (3, 1, 0, 1, 1), (3, -1, 0, 1, -1)),
    ((2, 2, 0, 1, 1), (2, 2, 0, 1, -1), (3, 2, 0, 1, 1), (3, 2, 0, 1, -1), (2, -1, 0, 1, 1), (3, -1, 0, 1, 1)),
    ((2, 0, 1, 1, -1), (3, 0, 1, 1, -1), (2, 1, 1, 1, -1), (3, 1, 1, 1, -1)),
    ((2, 2, -1, 1, 1), (3, 2, -1, 1, 1), (2, -1, 1, 1, -1), (3, -1, 1, 1, -1)),
    (),
    (),
    (),
    (),
)
SHARES = (
    ((0, 0, 0), (1, 0, 0), (2, 0, 0), (3, 0, 0)),
    (),
    ((0, -1, 0), (0, 1, 0), (1, -1, 0), (1, 1, 0)),
    (),
    ((0, 0, -1), (0, 0, 1)),
    ((1, 0, -1), (1, 0, 1)),
    (),
    ((1, 2, 0), (0, 1, 1), (0, 2, 0), (1, 1, 1)),
    ((0, 1, -1), (0, -1, 1), (1, 1, -1), (1, -1, 1), (3, 1, 0), (2, 1, 0)),
    ((0, -1, -1), (1, -1, -1)),
    ((0, 0, 2), (1, 0, 2), (0, 2, -1), (1, 2, -1)),
    ((0, 2, 1), (3, -1, 0), (1, 2, 1), (2, -1, 0)),
    ((0, 1, 2), (0, -1, 2), (1, 1, 2), (1, -1, 2)),
    ((3, 2, 0), (2, 2, 0), (0, 2, 2), (1, 2, 2)),
    ((2, 0, 1), (3, 0, 1), (2, 0, -1), (2, 1, 1), (3, 0, -1), (3, 1, 1)),
    ((2, 1, -1), (2, -1, 1), (3, 1, -1), (3, -1, 1), (2, 2, -1), (2, 2, 1), (3, 2, -1), (3, 2, 1), (2, -1, -1), (3, -1, -1), (2, 0, 2)),
    ((3, 0, 2), (2, 1, 2), (3, 1, 2), (3, -1, 2)),
    ((2, 2, 2), (3, 2, 2), (2, -1, 2)),
    (),
    (),
)

head_eps = 1e-05
row_eps = 1e-06


def silu(x):
    return x / (1.0 + jnp.exp(-x))


def dot(a, b):
    return jnp.dot(a, b, preferred_element_type=F32)


def dot_nt(a, b):
    return lax.dot_general(a, b, (((1,), (1,)), ((), ())), preferred_element_type=F32)


def dot_tn(a, b):
    return lax.dot_general(a, b, (((0,), (0,)), ((), ())), preferred_element_type=F32)


def kernel(
    res_in, vs_in, vl_in, gs_in, gl_in, sp_in, ws_in, wl_in, g_in, u_in, d_in,
    small_in_0, small_in_1, small_in_2, small_in_3, small_in_4, small_in_5, small_in_6, small_in_7,
    small_in_8, small_in_9, small_in_10, small_in_11,
    out,
    small,
    xin, sxin, gin, resv, halo, halo_m, cbuf, cmaps, conv_k, drive, fresh, inner, heads, hpart_0, hpart_1, lhs_0, lhs_1,
    wo, wg, wu, wd, st1, st2, parts_0, parts_1, left_0, left_1, right_0, right_1, ag, hid,
    dparts, dleft, dright, mid_0, mid_1,
    loc_sem, halo_sem, w_send, w_recv, pair_sem, st_sem, hp_sem, rs_sem, ag_sem, rs2_sem,
):
    z, y, x, c = (lax.axis_index(n) for n in ("z", "y", "x", "c"))
    rem = lax.rem
    o = 1 - c

    def at(base, by):
        return rem(base + (by % 4), 4)

    nxt = {"z": rem(z + lax.div(y + 1, 4), 4), "y": rem(y + 1, 4)}
    prv = {"z": rem(z + 3 + lax.div(y + 3, 4), 4), "y": rem(y + 3, 4)}

    def there(**kw):
        base = {"z": z, "y": y, "x": x, "c": c}
        base.update(kw)
        return (base["z"], base["y"], base["x"], base["c"])

    def remote(src, dst, send, recv, **kw):
        return pltpu.make_async_remote_copy(
            src_ref=src, dst_ref=dst, send_sem=send, recv_sem=recv,
            device_id=there(**kw), device_id_type=pl.DeviceIdType.MESH,
        )

    pending = []

    def go(cp):
        cp.start()
        pending.append(cp)
        return cp

    barrier = pltpu.get_barrier_semaphore()
    peers = [
        dict(c=o), dict(x=at(x, 1)), dict(x=at(x, 3)),
        dict(y=at(y, 1)), dict(y=at(y, 2)), dict(y=at(y, 3)),
        dict(z=at(z, 1)), dict(z=at(z, 2)), dict(z=at(z, 3)),
        nxt, prv,
    ]
    for p in peers:
        pl.semaphore_signal(barrier, inc=1, device_id=there(**p), device_id_type=pl.DeviceIdType.MESH)
    local = [
        *zip(
            (small_in_0, small_in_1, small_in_2, small_in_3, small_in_4, small_in_5, small_in_6,
             small_in_7, small_in_8, small_in_9, small_in_10, small_in_11), small,
        ),
        (vs_in, xin.at[:, pl.ds(0, 128)]),
        (vl_in, xin.at[:, pl.ds(128, 128)]),
        (sp_in, sxin),
        (gs_in, gin.at[:, pl.ds(0, 128)]),
        (gl_in, gin.at[:, pl.ds(128, 128)]),
        (res_in, resv),
        (ws_in, wo.at[c, pl.ds(0, 128)]),
        (wl_in, wo.at[c, pl.ds(128, 128)]),
        (g_in, wg.at[c, z, y]),
        (u_in, wu.at[c, z, y]),
        (d_in, wd.at[c, z, y]),
    ]
    local = [pltpu.make_async_copy(a, b, loc_sem.at[i]) for i, (a, b) in enumerate(local)]
    for cp in local:
        cp.start()
    fetched, local = local[:12], local[12:]
    steps_s, steps_l, offs_s, offs_l, rates_s, rates_l, taps_s, taps_l, taps_m, gain_s, gain_l, gain_n = small

    pl.semaphore_wait(barrier, len(peers))

    tail = pl.ds(T - 16, 16)
    halos = [
        go(remote(src, dst, halo_sem.at[0, i], halo_sem.at[1, i], **nxt))
        for i, (src, dst) in enumerate((
            (vs_in.at[tail], halo.at[:, pl.ds(0, 128)]),
            (vl_in.at[tail], halo.at[:, pl.ds(128, 128)]),
            (sp_in.at[pl.ds(4 * T - 64, 64)], halo_m),
        ))
    ]

    names = ("G", "U", "A", "B")
    own_src = {
        "G": g_in, "U": u_in,
        "A": d_in.at[pl.ds(0, CUT)], "B": d_in.at[pl.ds(CUT, CUT)],
    }

    def unit(name, rz, ry, core):
        zz, yy = at(z, rz), at(y, ry)
        if name == "G":
            return wg.at[core, zz, yy]
        if name == "U":
            return wu.at[core, zz, yy]
        rows = pl.ds(0, CUT) if name == "A" else pl.ds(CUT, CUT)
        return wd.at[core, zz, yy, rows]

    def place(name, f, s):
        return (f, s) if name in ("U", "B") else (s, f)

    def source(name, f, s):
        return own_src[name] if (f, s) == (0, 0) else unit(name, *place(name, f, s), c)

    def w_sem(name, rz, ry):
        return w_recv.at[names.index(name), rz % 4, ry % 4]

    n_sent = [0]
    here = {(n, 0, 0) for n in names}

    def w_wait(name, f, s):
        if (name, f, s) not in here:
            here.add((name, f, s))
            ref = unit(name, *place(name, f, s), c)
            remote(ref, ref, w_send.at[0], w_sem(name, *place(name, f, s))).wait_recv()

    def w_go(name, f, s, second, step):
        w_wait(name, f, s)
        dz, dy = place(name, 0, step) if second else place(name, step, 0)
        rz, ry = place(name, f, s)
        k = n_sent[0]
        n_sent[0] += 1
        go(remote(
            source(name, f, s), unit(name, rz, ry, c), w_send.at[k], w_sem(name, rz - dz, ry - dy),
            z=at(z, dz), y=at(y, dy),
        ))

    pair_index = {}

    def share(name, f, s):
        w_wait(name, f, s)
        k = pair_index.setdefault((name, f, s), len(pair_index))
        go(remote(
            source(name, f, s), unit(name, *place(name, f, s), c),
            pair_sem.at[0, k], pair_sem.at[1, k], c=o,
        ))

    def pair_wait(name, f, s):
        k = pair_index[(name, f, s)]
        ref = unit(name, *place(name, f, s), o)
        remote(ref, ref, pair_sem.at[0, k], pair_sem.at[1, k], c=o).wait_recv()

    def pump(i):
        for n, f, s, second, step in SENDS[i]:
            w_go(names[n], f, s, second, step)
        for n, f, s in SHARES[i]:
            share(names[n], f, s)

    pump(0)

    wo_copies = [
        go(remote(src, wo.at[c, rows], hp_sem.at[0, 8 + i], hp_sem.at[1, 8 + i], c=o))
        for i, (src, rows) in enumerate(((ws_in, pl.ds(0, 128)), (wl_in, pl.ds(128, 128))))
    ]

    for cp in fetched:
        cp.wait()
    lane = lax.broadcasted_iota(jnp.int32, (8, L), 1)
    rows = []
    both = []
    row8 = lax.broadcasted_iota(jnp.int32, (8, L), 0)
    raw_steps = jnp.concatenate([steps_s[...].astype(F32), steps_l[...].astype(F32)], axis=0)
    softened = jnp.maximum(raw_steps, 0.0) + jnp.log1p(jnp.exp(-jnp.abs(raw_steps)))
    head = lax.broadcasted_iota(jnp.int32, (3, T), 0)
    rate = jnp.where(head == 0, rates_s[0:1, 0:1], jnp.where(head == 1, rates_s[0:1, 1:2], rates_l[0:1, 0:1]))
    offsets = jnp.concatenate([offs_s[...], offs_l[...]], axis=0)
    meta = jnp.concatenate(
        [offsets - jnp.exp(rate) * softened, softened, jnp.zeros((2, T), F32)], axis=0
    )
    for k in range(NB):
        raw = meta[:, k * L : (k + 1) * L]
        acc = raw
        for sft in (1, 2, 4, 8, 16, 32, 64):
            acc = acc + jnp.where(lane >= sft, pltpu.roll(acc, sft, 1), 0.0)
        rows.append(acc)
        both.append(jnp.where(row8 < 3, acc, raw))
    both.append(jnp.zeros((L - 8 * NB, L), F32))
    cols = jnp.concatenate(both, axis=0).T
    grown = jnp.exp(cols)
    shrunk = jnp.exp(cols[L - 1 : L, :] - cols)

    half = lax.broadcasted_iota(jnp.int32, (L, L), 1) < 64
    half1 = lax.broadcasted_iota(jnp.int32, (1, L), 1) < 64

    def spread(m, k, off):
        b = 8 * k + off
        small = jnp.where(half, m[:, b : b + 1], m[:, b + 1 : b + 2])
        large = jnp.broadcast_to(m[:, b + 2 : b + 3], (L, L))
        return small, large

    def block_decay(k):
        b = 8 * k
        e = grown[L - 1 : L]
        small = jnp.where(half1, e[:, b : b + 1], e[:, b + 1 : b + 2])
        large = jnp.broadcast_to(e[:, b + 2 : b + 3], (1, L))
        return jnp.concatenate([small, large], axis=1)

    tap_rows = []
    for j in range(4):
        m = taps_m[j].astype(F32)
        tap_rows.append(
            [taps_s[j : j + 1].astype(F32), taps_l[j : j + 1].astype(F32)]
            + [m[i : i + 1] for i in range(4)]
        )

    def conv(k, g):
        total = None
        for j in range(4):
            row = k * L + 5 + j
            if g < 2:
                rows_j = cbuf[row : row + L, g * 128 : g * 128 + 128]
            else:
                rows_j = cmaps[pl.ds(4 * row + g - 2, L, 4), :]
            part = tap_rows[j][g] * rows_j
            total = part if total is None else total + part
        return silu(total)

    for i in range(3):
        local[i].wait()
    for k in range(NB):
        cbuf[8 + k * L : 8 + (k + 1) * L, :] = xin[k * L : (k + 1) * L, :].astype(F32)
        maps_k = pl.ds(32 + 4 * k * L, 4 * L)
        cmaps[maps_k, :] = sxin[4 * k * L : 4 * (k + 1) * L, :].astype(F32)
    decays = [block_decay(k) for k in range(NB)]

    def first_pass(k, kind):
        dt, sh = spread(cols, k, 3)[kind], spread(shrunk, k, 0)[kind]
        blk, at_kind = pl.ds(k * L, L), pl.ds(kind * 128, 128)
        d = conv(k, kind) * dt
        drive[blk, at_kind] = d.astype(BF16)
        key = conv(k, 2 + 2 * kind).astype(BF16)
        conv_k[blk, 256 * kind : 256 * kind + 128] = key
        conv_k[blk, 256 * kind + 128 : 256 * kind + 256] = conv(k, 3 + 2 * kind).astype(BF16)
        fresh[k, :, at_kind] = dot_tn(key, (d * sh).astype(BF16))

    for kind in range(2):
        for k in range(1, NB):
            first_pass(k, kind)
    for cp in halos:
        cp.wait_recv()
    start = jnp.where(jnp.logical_and(z == 0, y == 0), 0.0, 1.0)
    cbuf[0:8, :] = halo[8:16, :].astype(F32) * start
    cmaps[0:32, :] = halo_m[32:64, :].astype(F32) * start

    def state_out(buf, kind, state, total, stage, **axis):
        buf[kind, 0, 0:128] = state.astype(BF16)
        buf[kind, 0, 128:136] = jnp.broadcast_to(total, (8, 128)).astype(BF16)
        ((name, me),) = axis.items()
        copies = [
            remote(
                buf.at[kind, 0], buf.at[kind, r],
                st_sem.at[2 * stage, kind, r], st_sem.at[2 * stage + 1, kind, r],
                **{name: at(me, r)},
            )
            for r in (1, 2, 3)
        ]
        pending.extend(copies)
        return copies

    def start_all(copies):
        for cp in copies:
            cp.start()

    def states_in(buf, kind, stage):
        for r in (1, 2, 3):
            remote(
                buf.at[kind, 0], buf.at[kind, r],
                st_sem.at[2 * stage, kind, r], st_sem.at[2 * stage + 1, kind, r],
            ).wait_recv()

    def chained(buf, kind, me):
        line, line_d = jnp.zeros((128, 128), F32), jnp.ones((1, 128), F32)
        before, before_d = line, line_d
        for j in range(4):
            blob = buf[kind, rem(me - j + 4, 4)].astype(F32)
            line = line * blob[128:129] + blob[0:128]
            line_d = line_d * blob[128:129]
            before = jnp.where(j < me, line, before)
            before_d = jnp.where(j < me, line_d, before_d)
        return before, before_d, line, line_d

    later = []
    for kind in range(2):
        first_pass(0, kind)
        own = slice(kind * 128, kind * 128 + 128)
        state, total = fresh[0, :, own], decays[0][:, own]
        for k in range(1, NB):
            state = state * decays[k][:, own] + fresh[k, :, own]
            total = total * decays[k][:, own]
        copies = state_out(st1, kind, state, total, 0, y=y)
        pl.when(c == 0)(functools.partial(start_all, copies))
        later += copies

    mask = lax.broadcasted_iota(jnp.int32, (L, L), 0) >= lax.broadcasted_iota(jnp.int32, (L, L), 1)

    def weights_of(k, h):
        b = 8 * k + h
        diff = cols[:, b : b + 1] - rows[k][h : h + 1, :]
        return jnp.exp(jnp.where(mask, diff, -1e30))

    def second_pass(k):
        blk = pl.ds(k * L, L)
        s_s = dot_nt(conv_k[blk, 128:256], conv_k[blk, 0:128])
        s_l = dot_nt(conv_k[blk, 384:512], conv_k[blk, 256:384])
        d_s = drive[blk, 0:128]
        o_0 = dot((s_s * weights_of(k, 0)).astype(BF16), d_s)
        o_1 = dot((s_s * weights_of(k, 1)).astype(BF16), d_s)
        inner[blk, 0:128] = jnp.where(half, o_0, o_1)
        inner[blk, 128:256] = dot((s_l * weights_of(k, 2)).astype(BF16), drive[blk, 128:256])

    for k in range(NB):
        second_pass(k)
    pl.when(c == 1)(functools.partial(start_all, later))
    pump(1)
    inside = []
    for kind in range(2):
        states_in(st1, kind, 0)
        before, before_d, line, line_d = chained(st1, kind, y)
        inside.append((before, before_d))
        start_all(state_out(st2, kind, line, line_d, 1, z=z))
        if kind == 0:
            pump(2)
    pump(3)

    for i in (3, 4):
        local[i].wait()

    def third_pass(k, kind, carry):
        blk, cols_k = pl.ds(k * L, L), pl.ds(kind * 128, 128)
        own = slice(kind * 128, kind * 128 + 128)
        reads = conv_k[blk, 256 * kind + 128 : 256 * kind + 256]
        out_k = inner[blk, cols_k] + dot(reads, carry.astype(BF16)) * spread(grown, k, 0)[kind]
        carry = carry * decays[k][:, own] + fresh[k, :, own]
        out_k = out_k * silu(gin[blk, cols_k].astype(F32))
        sq = out_k * out_k
        if kind == 0:
            sq_0 = jnp.sum(jnp.where(half, sq, 0.0), axis=1, keepdims=True)
            sq_1 = jnp.sum(jnp.where(half, 0.0, sq), axis=1, keepdims=True)
            mean = jnp.where(half, sq_0, sq_1) * (1.0 / 64)
            gain = gain_s[...]
        else:
            mean = jnp.sum(sq, axis=1, keepdims=True) * (1.0 / 128)
            gain = gain_l[...]
        heads[blk, cols_k] = (out_k * lax.rsqrt(mean + head_eps) * gain).astype(BF16)
        return carry

    for kind in range(2):
        states_in(st2, kind, 1)
        before = chained(st2, kind, z)[0]
        carry = before * inside[kind][1] + inside[kind][0]
        for k in range(NB):
            carry = third_pass(k, kind, carry)
        if kind == 0:
            pump(4)

    hpart, lhs = (hpart_0, hpart_1), (lhs_0, lhs_1)
    parts, left, right = (parts_0, parts_1), (left_0, left_1), (right_0, right_1)
    mid = (mid_0, mid_1)

    def rows_of(b, core, t):
        first, n = LOTS[t]
        return pl.ds(pl.multiple_of((2 * b + core) * R + first, 16), n)

    def block_of(b, t):
        n = LOTS[t][1]
        return pl.ds(b * n if isinstance(b, int) else pl.multiple_of(b * n, 16), n)

    def row_of(b, t):
        first, n = LOTS[t]
        return pl.ds(pl.multiple_of(4 * first + b * n, 16), n)

    hp_copies = [
        [
            go(remote(
                heads.at[rows_of(b, o, t)], hpart[t].at[block_of(b, t)],
                hp_sem.at[0, 4 * t + b], hp_sem.at[1, 4 * t + b], c=o,
            ))
            for b in range(4)
        ]
        for t in range(2)
    ]
    for t in range(2):
        for b in range(4):
            lhs[t][block_of(b, t), :] = heads[rows_of(b, c, t), :]
    pump(5)
    for i in (6, 7):
        local[i].wait()
    for cp in wo_copies:
        cp.wait_recv()

    x1, x2, x3 = at(x, 1), at(x, 2), at(x, 3)

    class Sum:
        def __init__(self, part, from_left, from_right, sem):
            self.part, self.left, self.right, self.sem = part, from_left, from_right, sem

        def to_right(self, slot, block, role):
            go(remote(self.part(block, role), self.left(slot), self.sem(0, slot), self.sem(1, slot), x=x1))

        def to_left(self, slot, block, role):
            go(remote(self.part(block, role), self.right(slot), self.sem(2, slot), self.sem(3, slot), x=x3))

        def wait_left(self, slot):
            ref = self.left(slot)
            remote(ref, ref, self.sem(0, slot), self.sem(1, slot)).wait_recv()
            return ref[...].astype(F32)

        def wait_right(self, slot):
            ref = self.right(slot)
            remote(ref, ref, self.sem(2, slot), self.sem(3, slot)).wait_recv()
            return ref[...].astype(F32)

        def relayed(self):
            self.to_right(0, x2, 0)
            self.to_left(0, x2, 1)

        def direct(self):
            self.to_right(1, x1, 1)
            self.to_left(1, x3, 0)

        def merge(self):
            mine = self.part(x1, 0)
            mine[...] = (self.wait_left(0) + mine[...].astype(F32)).astype(BF16)
            self.to_right(2, x1, 0)
            mine = self.part(x3, 1)
            mine[...] = (self.wait_right(0) + mine[...].astype(F32)).astype(BF16)
            self.to_left(2, x3, 1)

        def result(self, role):
            a, b = (2, 1) if role == 0 else (1, 2)
            return self.part(x, role)[...].astype(F32) + self.wait_left(a) + self.wait_right(b)

    def mixed_sum(t):
        return Sum(
            lambda block, role: parts[t].at[block, role],
            lambda slot: left[t].at[slot], lambda slot: right[t].at[slot],
            lambda k, slot: rs_sem.at[t, k, slot],
        )

    mixed = [mixed_sum(0), mixed_sum(1)]

    def project(t):
        n = LOTS[t][1]
        for cp in hp_copies[t]:
            cp.wait_recv()
        mine, other = lhs[t][...], hpart[t][...]
        for role in range(2):
            for e in range(4):
                cols_e = pl.ds(role * H + e * 256, 256)
                acc = dot(mine, wo[c, :, cols_e]) + dot(other, wo[o, :, cols_e])
                parts[t][:, role, :, e * 256 : (e + 1) * 256] = acc.reshape(4, n, 256).astype(BF16)

    project(0)
    mixed[0].relayed()
    mixed[0].direct()
    project(1)
    mixed[1].relayed()
    pump(6)
    mixed[0].merge()
    mixed[1].direct()
    pump(7)
    mixed[1].merge()
    pump(8)
    local[5].wait()

    def norm(t):
        first, n = LOTS[t]
        wide = []
        for role in range(2):
            at_role = slice(role * H, role * H + H)
            m = (resv[first : first + n, at_role].astype(F32) + mixed[t].result(role)).astype(BF16)
            mid[t][:, at_role] = m
            wide.append(m.astype(F32))
        square = sum(jnp.sum(w * w, axis=1, keepdims=True) for w in wide)
        scale = lax.rsqrt(square * (1.0 / DM) + row_eps)
        for role in range(2):
            at_role = slice(role * H, role * H + H)
            ag[role, row_of(x, t), :] = (wide[role] * scale * gain_n[:, at_role]).astype(BF16)

    def ag_right(t, slot, block, role):
        ref = ag.at[role, row_of(block, t)]
        go(remote(ref, ref, ag_sem.at[t, 0, slot], ag_sem.at[t, 1, slot], x=x1))

    def ag_left(t, slot, block, role):
        ref = ag.at[role, row_of(block, t)]
        go(remote(ref, ref, ag_sem.at[t, 2, slot], ag_sem.at[t, 3, slot], x=x3))

    def ag_wait(t, side, slot, block, role):
        ref = ag.at[role, row_of(block, t)]
        remote(ref, ref, ag_sem.at[t, 0, slot], ag_sem.at[t, side, slot]).wait_recv()

    def ag_relay(t):
        ag_wait(t, 1, 0, x3, 0)
        ag_right(t, 2, x3, 0)
        ag_wait(t, 3, 0, x1, 1)
        ag_left(t, 2, x1, 1)

    def ag_rest(t):
        ag_wait(t, 1, 1, x3, 1)
        ag_wait(t, 3, 1, x1, 0)
        ag_wait(t, 1, 2, x2, 0)
        ag_wait(t, 3, 2, x2, 1)

    norm(0)
    ag_right(0, 0, x, 0)
    ag_left(0, 0, x, 1)
    ag_right(0, 1, x, 1)
    ag_left(0, 1, x, 0)
    pump(9)
    norm(1)
    ag_right(1, 0, x, 0)
    ag_left(1, 0, x, 1)
    pump(10)
    ag_relay(0)
    ag_right(1, 1, x, 1)
    ag_left(1, 1, x, 0)
    pump(11)
    ag_relay(1)
    pump(12)
    ag_rest(0)
    pump(13)
    ag_rest(1)
    for i in (8, 9, 10):
        local[i].wait()

    def lined_up(w, core, h, n0, n):
        pieces = [w[core, 2 * h + j // 4, j % 4, n0 : n0 + n, :] for j in range(8)]
        return jnp.concatenate(pieces, axis=1)

    def expand(core):
        for n0, n in ((0, 256), (256, 256), (512, 192)):
            gate = up = None
            for h in range(2):
                a = ag[h]
                w_gate = lined_up(wg, core, h, n0, n)
                w_up = lined_up(wu, core, h, n0, n)
                gate = dot_nt(a, w_gate) if gate is None else gate + dot_nt(a, w_gate)
                up = dot_nt(a, w_up) if up is None else up + dot_nt(a, w_up)
            hid[core, :, n0 : n0 + n] = (silu(gate) * up).astype(BF16)

    expand(c)
    pump(14)
    for name in ("G", "U"):
        for f in STEPS:
            for st in STEPS:
                pair_wait(name, f, st)
    expand(o)

    def rows_in(i, role):
        return role if i % 2 == 0 else 1 - role

    def down_sum(i):
        return Sum(
            lambda block, role: dparts[i][rows_in(i, role)].at[block],
            lambda slot: dleft[i][rows_in(i, slot % 2)].at[slot],
            lambda slot: dright[i][rows_in(i, 1 - slot % 2)].at[slot],
            lambda k, slot: rs2_sem.at[i, k, slot],
        )

    down = [down_sum(i) for i in range(5)]

    def finish(i):
        for role in range(2):
            t = rows_in(i, role)
            first, n = LOTS[t]
            total = down[i].result(role)
            for j, (rz, ry) in enumerate(COLUMNS[i]):
                at_j = pl.ds(pl.multiple_of((at(z, rz) * 4 + at(y, ry)) * 128, 128), 128)
                out[first : first + n, at_j] = (
                    mid[t][:, at_j].astype(F32) + total[:, 128 * j : 128 * j + 128]
                ).astype(BF16)

    for i in range(5):
        if i == 2:
            settled = len(pending)
        for rz, ry in COLUMNS[i]:
            for name in ("A", "B"):
                pair_wait(name, *place(name, rz, ry))
        for e in range(WIDTHS[i] // 256):
            acc = None
            for cc in range(2):
                w_down = jnp.concatenate(
                    [wd[cc, at(z, rz), at(y, ry)] for rz, ry in COLUMNS[i][2 * e : 2 * e + 2]], axis=1
                )
                acc = dot(hid[cc], w_down) if acc is None else acc + dot(hid[cc], w_down)
            for t, (first, n) in enumerate(LOTS):
                lot_acc = acc[4 * first : 4 * first + 4 * n].reshape(4, n, 256)
                dparts[i][t][:, :, e * 256 : (e + 1) * 256] = lot_acc.astype(BF16)
        down[i].relayed()
        for j in AFTER[i][0]:
            down[j].direct()
        for j in AFTER[i][1]:
            down[j].merge()
        for j in AFTER[i][2]:
            pump(j)
    down[2].merge()
    for cp in pending[:settled]:
        cp.wait_send()
    del pending[:settled]
    down[3].merge()
    down[4].merge()
    for i in range(5):
        finish(i)

    for cp in pending:
        cp.wait_send()


def on_device(
    residual, small_value_inputs, large_value_inputs, small_gate_inputs, large_gate_inputs,
    state_projections, small_step_inputs, large_step_inputs, small_decay_offsets,
    large_decay_offsets, small_decay_rates, large_decay_rates, small_filter_taps,
    large_filter_taps, state_filter_taps, small_head_gains, large_head_gains,
    small_output_projection, large_output_projection, channel_norm_gain, gate_matrix,
    up_matrix, down_matrix,
):
    flat = state_projections.reshape(4 * T, 128)

    anywhere = pl.BlockSpec(memory_space=pl.ANY)
    dma = pltpu.SemaphoreType.DMA
    V = pltpu.VMEM
    return pl.pallas_call(
        kernel,
        out_shape=pltpu.VMEM((R, DM), BF16),
        in_specs=[anywhere] * 23,
        out_specs=pl.BlockSpec(memory_space=pltpu.VMEM),
        scratch_shapes=[
            [
                V((2, T), BF16), V((1, T), BF16), V((2, T), F32), V((1, T), F32), V((1, 2), F32), V((1, 1), F32),
                V((4, 128), BF16), V((4, 128), BF16), V((4, 4, 128), BF16), V((1, 128), F32), V((1, 128), F32),
                V((1, DM), F32),
            ],
            V((T, 256), BF16),
            V((4 * T, 128), BF16),
            V((T, 256), BF16),
            V((R, DM), BF16),
            V((16, 256), BF16),
            V((64, 128), BF16),
            V((T + 8, 256), F32),
            V((4 * T + 32, 128), F32),
            V((T, 512), BF16),
            V((T, 256), BF16),
            V((NB, 128, 256), F32),
            V((T, 256), F32),
            V((T, 256), BF16),
            *[V((4 * n, 256), BF16) for _, n in LOTS],
            *[V((4 * n, 256), BF16) for _, n in LOTS],
            V((2, 256, DM), BF16),
            V((2, 4, 4, FD, KROWS), BF16),
            V((2, 4, 4, FD, KROWS), BF16),
            V((2, 4, 4, FD, KROWS), BF16),
            V((2, 4, 136, 128), BF16),
            V((2, 4, 136, 128), BF16),
            *[V((4, 2, n, H), BF16) for _, n in LOTS],
            *[V((3, n, H), BF16) for _, n in LOTS],
            *[V((3, n, H), BF16) for _, n in LOTS],
            V((2, 4 * R, H), BF16),
            V((2, 4 * R, FD), BF16),
            [[V((4, n, w), BF16) for _, n in LOTS] for w in WIDTHS],
            [[V((3, n, w), BF16) for _, n in LOTS] for w in WIDTHS],
            [[V((3, n, w), BF16) for _, n in LOTS] for w in WIDTHS],
            *[V((n, DM), BF16) for _, n in LOTS],
            dma((23,)),
            dma((2, 3)),
            dma((60,)),
            dma((4, 4, 4)),
            dma((2, 64)),
            dma((4, 2, 4)),
            dma((2, 10)),
            dma((2, 4, 3)),
            dma((2, 4, 3)),
            dma((5, 4, 3)),
        ],
        compiler_params=pltpu.CompilerParams(
            collective_id=0, has_side_effects=True, vmem_limit_bytes=60 * 1024 * 1024
        ),
    )(
        residual, small_value_inputs, large_value_inputs, small_gate_inputs, large_gate_inputs,
        flat, small_output_projection, large_output_projection, gate_matrix.T, up_matrix.T, down_matrix,
        small_step_inputs.T, large_step_inputs.T, small_decay_offsets.T, large_decay_offsets.T,
        small_decay_rates.reshape(1, 2), large_decay_rates.reshape(1, 1), small_filter_taps, large_filter_taps, state_filter_taps,
        small_head_gains.reshape(1, 128), large_head_gains.reshape(1, 128),
        channel_norm_gain.reshape(1, DM),
    )


def solution(mesh):
    split = Mesh(mesh.devices.reshape(4, 4, 4, 2), ("z", "y", "x", "c"))
    in_specs = (
        P(SP_TP, None),
        P(SP, TP),
        P(SP, TP),
        P(SP, TP),
        P(SP, TP),
        P(SP, None, None),
        P(SP, TP),
        P(SP, TP),
        P(SP, TP),
        P(SP, TP),
        P(TP),
        P(TP),
        P(None, TP),
        P(None, TP),
        P(),
        P(TP),
        P(TP),
        P(TP, None),
        P(TP, None),
        P(),
        P(SP, TP),
        P(SP, TP),
        P(TP, SP),
    )
    return jax.shard_map(
        on_device, mesh=split, in_specs=in_specs, out_specs=P(SP_TP, None), check_vma=False
    )
```

```python
import functools

import jax
import jax.numpy as jnp
from jax import lax
from jax.experimental import pallas as pl
from jax.experimental.pallas import tpu as pltpu
from jax.sharding import Mesh
from jax.sharding import PartitionSpec as P

F32 = jnp.float32
BF16 = jnp.bfloat16
SP = ("z", "y")
TP = ("x", "c")
SP_TP = ("z", "y", "x", "c")

T = 640
L = 128
NB = T // L
R = 80
FD = 704
DM = 2048
H = 1024
KROWS = 128
CUT = 352
AFTER = (((0,), (), ()), ((1,), (), (15,)), ((2,), (0,), (16, 17)), ((), (1,), ()), ((3, 4), (), (18, 19)))
WIDTHS = (512, 256, 512, 512, 256)
LOTS = ((0, 48), (48, 32))
STEPS = (0, 1, -1, 2)
COLUMNS = (
    ((0, 0), (1, 0), (0, 1), (-1, 0)),
    ((0, -1), (1, 1)),
    ((1, -1), (-1, 1), (2, 0), (-1, -1)),
    ((0, 2), (2, 1), (1, 2), (2, -1)),
    ((2, 2), (-1, 2)),
)
SENDS = (
    ((0, 0, 0, 0, 1), (0, 0, 0, 0, -1), (1, 0, 0, 0, 1), (1, 0, 0, 0, -1), (0, 0, 0, 1, 1), (0, 0, 0, 1, -1)),
    ((1, 0, 0, 1, 1), (1, 0, 0, 1, -1)),
    (),
    ((1, -1, 0, 0, 1), (0, -1, 0, 0, 1), (0, 1, 0, 1, -1), (1, 1, 0, 1, -1)),
    ((0, 1, 0, 1, 1), (0, -1, 0, 1, -1), (1, 1, 0, 1, 1), (1, -1, 0, 1, -1)),
    (),
    ((0, -1, 0, 1, 1), (1, -1, 0, 1, 1), (3, 0, 0, 0, -1), (2, 0, 0, 0, -1), (0, 0, 1, 1, -1), (1, 0, 1, 1, -1)),
    ((0, 2, 0, 1, 1), (1, 2, 0, 1, 1), (0, 2, 0, 1, -1), (1, 2, 0, 1, -1)),
    ((3, 0, 0, 0, 1), (2, 0, 0, 0, 1)),
    ((0, 1, -1, 1, 1), (0, -1, 1, 1, -1), (1, 1, -1, 1, 1), (1, -1, 1, 1, -1)),
    ((0, 2, -1, 1, 1), (1, 2, -1, 1, 1), (3, 1, 0, 0, -1), (2, 1, 0, 0, -1)),
    ((2, 0, 0, 1, -1), (3, 0, 0, 1, -1), (2, 0, 0, 1, 1), (2, 1, 0, 1, -1), (3, 0, 0, 1, 1), (3, 1, 0, 1, -1)),
    ((2, 1, 0, 1, 1), (2, -1, 0, 1, -1), (3, 1, 0, 1, 1), (3, -1, 0, 1, -1)),
    ((2, 2, 0, 1, 1), (2, 2, 0, 1, -1), (3, 2, 0, 1, 1), (3, 2, 0, 1, -1), (2, -1, 0, 1, 1), (3, -1, 0, 1, 1)),
    ((2, 0, 1, 1, -1), (3, 0, 1, 1, -1), (2, 1, 1, 1, -1), (3, 1, 1, 1, -1)),
    ((2, 2, -1, 1, 1), (3, 2, -1, 1, 1), (2, -1, 1, 1, -1), (3, -1, 1, 1, -1)),
    (),
    (),
    (),
    (),
)
SHARES = (
    (),
    (),
    ((0, -1, 0), (0, 1, 0), (1, -1, 0), (1, 1, 0)),
    ((0, 0, 0), (1, 0, 0), (2, 0, 0), (3, 0, 0)),
    ((0, 0, -1), (0, 0, 1)),
    ((1, 0, -1), (1, 0, 1)),
    (),
    ((1, 2, 0), (0, 1, 1), (0, 2, 0), (1, 1, 1), (0, 1, -1), (0, -1, 1)),
    ((1, 1, -1), (1, -1, 1), (3, 1, 0), (2, 1, 0)),
    ((0, -1, -1), (1, -1, -1), (0, 0, 2)),
    ((1, 0, 2), (0, 2, -1), (1, 2, -1)),
    ((0, 2, 1), (3, -1, 0), (1, 2, 1), (2, -1, 0)),
    ((0, 1, 2), (0, -1, 2), (1, 1, 2), (1, -1, 2)),
    ((3, 2, 0), (2, 2, 0), (0, 2, 2), (1, 2, 2)),
    ((2, 0, 1), (3, 0, 1), (2, 0, -1), (2, 1, 1), (3, 0, -1), (3, 1, 1)),
    ((2, 1, -1), (2, -1, 1), (3, 1, -1), (3, -1, 1), (2, 2, -1), (2, 2, 1), (3, 2, -1), (3, 2, 1), (2, -1, -1), (2, 0, 2), (3, -1, -1)),
    ((3, 0, 2), (2, 1, 2), (3, 1, 2), (2, -1, 2)),
    ((2, 2, 2), (3, 2, 2), (3, -1, 2)),
    (),
    (),
)

head_eps = 1e-05
row_eps = 1e-06


def silu(x):
    return x / (1.0 + jnp.exp(-x))


def dot(a, b):
    return jnp.dot(a, b, preferred_element_type=F32)


def dot_nt(a, b):
    return lax.dot_general(a, b, (((1,), (1,)), ((), ())), preferred_element_type=F32)


def dot_tn(a, b):
    return lax.dot_general(a, b, (((0,), (0,)), ((), ())), preferred_element_type=F32)


def kernel(
    res_in, vs_in, vl_in, gs_in, gl_in, sp_in, ws_in, wl_in, g_in, u_in, d_in,
    small_in_0, small_in_1, small_in_2, small_in_3, small_in_4, small_in_5, small_in_6, small_in_7,
    small_in_8, small_in_9, small_in_10, small_in_11,
    out,
    small,
    xin, sxin, gin, resv, halo, halo_m, cbuf, cmaps, conv_k, drive, fresh, inner, heads, hpart_0, hpart_1, lhs_0, lhs_1,
    wo, wg, wu, wd, st1, st2, parts_0, parts_1, left_0, left_1, right_0, right_1, ag, hid,
    dparts, dleft, dright, mid_0, mid_1,
    loc_sem, halo_sem, w_send, w_recv, pair_sem, st_sem, hp_sem, rs_sem, ag_sem, rs2_sem,
):
    z, y, x, c = (lax.axis_index(n) for n in ("z", "y", "x", "c"))
    rem = lax.rem
    o = 1 - c

    def at(base, by):
        return rem(base + (by % 4), 4)

    nxt = {"z": rem(z + lax.div(y + 1, 4), 4), "y": rem(y + 1, 4)}
    prv = {"z": rem(z + 3 + lax.div(y + 3, 4), 4), "y": rem(y + 3, 4)}

    def there(**kw):
        base = {"z": z, "y": y, "x": x, "c": c}
        base.update(kw)
        return (base["z"], base["y"], base["x"], base["c"])

    def remote(src, dst, send, recv, **kw):
        return pltpu.make_async_remote_copy(
            src_ref=src, dst_ref=dst, send_sem=send, recv_sem=recv,
            device_id=there(**kw), device_id_type=pl.DeviceIdType.MESH,
        )

    pending = []

    def go(cp):
        cp.start()
        pending.append(cp)
        return cp

    barrier = pltpu.get_barrier_semaphore()
    peers = [
        dict(c=o), dict(x=at(x, 1)), dict(x=at(x, 3)),
        dict(y=at(y, 1)), dict(y=at(y, 2)), dict(y=at(y, 3)),
        dict(z=at(z, 1)), dict(z=at(z, 2)), dict(z=at(z, 3)),
        nxt, prv,
    ]
    for p in peers:
        pl.semaphore_signal(barrier, inc=1, device_id=there(**p), device_id_type=pl.DeviceIdType.MESH)
    local = [
        *zip(
            (small_in_0, small_in_1, small_in_2, small_in_3, small_in_4, small_in_5, small_in_6,
             small_in_7, small_in_8, small_in_9, small_in_10, small_in_11), small,
        ),
        (vs_in, xin.at[:, pl.ds(0, 128)]),
        (vl_in, xin.at[:, pl.ds(128, 128)]),
        (sp_in, sxin),
        (gs_in, gin.at[:, pl.ds(0, 128)]),
        (gl_in, gin.at[:, pl.ds(128, 128)]),
        (res_in, resv),
        (ws_in, wo.at[c, pl.ds(0, 128)]),
        (wl_in, wo.at[c, pl.ds(128, 128)]),
        (g_in, wg.at[c, z, y]),
        (u_in, wu.at[c, z, y]),
        (d_in, wd.at[c, z, y]),
    ]
    local = [pltpu.make_async_copy(a, b, loc_sem.at[i]) for i, (a, b) in enumerate(local)]
    for cp in local:
        cp.start()
    fetched, local = local[:12], local[12:]
    steps_s, steps_l, offs_s, offs_l, rates_s, rates_l, taps_s, taps_l, taps_m, gain_s, gain_l, gain_n = small

    pl.semaphore_wait(barrier, len(peers))

    tail = pl.ds(T - 16, 16)
    halos = [
        go(remote(src, dst, halo_sem.at[0, i], halo_sem.at[1, i], **nxt))
        for i, (src, dst) in enumerate((
            (vs_in.at[tail], halo.at[:, pl.ds(0, 128)]),
            (vl_in.at[tail], halo.at[:, pl.ds(128, 128)]),
            (sp_in.at[pl.ds(4 * T - 64, 64)], halo_m),
        ))
    ]

    names = ("G", "U", "A", "B")
    own_src = {
        "G": g_in, "U": u_in,
        "A": d_in.at[pl.ds(0, CUT)], "B": d_in.at[pl.ds(CUT, CUT)],
    }

    def unit(name, rz, ry, core):
        zz, yy = at(z, rz), at(y, ry)
        if name == "G":
            return wg.at[core, zz, yy]
        if name == "U":
            return wu.at[core, zz, yy]
        rows = pl.ds(0, CUT) if name == "A" else pl.ds(CUT, CUT)
        return wd.at[core, zz, yy, rows]

    def place(name, f, s):
        return (f, s) if name in ("U", "B") else (s, f)

    def source(name, f, s):
        return own_src[name] if (f, s) == (0, 0) else unit(name, *place(name, f, s), c)

    def w_sem(name, rz, ry):
        return w_recv.at[names.index(name), rz % 4, ry % 4]

    n_sent = [0]
    here = {(n, 0, 0) for n in names}

    def w_wait(name, f, s):
        if (name, f, s) not in here:
            here.add((name, f, s))
            ref = unit(name, *place(name, f, s), c)
            remote(ref, ref, w_send.at[0], w_sem(name, *place(name, f, s))).wait_recv()

    def w_go(name, f, s, second, step):
        w_wait(name, f, s)
        dz, dy = place(name, 0, step) if second else place(name, step, 0)
        rz, ry = place(name, f, s)
        k = n_sent[0]
        n_sent[0] += 1
        go(remote(
            source(name, f, s), unit(name, rz, ry, c), w_send.at[k], w_sem(name, rz - dz, ry - dy),
            z=at(z, dz), y=at(y, dy),
        ))

    pair_index = {}

    def share(name, f, s):
        w_wait(name, f, s)
        k = pair_index.setdefault((name, f, s), len(pair_index))
        go(remote(
            source(name, f, s), unit(name, *place(name, f, s), c),
            pair_sem.at[0, k], pair_sem.at[1, k], c=o,
        ))

    def pair_wait(name, f, s):
        k = pair_index[(name, f, s)]
        ref = unit(name, *place(name, f, s), o)
        remote(ref, ref, pair_sem.at[0, k], pair_sem.at[1, k], c=o).wait_recv()

    def pump(i):
        for n, f, s, second, step in SENDS[i]:
            w_go(names[n], f, s, second, step)
        for n, f, s in SHARES[i]:
            share(names[n], f, s)

    pump(0)


    for cp in fetched:
        cp.wait()
    lane = lax.broadcasted_iota(jnp.int32, (8, L), 1)
    rows = []
    both = []
    row8 = lax.broadcasted_iota(jnp.int32, (8, L), 0)
    raw_steps = jnp.concatenate([steps_s[...].astype(F32), steps_l[...].astype(F32)], axis=0)
    softened = jnp.maximum(raw_steps, 0.0) + jnp.log1p(jnp.exp(-jnp.abs(raw_steps)))
    head = lax.broadcasted_iota(jnp.int32, (3, T), 0)
    rate = jnp.where(head == 0, rates_s[0:1, 0:1], jnp.where(head == 1, rates_s[0:1, 1:2], rates_l[0:1, 0:1]))
    offsets = jnp.concatenate([offs_s[...], offs_l[...]], axis=0)
    meta = jnp.concatenate(
        [offsets - jnp.exp(rate) * softened, softened, jnp.zeros((2, T), F32)], axis=0
    )
    for k in range(NB):
        raw = meta[:, k * L : (k + 1) * L]
        acc = raw
        for sft in (1, 2, 4, 8, 16, 32, 64):
            acc = acc + jnp.where(lane >= sft, pltpu.roll(acc, sft, 1), 0.0)
        rows.append(acc)
        both.append(jnp.where(row8 < 3, acc, raw))
    both.append(jnp.zeros((L - 8 * NB, L), F32))
    cols = jnp.concatenate(both, axis=0).T
    grown = jnp.exp(cols)
    shrunk = jnp.exp(cols[L - 1 : L, :] - cols)

    half = lax.broadcasted_iota(jnp.int32, (L, L), 1) < 64
    half1 = lax.broadcasted_iota(jnp.int32, (1, L), 1) < 64

    def spread(m, k, off):
        b = 8 * k + off
        small = jnp.where(half, m[:, b : b + 1], m[:, b + 1 : b + 2])
        large = jnp.broadcast_to(m[:, b + 2 : b + 3], (L, L))
        return small, large

    def block_decay(k):
        b = 8 * k
        e = grown[L - 1 : L]
        small = jnp.where(half1, e[:, b : b + 1], e[:, b + 1 : b + 2])
        large = jnp.broadcast_to(e[:, b + 2 : b + 3], (1, L))
        return jnp.concatenate([small, large], axis=1)

    tap_rows = []
    for j in range(4):
        m = taps_m[j].astype(F32)
        tap_rows.append(
            [taps_s[j : j + 1].astype(F32), taps_l[j : j + 1].astype(F32)]
            + [m[i : i + 1] for i in range(4)]
        )

    def conv(k, g):
        total = None
        for j in range(4):
            row = k * L + 5 + j
            if g < 2:
                rows_j = cbuf[row : row + L, g * 128 : g * 128 + 128]
            else:
                rows_j = cmaps[pl.ds(4 * row + g - 2, L, 4), :]
            part = tap_rows[j][g] * rows_j
            total = part if total is None else total + part
        return silu(total)

    for i in range(3):
        local[i].wait()
    for k in range(NB):
        cbuf[8 + k * L : 8 + (k + 1) * L, :] = xin[k * L : (k + 1) * L, :].astype(F32)
        maps_k = pl.ds(32 + 4 * k * L, 4 * L)
        cmaps[maps_k, :] = sxin[4 * k * L : 4 * (k + 1) * L, :].astype(F32)
    decays = [block_decay(k) for k in range(NB)]

    def first_pass(k, kind):
        dt, sh = spread(cols, k, 3)[kind], spread(shrunk, k, 0)[kind]
        blk, at_kind = pl.ds(k * L, L), pl.ds(kind * 128, 128)
        d = conv(k, kind) * dt
        drive[blk, at_kind] = d.astype(BF16)
        key = conv(k, 2 + 2 * kind).astype(BF16)
        conv_k[blk, 256 * kind : 256 * kind + 128] = key
        conv_k[blk, 256 * kind + 128 : 256 * kind + 256] = conv(k, 3 + 2 * kind).astype(BF16)
        fresh[k, :, at_kind] = dot_tn(key, (d * sh).astype(BF16))

    for kind in range(2):
        for k in range(1, NB):
            first_pass(k, kind)
    for cp in halos:
        cp.wait_recv()
    start = jnp.where(jnp.logical_and(z == 0, y == 0), 0.0, 1.0)
    cbuf[0:8, :] = halo[8:16, :].astype(F32) * start
    cmaps[0:32, :] = halo_m[32:64, :].astype(F32) * start

    def state_out(buf, kind, state, total, stage, **axis):
        buf[kind, 0, 0:128] = state.astype(BF16)
        buf[kind, 0, 128:136] = jnp.broadcast_to(total, (8, 128)).astype(BF16)
        ((name, me),) = axis.items()
        copies = [
            remote(
                buf.at[kind, 0], buf.at[kind, r],
                st_sem.at[2 * stage, kind, r], st_sem.at[2 * stage + 1, kind, r],
                **{name: at(me, r)},
            )
            for r in (1, 2, 3)
        ]
        pending.extend(copies)
        return copies

    def start_all(copies):
        for cp in copies:
            cp.start()

    def states_in(buf, kind, stage):
        for r in (1, 2, 3):
            remote(
                buf.at[kind, 0], buf.at[kind, r],
                st_sem.at[2 * stage, kind, r], st_sem.at[2 * stage + 1, kind, r],
            ).wait_recv()

    def chained(buf, kind, me):
        line, line_d = jnp.zeros((128, 128), F32), jnp.ones((1, 128), F32)
        before, before_d = line, line_d
        for j in range(4):
            blob = buf[kind, rem(me - j + 4, 4)].astype(F32)
            line = line * blob[128:129] + blob[0:128]
            line_d = line_d * blob[128:129]
            before = jnp.where(j < me, line, before)
            before_d = jnp.where(j < me, line_d, before_d)
        return before, before_d, line, line_d

    later = []
    for kind in range(2):
        first_pass(0, kind)
        own = slice(kind * 128, kind * 128 + 128)
        state, total = fresh[0, :, own], decays[0][:, own]
        for k in range(1, NB):
            state = state * decays[k][:, own] + fresh[k, :, own]
            total = total * decays[k][:, own]
        copies = state_out(st1, kind, state, total, 0, y=y)
        pl.when(c == 0)(functools.partial(start_all, copies))
        later += copies

    mask = lax.broadcasted_iota(jnp.int32, (L, L), 0) >= lax.broadcasted_iota(jnp.int32, (L, L), 1)

    def weights_of(k, h):
        b = 8 * k + h
        diff = cols[:, b : b + 1] - rows[k][h : h + 1, :]
        return jnp.exp(jnp.where(mask, diff, -1e30))

    def second_pass(k):
        blk = pl.ds(k * L, L)
        s_s = dot_nt(conv_k[blk, 128:256], conv_k[blk, 0:128])
        s_l = dot_nt(conv_k[blk, 384:512], conv_k[blk, 256:384])
        d_s = drive[blk, 0:128]
        o_0 = dot((s_s * weights_of(k, 0)).astype(BF16), d_s)
        o_1 = dot((s_s * weights_of(k, 1)).astype(BF16), d_s)
        inner[blk, 0:128] = jnp.where(half, o_0, o_1)
        inner[blk, 128:256] = dot((s_l * weights_of(k, 2)).astype(BF16), drive[blk, 128:256])

    for k in range(NB):
        second_pass(k)
    pl.when(c == 1)(functools.partial(start_all, later))
    pump(1)

    wo_copies = [
        go(remote(src, wo.at[c, rows], hp_sem.at[0, 8 + i], hp_sem.at[1, 8 + i], c=o))
        for i, (src, rows) in enumerate(((ws_in, pl.ds(0, 128)), (wl_in, pl.ds(128, 128))))
    ]
    inside = []
    for kind in range(2):
        states_in(st1, kind, 0)
        before, before_d, line, line_d = chained(st1, kind, y)
        inside.append((before, before_d))
        start_all(state_out(st2, kind, line, line_d, 1, z=z))
        if kind == 0:
            pump(2)
    pump(3)

    for i in (3, 4):
        local[i].wait()

    def third_pass(k, kind, carry):
        blk, cols_k = pl.ds(k * L, L), pl.ds(kind * 128, 128)
        own = slice(kind * 128, kind * 128 + 128)
        reads = conv_k[blk, 256 * kind + 128 : 256 * kind + 256]
        out_k = inner[blk, cols_k] + dot(reads, carry.astype(BF16)) * spread(grown, k, 0)[kind]
        carry = carry * decays[k][:, own] + fresh[k, :, own]
        out_k = out_k * silu(gin[blk, cols_k].astype(F32))
        sq = out_k * out_k
        if kind == 0:
            sq_0 = jnp.sum(jnp.where(half, sq, 0.0), axis=1, keepdims=True)
            sq_1 = jnp.sum(jnp.where(half, 0.0, sq), axis=1, keepdims=True)
            mean = jnp.where(half, sq_0, sq_1) * (1.0 / 64)
            gain = gain_s[...]
        else:
            mean = jnp.sum(sq, axis=1, keepdims=True) * (1.0 / 128)
            gain = gain_l[...]
        heads[blk, cols_k] = (out_k * lax.rsqrt(mean + head_eps) * gain).astype(BF16)
        return carry

    for kind in range(2):
        states_in(st2, kind, 1)
        before = chained(st2, kind, z)[0]
        carry = before * inside[kind][1] + inside[kind][0]
        for k in range(NB):
            carry = third_pass(k, kind, carry)
        if kind == 0:
            pump(4)

    hpart, lhs = (hpart_0, hpart_1), (lhs_0, lhs_1)
    parts, left, right = (parts_0, parts_1), (left_0, left_1), (right_0, right_1)
    mid = (mid_0, mid_1)

    def rows_of(b, core, t):
        first, n = LOTS[t]
        return pl.ds(pl.multiple_of((2 * b + core) * R + first, 16), n)

    def block_of(b, t):
        n = LOTS[t][1]
        return pl.ds(b * n if isinstance(b, int) else pl.multiple_of(b * n, 16), n)

    def row_of(b, t):
        first, n = LOTS[t]
        return pl.ds(pl.multiple_of(4 * first + b * n, 16), n)

    hp_copies = [
        [
            go(remote(
                heads.at[rows_of(b, o, t)], hpart[t].at[block_of(b, t)],
                hp_sem.at[0, 4 * t + b], hp_sem.at[1, 4 * t + b], c=o,
            ))
            for b in range(4)
        ]
        for t in range(2)
    ]
    for t in range(2):
        for b in range(4):
            lhs[t][block_of(b, t), :] = heads[rows_of(b, c, t), :]
    pump(5)
    for i in (6, 7):
        local[i].wait()
    for cp in wo_copies:
        cp.wait_recv()

    x1, x2, x3 = at(x, 1), at(x, 2), at(x, 3)

    class Sum:
        def __init__(self, part, from_left, from_right, sem):
            self.part, self.left, self.right, self.sem = part, from_left, from_right, sem

        def to_right(self, slot, block, role):
            go(remote(self.part(block, role), self.left(slot), self.sem(0, slot), self.sem(1, slot), x=x1))

        def to_left(self, slot, block, role):
            go(remote(self.part(block, role), self.right(slot), self.sem(2, slot), self.sem(3, slot), x=x3))

        def wait_left(self, slot):
            ref = self.left(slot)
            remote(ref, ref, self.sem(0, slot), self.sem(1, slot)).wait_recv()
            return ref[...].astype(F32)

        def wait_right(self, slot):
            ref = self.right(slot)
            remote(ref, ref, self.sem(2, slot), self.sem(3, slot)).wait_recv()
            return ref[...].astype(F32)

        def relayed(self):
            self.to_right(0, x2, 0)
            self.to_left(0, x2, 1)

        def direct(self):
            self.to_right(1, x1, 1)
            self.to_left(1, x3, 0)

        def merge(self):
            mine = self.part(x1, 0)
            mine[...] = (self.wait_left(0) + mine[...].astype(F32)).astype(BF16)
            self.to_right(2, x1, 0)
            mine = self.part(x3, 1)
            mine[...] = (self.wait_right(0) + mine[...].astype(F32)).astype(BF16)
            self.to_left(2, x3, 1)

        def result(self, role):
            a, b = (2, 1) if role == 0 else (1, 2)
            return self.part(x, role)[...].astype(F32) + self.wait_left(a) + self.wait_right(b)

    def mixed_sum(t):
        return Sum(
            lambda block, role: parts[t].at[block, role],
            lambda slot: left[t].at[slot], lambda slot: right[t].at[slot],
            lambda k, slot: rs_sem.at[t, k, slot],
        )

    mixed = [mixed_sum(0), mixed_sum(1)]

    def project(t):
        n = LOTS[t][1]
        for cp in hp_copies[t]:
            cp.wait_recv()
        mine, other = lhs[t][...], hpart[t][...]
        for role in range(2):
            for e in range(4):
                cols_e = pl.ds(role * H + e * 256, 256)
                acc = dot(mine, wo[c, :, cols_e]) + dot(other, wo[o, :, cols_e])
                parts[t][:, role, :, e * 256 : (e + 1) * 256] = acc.reshape(4, n, 256).astype(BF16)

    project(0)
    mixed[0].relayed()
    mixed[0].direct()
    project(1)
    mixed[1].relayed()
    pump(6)
    mixed[0].merge()
    mixed[1].direct()
    pump(7)
    mixed[1].merge()
    pump(8)
    local[5].wait()

    def norm(t):
        first, n = LOTS[t]
        wide = []
        for role in range(2):
            at_role = slice(role * H, role * H + H)
            m = (resv[first : first + n, at_role].astype(F32) + mixed[t].result(role)).astype(BF16)
            mid[t][:, at_role] = m
            wide.append(m.astype(F32))
        square = sum(jnp.sum(w * w, axis=1, keepdims=True) for w in wide)
        scale = lax.rsqrt(square * (1.0 / DM) + row_eps)
        for role in range(2):
            at_role = slice(role * H, role * H + H)
            ag[role, row_of(x, t), :] = (wide[role] * scale * gain_n[:, at_role]).astype(BF16)

    def ag_right(t, slot, block, role):
        ref = ag.at[role, row_of(block, t)]
        go(remote(ref, ref, ag_sem.at[t, 0, slot], ag_sem.at[t, 1, slot], x=x1))

    def ag_left(t, slot, block, role):
        ref = ag.at[role, row_of(block, t)]
        go(remote(ref, ref, ag_sem.at[t, 2, slot], ag_sem.at[t, 3, slot], x=x3))

    def ag_wait(t, side, slot, block, role):
        ref = ag.at[role, row_of(block, t)]
        remote(ref, ref, ag_sem.at[t, 0, slot], ag_sem.at[t, side, slot]).wait_recv()

    def ag_relay(t):
        ag_wait(t, 1, 0, x3, 0)
        ag_right(t, 2, x3, 0)
        ag_wait(t, 3, 0, x1, 1)
        ag_left(t, 2, x1, 1)

    def ag_rest(t):
        ag_wait(t, 1, 1, x3, 1)
        ag_wait(t, 3, 1, x1, 0)
        ag_wait(t, 1, 2, x2, 0)
        ag_wait(t, 3, 2, x2, 1)

    norm(0)
    ag_right(0, 0, x, 0)
    ag_left(0, 0, x, 1)
    ag_right(0, 1, x, 1)
    ag_left(0, 1, x, 0)
    pump(9)
    norm(1)
    ag_right(1, 0, x, 0)
    ag_left(1, 0, x, 1)
    pump(10)
    ag_relay(0)
    ag_right(1, 1, x, 1)
    ag_left(1, 1, x, 0)
    pump(11)
    ag_relay(1)
    pump(12)
    ag_rest(0)
    pump(13)
    ag_rest(1)
    for i in (8, 9, 10):
        local[i].wait()

    def lined_up(w, core, h, n0, n):
        pieces = [w[core, 2 * h + j // 4, j % 4, n0 : n0 + n, :] for j in range(8)]
        return jnp.concatenate(pieces, axis=1)

    def expand(core):
        for n0, n in ((0, 256), (256, 256), (512, 192)):
            gate = up = None
            for h in range(2):
                a = ag[h]
                w_gate = lined_up(wg, core, h, n0, n)
                w_up = lined_up(wu, core, h, n0, n)
                gate = dot_nt(a, w_gate) if gate is None else gate + dot_nt(a, w_gate)
                up = dot_nt(a, w_up) if up is None else up + dot_nt(a, w_up)
            hid[core, :, n0 : n0 + n] = (silu(gate) * up).astype(BF16)

    expand(c)
    pump(14)
    for name in ("G", "U"):
        for f in STEPS:
            for st in STEPS:
                pair_wait(name, f, st)
    expand(o)

    def rows_in(i, role):
        return role if i % 2 == 0 else 1 - role

    def down_sum(i):
        return Sum(
            lambda block, role: dparts[i][rows_in(i, role)].at[block],
            lambda slot: dleft[i][rows_in(i, slot % 2)].at[slot],
            lambda slot: dright[i][rows_in(i, 1 - slot % 2)].at[slot],
            lambda k, slot: rs2_sem.at[i, k, slot],
        )

    down = [down_sum(i) for i in range(5)]

    def finish(i):
        for role in range(2):
            t = rows_in(i, role)
            first, n = LOTS[t]
            total = down[i].result(role)
            for j, (rz, ry) in enumerate(COLUMNS[i]):
                at_j = pl.ds(pl.multiple_of((at(z, rz) * 4 + at(y, ry)) * 128, 128), 128)
                out[first : first + n, at_j] = (
                    mid[t][:, at_j].astype(F32) + total[:, 128 * j : 128 * j + 128]
                ).astype(BF16)

    for i in range(5):
        if i == 2:
            settled = len(pending)
        for rz, ry in COLUMNS[i]:
            for name in ("A", "B"):
                pair_wait(name, *place(name, rz, ry))
        for e in range(WIDTHS[i] // 256):
            acc = None
            for cc in range(2):
                w_down = jnp.concatenate(
                    [wd[cc, at(z, rz), at(y, ry)] for rz, ry in COLUMNS[i][2 * e : 2 * e + 2]], axis=1
                )
                acc = dot(hid[cc], w_down) if acc is None else acc + dot(hid[cc], w_down)
            for t, (first, n) in enumerate(LOTS):
                lot_acc = acc[4 * first : 4 * first + 4 * n].reshape(4, n, 256)
                dparts[i][t][:, :, e * 256 : (e + 1) * 256] = lot_acc.astype(BF16)
        down[i].relayed()
        for j in AFTER[i][0]:
            down[j].direct()
        for j in AFTER[i][1]:
            down[j].merge()
        for j in AFTER[i][2]:
            pump(j)
    down[2].merge()
    for cp in pending[:settled]:
        cp.wait_send()
    del pending[:settled]
    down[3].merge()
    down[4].merge()
    for i in range(5):
        finish(i)

    for cp in pending:
        cp.wait_send()


def on_device(
    residual, small_value_inputs, large_value_inputs, small_gate_inputs, large_gate_inputs,
    state_projections, small_step_inputs, large_step_inputs, small_decay_offsets,
    large_decay_offsets, small_decay_rates, large_decay_rates, small_filter_taps,
    large_filter_taps, state_filter_taps, small_head_gains, large_head_gains,
    small_output_projection, large_output_projection, channel_norm_gain, gate_matrix,
    up_matrix, down_matrix,
):
    flat = state_projections.reshape(4 * T, 128)

    anywhere = pl.BlockSpec(memory_space=pl.ANY)
    dma = pltpu.SemaphoreType.DMA
    V = pltpu.VMEM
    return pl.pallas_call(
        kernel,
        out_shape=pltpu.VMEM((R, DM), BF16),
        in_specs=[anywhere] * 23,
        out_specs=pl.BlockSpec(memory_space=pltpu.VMEM),
        scratch_shapes=[
            [
                V((2, T), BF16), V((1, T), BF16), V((2, T), F32), V((1, T), F32), V((1, 2), F32), V((1, 1), F32),
                V((4, 128), BF16), V((4, 128), BF16), V((4, 4, 128), BF16), V((1, 128), F32), V((1, 128), F32),
                V((1, DM), F32),
            ],
            V((T, 256), BF16),
            V((4 * T, 128), BF16),
            V((T, 256), BF16),
            V((R, DM), BF16),
            V((16, 256), BF16),
            V((64, 128), BF16),
            V((T + 8, 256), F32),
            V((4 * T + 32, 128), F32),
            V((T, 512), BF16),
            V((T, 256), BF16),
            V((NB, 128, 256), F32),
            V((T, 256), F32),
            V((T, 256), BF16),
            *[V((4 * n, 256), BF16) for _, n in LOTS],
            *[V((4 * n, 256), BF16) for _, n in LOTS],
            V((2, 256, DM), BF16),
            V((2, 4, 4, FD, KROWS), BF16),
            V((2, 4, 4, FD, KROWS), BF16),
            V((2, 4, 4, FD, KROWS), BF16),
            V((2, 4, 136, 128), BF16),
            V((2, 4, 136, 128), BF16),
            *[V((4, 2, n, H), BF16) for _, n in LOTS],
            *[V((3, n, H), BF16) for _, n in LOTS],
            *[V((3, n, H), BF16) for _, n in LOTS],
            V((2, 4 * R, H), BF16),
            V((2, 4 * R, FD), BF16),
            [[V((4, n, w), BF16) for _, n in LOTS] for w in WIDTHS],
            [[V((3, n, w), BF16) for _, n in LOTS] for w in WIDTHS],
            [[V((3, n, w), BF16) for _, n in LOTS] for w in WIDTHS],
            *[V((n, DM), BF16) for _, n in LOTS],
            dma((23,)),
            dma((2, 3)),
            dma((60,)),
            dma((4, 4, 4)),
            dma((2, 64)),
            dma((4, 2, 4)),
            dma((2, 10)),
            dma((2, 4, 3)),
            dma((2, 4, 3)),
            dma((5, 4, 3)),
        ],
        compiler_params=pltpu.CompilerParams(
            collective_id=0, has_side_effects=True, vmem_limit_bytes=60 * 1024 * 1024
        ),
    )(
        residual, small_value_inputs, large_value_inputs, small_gate_inputs, large_gate_inputs,
        flat, small_output_projection, large_output_projection, gate_matrix.T, up_matrix.T, down_matrix,
        small_step_inputs.T, large_step_inputs.T, small_decay_offsets.T, large_decay_offsets.T,
        small_decay_rates.reshape(1, 2), large_decay_rates.reshape(1, 1), small_filter_taps, large_filter_taps, state_filter_taps,
        small_head_gains.reshape(1, 128), large_head_gains.reshape(1, 128),
        channel_norm_gain.reshape(1, DM),
    )


def solution(mesh):
    split = Mesh(mesh.devices.reshape(4, 4, 4, 2), ("z", "y", "x", "c"))
    in_specs = (
        P(SP_TP, None),
        P(SP, TP),
        P(SP, TP),
        P(SP, TP),
        P(SP, TP),
        P(SP, None, None),
        P(SP, TP),
        P(SP, TP),
        P(SP, TP),
        P(SP, TP),
        P(TP),
        P(TP),
        P(None, TP),
        P(None, TP),
        P(),
        P(TP),
        P(TP),
        P(TP, None),
        P(TP, None),
        P(),
        P(SP, TP),
        P(SP, TP),
        P(TP, SP),
    )
    return jax.shard_map(
        on_device, mesh=split, in_specs=in_specs, out_specs=P(SP_TP, None), check_vma=False
    )
```

```python
import functools

import jax
import jax.numpy as jnp
from jax import lax
from jax.experimental import pallas as pl
from jax.experimental.pallas import tpu as pltpu
from jax.sharding import Mesh
from jax.sharding import PartitionSpec as P

F32 = jnp.float32
BF16 = jnp.bfloat16
SP = ("z", "y")
TP = ("x", "c")
SP_TP = ("z", "y", "x", "c")

T = 640
L = 128
NB = T // L
R = 80
FD = 704
DM = 2048
H = 1024
KROWS = 128
CUT = 352
AFTER = (((0,), (), ()), ((1,), (), (15,)), ((2,), (0,), (16, 17)), ((), (1,), ()), ((3, 4), (), (18, 19)))
WIDTHS = (512, 256, 512, 512, 256)
LOTS = ((0, 48), (48, 32))
STEPS = (0, 1, -1, 2)
COLUMNS = (
    ((0, 0), (1, 0), (0, 1), (-1, 0)),
    ((0, -1), (1, 1)),
    ((1, -1), (-1, 1), (2, 0), (-1, -1)),
    ((0, 2), (2, 1), (1, 2), (2, -1)),
    ((2, 2), (-1, 2)),
)
SENDS = (
    ((0, 0, 0, 0, 1), (0, 0, 0, 0, -1), (1, 0, 0, 0, 1), (1, 0, 0, 0, -1), (0, 0, 0, 1, 1), (0, 0, 0, 1, -1)),
    ((1, 0, 0, 1, 1), (1, 0, 0, 1, -1)),
    (),
    ((1, -1, 0, 0, 1), (0, -1, 0, 0, 1), (0, 1, 0, 1, -1), (1, 1, 0, 1, -1)),
    ((0, 1, 0, 1, 1), (0, -1, 0, 1, -1), (1, 1, 0, 1, 1), (1, -1, 0, 1, -1)),
    (),
    ((0, -1, 0, 1, 1), (1, -1, 0, 1, 1), (3, 0, 0, 0, -1), (2, 0, 0, 0, -1), (0, 0, 1, 1, -1), (1, 0, 1, 1, -1)),
    ((0, 2, 0, 1, 1), (1, 2, 0, 1, 1), (0, 2, 0, 1, -1), (1, 2, 0, 1, -1)),
    ((3, 0, 0, 0, 1), (2, 0, 0, 0, 1)),
    ((0, 1, -1, 1, 1), (0, -1, 1, 1, -1), (1, 1, -1, 1, 1), (1, -1, 1, 1, -1)),
    ((0, 2, -1, 1, 1), (1, 2, -1, 1, 1), (3, 1, 0, 0, -1), (2, 1, 0, 0, -1)),
    ((2, 0, 0, 1, -1), (3, 0, 0, 1, -1), (2, 0, 0, 1, 1), (2, 1, 0, 1, -1), (3, 0, 0, 1, 1), (3, 1, 0, 1, -1)),
    ((2, 1, 0, 1, 1), (2, -1, 0, 1, -1), (3, 1, 0, 1, 1), (3, -1, 0, 1, -1)),
    ((2, 2, 0, 1, 1), (2, 2, 0, 1, -1), (3, 2, 0, 1, 1), (3, 2, 0, 1, -1), (2, -1, 0, 1, 1), (3, -1, 0, 1, 1)),
    ((2, 0, 1, 1, -1), (3, 0, 1, 1, -1), (2, 1, 1, 1, -1), (3, 1, 1, 1, -1)),
    ((2, 2, -1, 1, 1), (3, 2, -1, 1, 1), (2, -1, 1, 1, -1), (3, -1, 1, 1, -1)),
    (),
    (),
    (),
    (),
)
SHARES = (
    (),
    (),
    ((0, -1, 0), (0, 1, 0), (1, -1, 0), (1, 1, 0)),
    ((0, 0, 0), (1, 0, 0), (2, 0, 0), (3, 0, 0)),
    ((0, 0, -1), (0, 0, 1)),
    ((1, 0, -1), (1, 0, 1)),
    (),
    ((1, 2, 0), (0, 1, 1), (0, 2, 0), (1, 1, 1), (0, 1, -1), (0, -1, 1)),
    ((1, 1, -1), (1, -1, 1), (3, 1, 0), (2, 1, 0)),
    ((0, -1, -1), (1, -1, -1), (0, 0, 2)),
    ((1, 0, 2), (0, 2, -1), (1, 2, -1)),
    ((0, 2, 1), (3, -1, 0), (1, 2, 1), (2, -1, 0)),
    ((0, 1, 2), (0, -1, 2), (1, 1, 2), (1, -1, 2)),
    ((3, 2, 0), (2, 2, 0), (0, 2, 2), (1, 2, 2)),
    ((2, 0, 1), (3, 0, 1), (2, 0, -1), (2, 1, 1), (3, 0, -1), (3, 1, 1)),
    ((2, 1, -1), (2, -1, 1), (3, 1, -1), (3, -1, 1), (2, 2, -1), (2, 2, 1), (3, 2, -1), (3, 2, 1), (2, -1, -1), (2, 0, 2), (3, -1, -1)),
    ((3, 0, 2), (2, 1, 2), (3, 1, 2), (2, -1, 2)),
    ((2, 2, 2), (3, 2, 2), (3, -1, 2)),
    (),
    (),
)

head_eps = 1e-05
row_eps = 1e-06


def silu(x):
    return x / (1.0 + jnp.exp(-x))


def dot(a, b):
    return jnp.dot(a, b, preferred_element_type=F32)


def dot_nt(a, b):
    return lax.dot_general(a, b, (((1,), (1,)), ((), ())), preferred_element_type=F32)


def dot_tn(a, b):
    return lax.dot_general(a, b, (((0,), (0,)), ((), ())), preferred_element_type=F32)


def kernel(
    res_in, vs_in, vl_in, gs_in, gl_in, sp_in, ws_in, wl_in, g_in, u_in, d_in,
    small_in_0, small_in_1, small_in_2, small_in_3, small_in_4, small_in_5, small_in_6, small_in_7,
    small_in_8, small_in_9, small_in_10, small_in_11,
    out,
    small,
    xin, sxin, gin, resv, halo, halo_m, cbuf, cmaps, conv_k, drive, fresh, inner, heads, hpart_0, hpart_1, lhs_0, lhs_1,
    wo, wg, wu, wd, st1, st2, parts_0, parts_1, left_0, left_1, right_0, right_1, ag, hid,
    dparts, dleft, dright, mid_0, mid_1,
    loc_sem, halo_sem, w_send, w_recv, pair_sem, st_sem, hp_sem, rs_sem, ag_sem, rs2_sem,
):
    z, y, x, c = (lax.axis_index(n) for n in ("z", "y", "x", "c"))
    rem = lax.rem
    o = 1 - c

    def at(base, by):
        return rem(base + (by % 4), 4)

    nxt = {"z": rem(z + lax.div(y + 1, 4), 4), "y": rem(y + 1, 4)}
    prv = {"z": rem(z + 3 + lax.div(y + 3, 4), 4), "y": rem(y + 3, 4)}

    def there(**kw):
        base = {"z": z, "y": y, "x": x, "c": c}
        base.update(kw)
        return (base["z"], base["y"], base["x"], base["c"])

    def remote(src, dst, send, recv, **kw):
        return pltpu.make_async_remote_copy(
            src_ref=src, dst_ref=dst, send_sem=send, recv_sem=recv,
            device_id=there(**kw), device_id_type=pl.DeviceIdType.MESH,
        )

    pending = []

    def go(cp):
        cp.start()
        pending.append(cp)
        return cp

    barrier = pltpu.get_barrier_semaphore()
    peers = [
        dict(c=o), dict(x=at(x, 1)), dict(x=at(x, 3)),
        dict(y=at(y, 1)), dict(y=at(y, 2)), dict(y=at(y, 3)),
        dict(z=at(z, 1)), dict(z=at(z, 2)), dict(z=at(z, 3)),
        nxt, prv,
    ]
    for p in peers:
        pl.semaphore_signal(barrier, inc=1, device_id=there(**p), device_id_type=pl.DeviceIdType.MESH)
    local = [
        *zip(
            (small_in_0, small_in_1, small_in_2, small_in_3, small_in_4, small_in_5, small_in_6,
             small_in_7, small_in_8, small_in_9, small_in_10, small_in_11), small,
        ),
        (vs_in, xin.at[:, pl.ds(0, 128)]),
        (vl_in, xin.at[:, pl.ds(128, 128)]),
        (sp_in, sxin),
        (gs_in, gin.at[:, pl.ds(0, 128)]),
        (gl_in, gin.at[:, pl.ds(128, 128)]),
        (res_in, resv),
        (ws_in, wo.at[c, pl.ds(0, 128)]),
        (wl_in, wo.at[c, pl.ds(128, 128)]),
        (g_in, wg.at[c, z, y]),
        (u_in, wu.at[c, z, y]),
        (d_in, wd.at[c, z, y]),
    ]
    local = [pltpu.make_async_copy(a, b, loc_sem.at[i]) for i, (a, b) in enumerate(local)]
    for cp in local:
        cp.start()
    fetched, local = local[:12], local[12:]
    steps_s, steps_l, offs_s, offs_l, rates_s, rates_l, taps_s, taps_l, taps_m, gain_s, gain_l, gain_n = small

    pl.semaphore_wait(barrier, len(peers))

    tail = pl.ds(T - 16, 16)
    halos = [
        go(remote(src, dst, halo_sem.at[0, i], halo_sem.at[1, i], **nxt))
        for i, (src, dst) in enumerate((
            (vs_in.at[tail], halo.at[:, pl.ds(0, 128)]),
            (vl_in.at[tail], halo.at[:, pl.ds(128, 128)]),
            (sp_in.at[pl.ds(4 * T - 64, 64)], halo_m),
        ))
    ]

    names = ("G", "U", "A", "B")
    own_src = {
        "G": g_in, "U": u_in,
        "A": d_in.at[pl.ds(0, CUT)], "B": d_in.at[pl.ds(CUT, CUT)],
    }

    def unit(name, rz, ry, core):
        zz, yy = at(z, rz), at(y, ry)
        if name == "G":
            return wg.at[core, zz, yy]
        if name == "U":
            return wu.at[core, zz, yy]
        rows = pl.ds(0, CUT) if name == "A" else pl.ds(CUT, CUT)
        return wd.at[core, zz, yy, rows]

    def place(name, f, s):
        return (f, s) if name in ("U", "B") else (s, f)

    def source(name, f, s):
        return own_src[name] if (f, s) == (0, 0) else unit(name, *place(name, f, s), c)

    def w_sem(name, rz, ry):
        return w_recv.at[names.index(name), rz % 4, ry % 4]

    n_sent = [0]
    here = {(n, 0, 0) for n in names}

    def w_wait(name, f, s):
        if (name, f, s) not in here:
            here.add((name, f, s))
            ref = unit(name, *place(name, f, s), c)
            remote(ref, ref, w_send.at[0], w_sem(name, *place(name, f, s))).wait_recv()

    def w_go(name, f, s, second, step):
        w_wait(name, f, s)
        dz, dy = place(name, 0, step) if second else place(name, step, 0)
        rz, ry = place(name, f, s)
        k = n_sent[0]
        n_sent[0] += 1
        go(remote(
            source(name, f, s), unit(name, rz, ry, c), w_send.at[k], w_sem(name, rz - dz, ry - dy),
            z=at(z, dz), y=at(y, dy),
        ))

    pair_index = {}

    def share(name, f, s):
        w_wait(name, f, s)
        k = pair_index.setdefault((name, f, s), len(pair_index))
        go(remote(
            source(name, f, s), unit(name, *place(name, f, s), c),
            pair_sem.at[0, k], pair_sem.at[1, k], c=o,
        ))

    def pair_wait(name, f, s):
        k = pair_index[(name, f, s)]
        ref = unit(name, *place(name, f, s), o)
        remote(ref, ref, pair_sem.at[0, k], pair_sem.at[1, k], c=o).wait_recv()

    def pump(i):
        for n, f, s, second, step in SENDS[i]:
            w_go(names[n], f, s, second, step)
        for n, f, s in SHARES[i]:
            share(names[n], f, s)

    pump(0)


    for cp in fetched:
        cp.wait()
    lane = lax.broadcasted_iota(jnp.int32, (8, L), 1)
    rows = []
    both = []
    row8 = lax.broadcasted_iota(jnp.int32, (8, L), 0)
    raw_steps = jnp.concatenate([steps_s[...].astype(F32), steps_l[...].astype(F32)], axis=0)
    softened = jnp.maximum(raw_steps, 0.0) + jnp.log1p(jnp.exp(-jnp.abs(raw_steps)))
    head = lax.broadcasted_iota(jnp.int32, (3, T), 0)
    rate = jnp.where(head == 0, rates_s[0:1, 0:1], jnp.where(head == 1, rates_s[0:1, 1:2], rates_l[0:1, 0:1]))
    offsets = jnp.concatenate([offs_s[...], offs_l[...]], axis=0)
    meta = jnp.concatenate(
        [offsets - jnp.exp(rate) * softened, softened, jnp.zeros((2, T), F32)], axis=0
    )
    for k in range(NB):
        raw = meta[:, k * L : (k + 1) * L]
        acc = raw
        for sft in (1, 2, 4, 8, 16, 32, 64):
            acc = acc + jnp.where(lane >= sft, pltpu.roll(acc, sft, 1), 0.0)
        rows.append(acc)
        both.append(jnp.where(row8 < 3, acc, raw))
    both.append(jnp.zeros((L - 8 * NB, L), F32))
    cols = jnp.concatenate(both, axis=0).T
    grown = jnp.exp(cols)
    shrunk = jnp.exp(cols[L - 1 : L, :] - cols)

    half = lax.broadcasted_iota(jnp.int32, (L, L), 1) < 64
    half1 = lax.broadcasted_iota(jnp.int32, (1, L), 1) < 64

    def spread(m, k, off):
        b = 8 * k + off
        small = jnp.where(half, m[:, b : b + 1], m[:, b + 1 : b + 2])
        large = jnp.broadcast_to(m[:, b + 2 : b + 3], (L, L))
        return small, large

    def block_decay(k):
        b = 8 * k
        e = grown[L - 1 : L]
        small = jnp.where(half1, e[:, b : b + 1], e[:, b + 1 : b + 2])
        large = jnp.broadcast_to(e[:, b + 2 : b + 3], (1, L))
        return jnp.concatenate([small, large], axis=1)

    tap_rows = []
    for j in range(4):
        m = taps_m[j].astype(F32)
        tap_rows.append(
            [taps_s[j : j + 1].astype(F32), taps_l[j : j + 1].astype(F32)]
            + [m[i : i + 1] for i in range(4)]
        )

    def conv(k, g):
        total = None
        for j in range(4):
            row = k * L + 5 + j
            if g < 2:
                rows_j = cbuf[row : row + L, g * 128 : g * 128 + 128]
            else:
                rows_j = cmaps[pl.ds(4 * row + g - 2, L, 4), :]
            part = tap_rows[j][g] * rows_j
            total = part if total is None else total + part
        return silu(total)

    for i in range(3):
        local[i].wait()
    for k in range(NB):
        cbuf[8 + k * L : 8 + (k + 1) * L, :] = xin[k * L : (k + 1) * L, :].astype(F32)
        maps_k = pl.ds(32 + 4 * k * L, 4 * L)
        cmaps[maps_k, :] = sxin[4 * k * L : 4 * (k + 1) * L, :].astype(F32)
    decays = [block_decay(k) for k in range(NB)]

    def first_pass(k, kind):
        dt, sh = spread(cols, k, 3)[kind], spread(shrunk, k, 0)[kind]
        blk, at_kind = pl.ds(k * L, L), pl.ds(kind * 128, 128)
        d = conv(k, kind) * dt
        drive[blk, at_kind] = d.astype(BF16)
        key = conv(k, 2 + 2 * kind).astype(BF16)
        conv_k[blk, 256 * kind : 256 * kind + 128] = key
        conv_k[blk, 256 * kind + 128 : 256 * kind + 256] = conv(k, 3 + 2 * kind).astype(BF16)
        fresh[k, :, at_kind] = dot_tn(key, (d * sh).astype(BF16))

    for kind in range(2):
        for k in range(1, NB):
            first_pass(k, kind)
    for cp in halos:
        cp.wait_recv()
    start = jnp.where(jnp.logical_and(z == 0, y == 0), 0.0, 1.0)
    cbuf[0:8, :] = halo[8:16, :].astype(F32) * start
    cmaps[0:32, :] = halo_m[32:64, :].astype(F32) * start

    def state_out(buf, kind, state, total, stage, **axis):
        buf[kind, 0, 0:128] = state.astype(BF16)
        buf[kind, 0, 128:136] = jnp.broadcast_to(total, (8, 128)).astype(BF16)
        ((name, me),) = axis.items()
        copies = [
            remote(
                buf.at[kind, 0], buf.at[kind, r],
                st_sem.at[2 * stage, kind, r], st_sem.at[2 * stage + 1, kind, r],
                **{name: at(me, r)},
            )
            for r in (1, 2, 3)
        ]
        pending.extend(copies)
        return copies

    def start_all(copies):
        for cp in copies:
            cp.start()

    def states_in(buf, kind, stage):
        for r in (1, 2, 3):
            remote(
                buf.at[kind, 0], buf.at[kind, r],
                st_sem.at[2 * stage, kind, r], st_sem.at[2 * stage + 1, kind, r],
            ).wait_recv()

    def chained(buf, kind, me):
        line, line_d = jnp.zeros((128, 128), F32), jnp.ones((1, 128), F32)
        before, before_d = line, line_d
        for j in range(4):
            blob = buf[kind, rem(me - j + 4, 4)].astype(F32)
            line = line * blob[128:129] + blob[0:128]
            line_d = line_d * blob[128:129]
            before = jnp.where(j < me, line, before)
            before_d = jnp.where(j < me, line_d, before_d)
        return before, before_d, line, line_d

    later = []
    for kind in range(2):
        first_pass(0, kind)
        own = slice(kind * 128, kind * 128 + 128)
        state, total = fresh[0, :, own], decays[0][:, own]
        for k in range(1, NB):
            state = state * decays[k][:, own] + fresh[k, :, own]
            total = total * decays[k][:, own]
        copies = state_out(st1, kind, state, total, 0, y=y)
        pl.when(c == 0)(functools.partial(start_all, copies))
        later += copies

    mask = lax.broadcasted_iota(jnp.int32, (L, L), 0) >= lax.broadcasted_iota(jnp.int32, (L, L), 1)

    def weights_of(k, h):
        b = 8 * k + h
        diff = cols[:, b : b + 1] - rows[k][h : h + 1, :]
        return jnp.exp(jnp.where(mask, diff, -1e30))

    def second_pass(k):
        blk = pl.ds(k * L, L)
        s_s = dot_nt(conv_k[blk, 128:256], conv_k[blk, 0:128])
        s_l = dot_nt(conv_k[blk, 384:512], conv_k[blk, 256:384])
        d_s = drive[blk, 0:128]
        o_0 = dot((s_s * weights_of(k, 0)).astype(BF16), d_s)
        o_1 = dot((s_s * weights_of(k, 1)).astype(BF16), d_s)
        inner[blk, 0:128] = jnp.where(half, o_0, o_1)
        inner[blk, 128:256] = dot((s_l * weights_of(k, 2)).astype(BF16), drive[blk, 128:256])

    for k in range(NB):
        second_pass(k)
    pl.when(c == 1)(functools.partial(start_all, later))
    pump(1)

    wo_copies = [
        go(remote(src, wo.at[c, rows], hp_sem.at[0, 8 + i], hp_sem.at[1, 8 + i], c=o))
        for i, (src, rows) in enumerate(((ws_in, pl.ds(0, 128)), (wl_in, pl.ds(128, 128))))
    ]
    inside = []
    for kind in range(2):
        states_in(st1, kind, 0)
        before, before_d, line, line_d = chained(st1, kind, y)
        inside.append((before, before_d))
        start_all(state_out(st2, kind, line, line_d, 1, z=z))
        if kind == 0:
            pump(2)
    pump(3)

    for i in (3, 4):
        local[i].wait()

    def third_pass(k, kind, carry):
        blk, cols_k = pl.ds(k * L, L), pl.ds(kind * 128, 128)
        own = slice(kind * 128, kind * 128 + 128)
        reads = conv_k[blk, 256 * kind + 128 : 256 * kind + 256]
        out_k = inner[blk, cols_k] + dot(reads, carry.astype(BF16)) * spread(grown, k, 0)[kind]
        carry = carry * decays[k][:, own] + fresh[k, :, own]
        out_k = out_k * silu(gin[blk, cols_k].astype(F32))
        sq = out_k * out_k
        if kind == 0:
            sq_0 = jnp.sum(jnp.where(half, sq, 0.0), axis=1, keepdims=True)
            sq_1 = jnp.sum(jnp.where(half, 0.0, sq), axis=1, keepdims=True)
            mean = jnp.where(half, sq_0, sq_1) * (1.0 / 64)
            gain = gain_s[...]
        else:
            mean = jnp.sum(sq, axis=1, keepdims=True) * (1.0 / 128)
            gain = gain_l[...]
        heads[blk, cols_k] = (out_k * lax.rsqrt(mean + head_eps) * gain).astype(BF16)
        return carry

    for kind in range(2):
        states_in(st2, kind, 1)
        before = chained(st2, kind, z)[0]
        carry = before * inside[kind][1] + inside[kind][0]
        for k in range(NB):
            carry = third_pass(k, kind, carry)
        if kind == 0:
            pump(4)

    hpart, lhs = (hpart_0, hpart_1), (lhs_0, lhs_1)
    parts, left, right = (parts_0, parts_1), (left_0, left_1), (right_0, right_1)
    mid = (mid_0, mid_1)

    def rows_of(b, core, t):
        first, n = LOTS[t]
        return pl.ds(pl.multiple_of((2 * b + core) * R + first, 16), n)

    def block_of(b, t):
        n = LOTS[t][1]
        return pl.ds(b * n if isinstance(b, int) else pl.multiple_of(b * n, 16), n)

    def row_of(b, t):
        first, n = LOTS[t]
        return pl.ds(pl.multiple_of(4 * first + b * n, 16), n)

    hp_copies = [
        [
            go(remote(
                heads.at[rows_of(b, o, t)], hpart[t].at[block_of(b, t)],
                hp_sem.at[0, 4 * t + b], hp_sem.at[1, 4 * t + b], c=o,
            ))
            for b in range(4)
        ]
        for t in range(2)
    ]
    for t in range(2):
        for b in range(4):
            lhs[t][block_of(b, t), :] = heads[rows_of(b, c, t), :]
    pump(5)
    for i in (6, 7):
        local[i].wait()
    for cp in wo_copies:
        cp.wait_recv()

    x1, x2, x3 = at(x, 1), at(x, 2), at(x, 3)

    class Sum:
        def __init__(self, part, from_left, from_right, sem):
            self.part, self.left, self.right, self.sem = part, from_left, from_right, sem

        def to_right(self, slot, block, role):
            go(remote(self.part(block, role), self.left(slot), self.sem(0, slot), self.sem(1, slot), x=x1))

        def to_left(self, slot, block, role):
            go(remote(self.part(block, role), self.right(slot), self.sem(2, slot), self.sem(3, slot), x=x3))

        def wait_left(self, slot):
            ref = self.left(slot)
            remote(ref, ref, self.sem(0, slot), self.sem(1, slot)).wait_recv()
            return ref[...].astype(F32)

        def wait_right(self, slot):
            ref = self.right(slot)
            remote(ref, ref, self.sem(2, slot), self.sem(3, slot)).wait_recv()
            return ref[...].astype(F32)

        def relayed(self):
            self.to_right(0, x2, 0)
            self.to_left(0, x2, 1)

        def direct(self):
            self.to_right(1, x1, 1)
            self.to_left(1, x3, 0)

        def merge(self):
            mine = self.part(x1, 0)
            mine[...] = (self.wait_left(0) + mine[...].astype(F32)).astype(BF16)
            self.to_right(2, x1, 0)
            mine = self.part(x3, 1)
            mine[...] = (self.wait_right(0) + mine[...].astype(F32)).astype(BF16)
            self.to_left(2, x3, 1)

        def result(self, role):
            a, b = (2, 1) if role == 0 else (1, 2)
            return self.part(x, role)[...].astype(F32) + self.wait_left(a) + self.wait_right(b)

    def mixed_sum(t):
        return Sum(
            lambda block, role: parts[t].at[block, role],
            lambda slot: left[t].at[slot], lambda slot: right[t].at[slot],
            lambda k, slot: rs_sem.at[t, k, slot],
        )

    mixed = [mixed_sum(0), mixed_sum(1)]

    def project(t):
        n = LOTS[t][1]
        for cp in hp_copies[t]:
            cp.wait_recv()
        mine, other = lhs[t][...], hpart[t][...]
        for role in range(2):
            for e in range(4):
                cols_e = pl.ds(role * H + e * 256, 256)
                acc = dot(mine, wo[c, :, cols_e]) + dot(other, wo[o, :, cols_e])
                parts[t][:, role, :, e * 256 : (e + 1) * 256] = acc.reshape(4, n, 256).astype(BF16)
            if role == 0:
                mixed[t].to_right(0, x2, 0)
            else:
                mixed[t].to_left(0, x2, 1)

    project(0)
    mixed[0].direct()
    project(1)
    pump(6)
    mixed[0].merge()
    mixed[1].direct()
    pump(7)
    mixed[1].merge()
    pump(8)
    local[5].wait()

    def norm(t):
        first, n = LOTS[t]
        wide = []
        for role in range(2):
            at_role = slice(role * H, role * H + H)
            m = (resv[first : first + n, at_role].astype(F32) + mixed[t].result(role)).astype(BF16)
            mid[t][:, at_role] = m
            wide.append(m.astype(F32))
        square = sum(jnp.sum(w * w, axis=1, keepdims=True) for w in wide)
        scale = lax.rsqrt(square * (1.0 / DM) + row_eps)
        for role in range(2):
            at_role = slice(role * H, role * H + H)
            ag[role, row_of(x, t), :] = (wide[role] * scale * gain_n[:, at_role]).astype(BF16)

    def ag_right(t, slot, block, role):
        ref = ag.at[role, row_of(block, t)]
        go(remote(ref, ref, ag_sem.at[t, 0, slot], ag_sem.at[t, 1, slot], x=x1))

    def ag_left(t, slot, block, role):
        ref = ag.at[role, row_of(block, t)]
        go(remote(ref, ref, ag_sem.at[t, 2, slot], ag_sem.at[t, 3, slot], x=x3))

    def ag_wait(t, side, slot, block, role):
        ref = ag.at[role, row_of(block, t)]
        remote(ref, ref, ag_sem.at[t, 0, slot], ag_sem.at[t, side, slot]).wait_recv()

    def ag_relay(t):
        ag_wait(t, 1, 0, x3, 0)
        ag_right(t, 2, x3, 0)
        ag_wait(t, 3, 0, x1, 1)
        ag_left(t, 2, x1, 1)

    def ag_rest(t):
        ag_wait(t, 1, 1, x3, 1)
        ag_wait(t, 3, 1, x1, 0)
        ag_wait(t, 1, 2, x2, 0)
        ag_wait(t, 3, 2, x2, 1)

    norm(0)
    ag_right(0, 0, x, 0)
    ag_left(0, 0, x, 1)
    ag_right(0, 1, x, 1)
    ag_left(0, 1, x, 0)
    pump(9)
    norm(1)
    ag_right(1, 0, x, 0)
    ag_left(1, 0, x, 1)
    pump(10)
    ag_relay(0)
    ag_right(1, 1, x, 1)
    ag_left(1, 1, x, 0)
    pump(11)
    ag_relay(1)
    pump(12)
    ag_rest(0)
    pump(13)
    ag_rest(1)
    for i in (8, 9, 10):
        local[i].wait()

    def lined_up(w, core, h, n0, n):
        pieces = [w[core, 2 * h + j // 4, j % 4, n0 : n0 + n, :] for j in range(8)]
        return jnp.concatenate(pieces, axis=1)

    def expand(core):
        for n0, n in ((0, 256), (256, 256), (512, 192)):
            gate = up = None
            for h in range(2):
                a = ag[h]
                w_gate = lined_up(wg, core, h, n0, n)
                w_up = lined_up(wu, core, h, n0, n)
                gate = dot_nt(a, w_gate) if gate is None else gate + dot_nt(a, w_gate)
                up = dot_nt(a, w_up) if up is None else up + dot_nt(a, w_up)
            hid[core, :, n0 : n0 + n] = (silu(gate) * up).astype(BF16)

    expand(c)
    pump(14)
    for name in ("G", "U"):
        for f in STEPS:
            for st in STEPS:
                pair_wait(name, f, st)
    expand(o)

    def rows_in(i, role):
        return role if i % 2 == 0 else 1 - role

    def down_sum(i):
        return Sum(
            lambda block, role: dparts[i][rows_in(i, role)].at[block],
            lambda slot: dleft[i][rows_in(i, slot % 2)].at[slot],
            lambda slot: dright[i][rows_in(i, 1 - slot % 2)].at[slot],
            lambda k, slot: rs2_sem.at[i, k, slot],
        )

    down = [down_sum(i) for i in range(5)]

    def finish(i):
        for role in range(2):
            t = rows_in(i, role)
            first, n = LOTS[t]
            total = down[i].result(role)
            for j, (rz, ry) in enumerate(COLUMNS[i]):
                at_j = pl.ds(pl.multiple_of((at(z, rz) * 4 + at(y, ry)) * 128, 128), 128)
                out[first : first + n, at_j] = (
                    mid[t][:, at_j].astype(F32) + total[:, 128 * j : 128 * j + 128]
                ).astype(BF16)

    for i in range(5):
        if i == 2:
            settled = len(pending)
        for rz, ry in COLUMNS[i]:
            for name in ("A", "B"):
                pair_wait(name, *place(name, rz, ry))
        for e in range(WIDTHS[i] // 256):
            acc = None
            for cc in range(2):
                w_down = jnp.concatenate(
                    [wd[cc, at(z, rz), at(y, ry)] for rz, ry in COLUMNS[i][2 * e : 2 * e + 2]], axis=1
                )
                acc = dot(hid[cc], w_down) if acc is None else acc + dot(hid[cc], w_down)
            for t, (first, n) in enumerate(LOTS):
                lot_acc = acc[4 * first : 4 * first + 4 * n].reshape(4, n, 256)
                dparts[i][t][:, :, e * 256 : (e + 1) * 256] = lot_acc.astype(BF16)
        down[i].relayed()
        for j in AFTER[i][0]:
            down[j].direct()
        for j in AFTER[i][1]:
            down[j].merge()
        for j in AFTER[i][2]:
            pump(j)
    down[2].merge()
    for cp in pending[:settled]:
        cp.wait_send()
    del pending[:settled]
    down[3].merge()
    down[4].merge()
    for i in range(5):
        finish(i)

    for cp in pending:
        cp.wait_send()


def on_device(
    residual, small_value_inputs, large_value_inputs, small_gate_inputs, large_gate_inputs,
    state_projections, small_step_inputs, large_step_inputs, small_decay_offsets,
    large_decay_offsets, small_decay_rates, large_decay_rates, small_filter_taps,
    large_filter_taps, state_filter_taps, small_head_gains, large_head_gains,
    small_output_projection, large_output_projection, channel_norm_gain, gate_matrix,
    up_matrix, down_matrix,
):
    flat = state_projections.reshape(4 * T, 128)

    anywhere = pl.BlockSpec(memory_space=pl.ANY)
    dma = pltpu.SemaphoreType.DMA
    V = pltpu.VMEM
    return pl.pallas_call(
        kernel,
        out_shape=pltpu.VMEM((R, DM), BF16),
        in_specs=[anywhere] * 23,
        out_specs=pl.BlockSpec(memory_space=pltpu.VMEM),
        scratch_shapes=[
            [
                V((2, T), BF16), V((1, T), BF16), V((2, T), F32), V((1, T), F32), V((1, 2), F32), V((1, 1), F32),
                V((4, 128), BF16), V((4, 128), BF16), V((4, 4, 128), BF16), V((1, 128), F32), V((1, 128), F32),
                V((1, DM), F32),
            ],
            V((T, 256), BF16),
            V((4 * T, 128), BF16),
            V((T, 256), BF16),
            V((R, DM), BF16),
            V((16, 256), BF16),
            V((64, 128), BF16),
            V((T + 8, 256), F32),
            V((4 * T + 32, 128), F32),
            V((T, 512), BF16),
            V((T, 256), BF16),
            V((NB, 128, 256), F32),
            V((T, 256), F32),
            V((T, 256), BF16),
            *[V((4 * n, 256), BF16) for _, n in LOTS],
            *[V((4 * n, 256), BF16) for _, n in LOTS],
            V((2, 256, DM), BF16),
            V((2, 4, 4, FD, KROWS), BF16),
            V((2, 4, 4, FD, KROWS), BF16),
            V((2, 4, 4, FD, KROWS), BF16),
            V((2, 4, 136, 128), BF16),
            V((2, 4, 136, 128), BF16),
            *[V((4, 2, n, H), BF16) for _, n in LOTS],
            *[V((3, n, H), BF16) for _, n in LOTS],
            *[V((3, n, H), BF16) for _, n in LOTS],
            V((2, 4 * R, H), BF16),
            V((2, 4 * R, FD), BF16),
            [[V((4, n, w), BF16) for _, n in LOTS] for w in WIDTHS],
            [[V((3, n, w), BF16) for _, n in LOTS] for w in WIDTHS],
            [[V((3, n, w), BF16) for _, n in LOTS] for w in WIDTHS],
            *[V((n, DM), BF16) for _, n in LOTS],
            dma((23,)),
            dma((2, 3)),
            dma((60,)),
            dma((4, 4, 4)),
            dma((2, 64)),
            dma((4, 2, 4)),
            dma((2, 10)),
            dma((2, 4, 3)),
            dma((2, 4, 3)),
            dma((5, 4, 3)),
        ],
        compiler_params=pltpu.CompilerParams(
            collective_id=0, has_side_effects=True, vmem_limit_bytes=60 * 1024 * 1024
        ),
    )(
        residual, small_value_inputs, large_value_inputs, small_gate_inputs, large_gate_inputs,
        flat, small_output_projection, large_output_projection, gate_matrix.T, up_matrix.T, down_matrix,
        small_step_inputs.T, large_step_inputs.T, small_decay_offsets.T, large_decay_offsets.T,
        small_decay_rates.reshape(1, 2), large_decay_rates.reshape(1, 1), small_filter_taps, large_filter_taps, state_filter_taps,
        small_head_gains.reshape(1, 128), large_head_gains.reshape(1, 128),
        channel_norm_gain.reshape(1, DM),
    )


def solution(mesh):
    split = Mesh(mesh.devices.reshape(4, 4, 4, 2), ("z", "y", "x", "c"))
    in_specs = (
        P(SP_TP, None),
        P(SP, TP),
        P(SP, TP),
        P(SP, TP),
        P(SP, TP),
        P(SP, None, None),
        P(SP, TP),
        P(SP, TP),
        P(SP, TP),
        P(SP, TP),
        P(TP),
        P(TP),
        P(None, TP),
        P(None, TP),
        P(),
        P(TP),
        P(TP),
        P(TP, None),
        P(TP, None),
        P(),
        P(SP, TP),
        P(SP, TP),
        P(TP, SP),
    )
    return jax.shard_map(
        on_device, mesh=split, in_specs=in_specs, out_specs=P(SP_TP, None), check_vma=False
    )
```
